256 devices in a mesh: grp: 2 (over z), sp: 64 (over y, x), tp: 2 (over core).
Axes of the slice: x: 8, y: 8, z: 2, core: 2. Of those that a mesh axis runs over, the one named last changes fastest.
The devices are a block of a 8x8x16 slice.
Arguments:
- resid: bfloat16 [16384, 2048], P(('grp', 'sp')), parts along dimension 0, may hold values from -6 to 6
- queries_first: bfloat16 [16384, 2048], P(('grp', 'sp'), 'tp'), parts along dimension 0, may hold values from -150 to 150
- keys_first: bfloat16 [16384, 2048], P(('grp', 'sp'), 'tp'), parts along dimension 0, may hold values from -6 to 6
- values_first: bfloat16 [16384, 2048], P(('grp', 'sp'), 'tp'), parts along dimension 0, may hold values from -6 to 6
- rel_first: float32 [16, 257], P('tp'), may hold values from -4 to 4
- post_first: float32 [2048], replicated, may hold values from 0.1 to 1.9
- out_first: bfloat16 [2048, 2048], P('tp', 'sp'), may hold values from -0.125 to 0.125
- pre_second: float32 [2048], replicated, may hold values from 0.1 to 1.9
- query_weight: bfloat16 [2048, 2048], P('sp', 'tp'), may hold values from -0.125 to 0.125
- key_weight: bfloat16 [2048, 2048], P('sp', 'tp'), may hold values from -0.125 to 0.125
- value_weight: bfloat16 [2048, 2048], P('sp', 'tp'), may hold values from -0.125 to 0.125
- rel_second: float32 [16, 257], P('tp'), may hold values from -4 to 4
- post_second: float32 [2048], replicated, may hold values from 0.1 to 1.9
- out_second: bfloat16 [2048, 2048], P('tp', 'sp'), may hold values from -0.125 to 0.125
Outputs:
- hidden_two: bfloat16 [16384, 2048], P(('grp', 'sp')), parts along dimension 0
The draws below stay inside these ranges and needn't reach their ends.
There are 2 independent parts, one for each index of `grp`. The reference program is written for one: setup_inputs(seed, part) draws one part's arguments, and reference() takes and returns one part's arrays. A program takes and returns all parts, laid end to end along the dimension named above; an argument that names none is the same for every part. Nothing has to cross between parts.
All inputs are finite; a program needn't handle non-finite values.
Results may differ from the reference program's by a relative error of at most 0.017.
Values may be sent and summed in bfloat16 or wider, within the bound.
A program may use at most 128 MiB of HBM per device.

```python
import jax
import jax.numpy as jnp
from jax import lax

D = 2048
HEADS = 16
SEG = 64
LEFT = 8
REACH = 512
REL_CLIP = 128
TOK_DEV = 128
TOKENS = 8192
N_SP = 64
N_TP = 2


def draw_pair(key):
    base = jax.random.fold_in(key, 41)
    key_draw = jnp.clip(jax.random.normal(jax.random.fold_in(base, 1), (TOKENS, D), jnp.float32), -6.0, 6.0)
    query_draw = jnp.clip(jax.random.normal(jax.random.fold_in(base, 2), (TOKENS, D), jnp.float32), -6.0, 6.0)
    return (query_draw, key_draw)


def draw_keys_first(key, part):
    return draw_pair(key)[1].astype(jnp.bfloat16)


def draw_queries_first(key, part):
    query_draw, key_draw = draw_pair(key)
    return query_draw.astype(jnp.bfloat16)


def block_levels(own_key, dims, cuts, smallest, top_value):
    def one(dim, parts):
        draws = jax.random.uniform(jax.random.fold_in(jax.random.fold_in(own_key, 6), dim), (parts,), jnp.float32, smallest / len(cuts), top_value / len(cuts))
        return jnp.repeat(jnp.exp(draws), dims[dim] // parts).reshape((-1,) + (1,) * (len(dims) - dim - 1))

    level = one(*cuts[0])
    for cut in cuts[1:]:
        level = level * one(*cut)
    return level


def normal_values(rng, shape, deviation, reach, shards=(), kind=jnp.bfloat16):
    values = jax.random.normal(rng, shape, jnp.float32) * deviation
    if len(shards) > 0:
        values = block_levels(rng, shape, shards, -0.22, 0.18) * values
    return jnp.clip(values, min=-reach, max=reach).astype(kind)


def setup_inputs(seed: int = 0, part: int = 0) -> dict:
    seeds = jax.random.split(jax.random.key(seed), 15)
    part_keys = jax.random.split(jax.random.fold_in(seeds[14], part), 15)
    return {
        "resid": normal_values(part_keys[0], (TOKENS, D), 1.0, 6.0, ((0, 64),)),
        "queries_first": draw_queries_first(jax.random.fold_in(jax.random.fold_in(seeds[14], part), 71), part),
        "keys_first": draw_keys_first(jax.random.fold_in(jax.random.fold_in(seeds[14], part), 71), part),
        "values_first": normal_values(part_keys[3], (TOKENS, D), 1.0, 6.0, ((0, 64), (1, 2))),
        "rel_first": normal_values(seeds[4], (HEADS, 2 * REL_CLIP + 1), 1.0, 4.0, ((0, 2),), jnp.float32),
        "post_first": jnp.clip(1.0 + 0.18 * jax.random.normal(seeds[5], (D,), jnp.float32), 0.1, 1.9),
        "out_first": normal_values(seeds[6], (D, D), D ** -0.5, 0.125, ((0, 2), (1, 64))),
        "pre_second": jnp.clip(1.0 + 0.18 * jax.random.normal(seeds[7], (D,), jnp.float32), 0.1, 1.9),
        "query_weight": normal_values(seeds[8], (D, D), D ** -0.5, 0.125, ((0, 64), (1, 2))),
        "key_weight": normal_values(seeds[9], (D, D), D ** -0.5, 0.125, ((0, 64), (1, 2))),
        "value_weight": normal_values(seeds[10], (D, D), D ** -0.5, 0.125, ((0, 64), (1, 2))),
        "rel_second": normal_values(seeds[11], (HEADS, 2 * REL_CLIP + 1), 1.0, 4.0, ((0, 2),), jnp.float32),
        "post_second": jnp.clip(1.0 + 0.18 * jax.random.normal(seeds[12], (D,), jnp.float32), 0.1, 1.9),
        "out_second": normal_values(seeds[13], (D, D), D ** -0.5, 0.125, ((0, 2), (1, 64))),
    }


EPS = 1e-06
NEG_FILL = -1e+30

def band_bias(bias_table):
    heads_here = bias_table.shape[0]
    band = (LEFT + 1) * SEG
    length = SEG + band
    index = jnp.arange(length, dtype=jnp.int32)
    distance = jnp.where(index < band, LEFT * SEG - index, LEFT * SEG + length - index)
    slot = jnp.clip(distance, -REL_CLIP, REL_CLIP) + REL_CLIP
    onehot = (slot[:, None] == jnp.arange(2 * REL_CLIP + 1, dtype=jnp.int32)[None, :]).astype(jnp.float32)
    diagonal_values = jnp.dot(bias_table, onehot.T, precision=lax.Precision.HIGHEST)
    spread = jnp.broadcast_to(diagonal_values[:, None, :], (heads_here, SEG, length)).reshape(heads_here, SEG * length)
    return spread[:, :SEG * (length - 1)].reshape(heads_here, SEG, length - 1)[:, :, :band]

def attend_band(queries, key_rows, value_rows, bias, key_live):
    rows, width = queries.shape
    heads_here = bias.shape[0]
    head_size = width // heads_here
    blocks = rows // SEG
    query_seg = queries.reshape(blocks, SEG, heads_here, head_size).astype(jnp.float32)
    key_seg = key_rows.reshape(blocks + LEFT, SEG, heads_here, head_size).astype(jnp.float32)
    value_seg = value_rows.reshape(blocks + LEFT, SEG, heads_here, head_size).astype(jnp.float32)
    live_seg = key_live.reshape(blocks + LEFT, SEG)
    key_band = jnp.concatenate([key_seg[earlier:earlier + blocks] for earlier in range(LEFT + 1)], axis=1)
    value_band = jnp.concatenate([value_seg[earlier:earlier + blocks] for earlier in range(LEFT + 1)], axis=1)
    live_band = jnp.concatenate([live_seg[earlier:earlier + blocks] for earlier in range(LEFT + 1)], axis=1)
    scores = jnp.einsum('nqhd,nkhd->nhqk', query_seg, key_band) * head_size ** (-0.5) + bias[None]
    scores = jnp.where(live_band[:, None, None, :], scores, NEG_FILL)
    largest = lax.optimization_barrier(jnp.max(scores, axis=-1, keepdims=True))
    weights = jnp.exp(scores - largest)
    weights = (weights / lax.optimization_barrier(jnp.sum(weights, axis=-1, keepdims=True))).astype(jnp.bfloat16)
    mixed = jnp.einsum('nhqk,nkhd->nqhd', weights.astype(jnp.float32), value_band)
    return mixed.astype(jnp.bfloat16).reshape(rows, width)

def attention_whole(queries, key_rows, value_rows, bias_table):
    bias = band_bias(bias_table)
    padding = jnp.zeros((REACH, key_rows.shape[1]), jnp.bfloat16)
    key_padded = jnp.concatenate([padding, key_rows], axis=0)
    value_padded = jnp.concatenate([padding, value_rows], axis=0)

    def one_block(number):
        start = (number * TOK_DEV).astype(jnp.int32)
        query_block = lax.dynamic_slice_in_dim(queries, start, TOK_DEV, 0)
        key_block = lax.dynamic_slice_in_dim(key_padded, start, TOK_DEV + REACH, 0)
        value_block = lax.dynamic_slice_in_dim(value_padded, start, TOK_DEV + REACH, 0)
        position = start - REACH + jnp.arange(TOK_DEV + REACH, dtype=jnp.int32)
        return attend_band(query_block, key_block, value_block, bias, position >= 0)
    result = lax.map(one_block, jnp.arange(N_SP, dtype=jnp.int32))
    return result.reshape(TOKENS, key_rows.shape[1])

def project_out(mixed, weight):
    width = D // N_TP
    total = jnp.zeros((mixed.shape[0], D), jnp.float32)
    for member in range(N_TP):
        term = jnp.dot(mixed[:, member * width:(member + 1) * width], weight[member * width:(member + 1) * width], preferred_element_type=jnp.float32).astype(jnp.bfloat16)
        total = total + term.astype(jnp.float32)
    return total.astype(jnp.bfloat16)

def normed(hidden, gain):
    values = hidden.astype(jnp.float32)
    scale = lax.rsqrt(lax.optimization_barrier(jnp.mean(values * values, axis=-1, keepdims=True)) + EPS)
    return (values * scale * gain).astype(jnp.bfloat16)

def residual_add(branch, residual, gain):
    values = branch.astype(jnp.float32)
    scale = lax.rsqrt(lax.optimization_barrier(jnp.mean(values * values, axis=-1, keepdims=True)) + EPS)
    return (residual.astype(jnp.float32) + values * scale * gain).astype(jnp.bfloat16)

def reference(resid, queries_first, keys_first, values_first, rel_first, post_first, out_first, pre_second, query_weight, key_weight, value_weight, rel_second, post_second, out_second):
    first = attention_whole(queries_first, keys_first, values_first, rel_first)
    hidden_one = residual_add(project_out(first, out_first), resid, post_first)
    inputs_two = normed(hidden_one, pre_second)
    queries_two = jnp.dot(inputs_two, query_weight, preferred_element_type=jnp.float32).astype(jnp.bfloat16)
    keys_two = jnp.dot(inputs_two, key_weight, preferred_element_type=jnp.float32).astype(jnp.bfloat16)
    values_two = jnp.dot(inputs_two, value_weight, preferred_element_type=jnp.float32).astype(jnp.bfloat16)
    second = attention_whole(queries_two, keys_two, values_two, rel_second)
    return residual_add(project_out(second, out_second), hidden_one, post_second)
```

```python
import functools
import math

import jax
import jax.numpy as jnp
from jax import lax
from jax.experimental import pallas as pl
from jax.experimental.pallas import tpu as pltpu
from jax.sharding import PartitionSpec as P

SEG = 64
LEFT = 8
REACH = 512
REL_CLIP = 128
EPS = 1e-06
NEG_FILL = -1e30
LOG2E = 1.4426950408889634
BF = jnp.bfloat16
F32 = jnp.float32
MESH = pl.DeviceIdType.MESH
VM = pl.BlockSpec(memory_space=pltpu.VMEM)
ANY = pl.BlockSpec(memory_space=pl.ANY)
NT = (((1,), (1,)), ((), ()))


def place(side):
    sp = lax.axis_index("sp")
    return lax.rem(sp, side), lax.div(sp, side), lax.axis_index("tp")


def remote(src, dst, send, recv, **where):
    return pltpu.make_async_remote_copy(
        src_ref=src,
        dst_ref=dst,
        send_sem=send,
        recv_sem=recv,
        device_id=dict(where),
        device_id_type=MESH,
    )


def greet(side, x, y, rows, core):
    barrier = pltpu.get_barrier_semaphore()
    count = 0
    if rows:
        for d in range(1, side):
            peer = y * side + lax.rem(x + d, side)
            pl.semaphore_signal(barrier, inc=1, device_id={"sp": peer}, device_id_type=MESH)
            count += 1
        for d in (1, side - 1):
            peer = lax.rem(y + d, side) * side + x
            pl.semaphore_signal(barrier, inc=1, device_id={"sp": peer}, device_id_type=MESH)
            count += 1
    if core:
        pl.semaphore_signal(
            barrier, inc=1, device_id={"tp": 1 - lax.axis_index("tp")}, device_id_type=MESH
        )
        count += 1
    pl.semaphore_wait(barrier, count)


def spread_bias(diag_ref, band_ref, x):
    tok, window = band_ref.shape
    line = diag_ref[pl.ds(x, 1), :]
    wide = jnp.broadcast_to(line, (tok, line.shape[1]))
    wide = pltpu.roll(wide, 0, 1, stride=1, stride_axis=0)[:, :window] * LOG2E
    qseg = lax.broadcasted_iota(jnp.int32, (tok, window), 0) // SEG
    kseg = lax.broadcasted_iota(jnp.int32, (tok, window), 1) // SEG
    band_ref[...] = jnp.where((kseg >= qseg) & (kseg <= qseg + LEFT), wide, NEG_FILL)


def attend(block, first_row, qs, ks, vs, band_ref):
    tok, window = band_ref.shape
    head = qs.shape[1]
    at = pl.multiple_of(block * tok, tok)
    query = qs[pl.ds(at, tok), :]
    keys = ks[pl.ds(at, window), :]
    values = vs[pl.ds(at, window), :]
    scores = lax.dot_general(query, keys, NT, preferred_element_type=F32)
    scores = scores * (head**-0.5 * LOG2E) + band_ref[...]
    if first_row is not None:
        column = lax.broadcasted_iota(jnp.int32, (1, window), 1) + block * tok
        hidden = jnp.logical_and(column < REACH, first_row)
        scores = scores + jnp.where(hidden, NEG_FILL, 0.0)
    largest = jnp.max(scores, axis=-1, keepdims=True)
    weights = jnp.exp2(scores - largest)
    total = jnp.sum(weights, axis=-1, keepdims=True)
    mixed = jnp.dot(weights.astype(BF), values, preferred_element_type=F32)
    return (mixed / total).astype(BF)


def attend_rows(side, x, y, qs, ks, vs, band, outs, mixed, ssem, rsem, halo_wait):
    tok, head = band.shape[0], qs.shape[1]
    here = pl.ds(pl.multiple_of(x * head, head), head)

    def hand_back(block):
        rows = pl.ds(pl.multiple_of(block * tok, tok), tok)
        return remote(
            outs.at[rows, :], mixed.at[:, here], ssem.at[block], rsem.at[x], sp=y * side + block
        )

    def run(block, first_row):
        result = attend(block, first_row, qs, ks, vs, band)
        outs[pl.ds(pl.multiple_of(block * tok, tok), tok), :] = result

        @pl.when(block != x)
        def _():
            hand_back(block).start()

        @pl.when(block == x)
        def _():
            mixed[:, here] = result

    half = REACH // tok

    def late(i, carry):
        run(i + half, None)
        return carry

    lax.fori_loop(0, side - half, late, 0)
    halo_wait()

    def early(i, carry):
        run(i, y == 0)
        return carry

    lax.fori_loop(0, half, early, 0)

    def finish(block, carry):
        @pl.when(block != x)
        def _():
            hand_back(block).wait_send()
            there = pl.ds(pl.multiple_of(block * head, head), head)
            remote(
                outs.at[pl.ds(0, tok), :],
                mixed.at[:, there],
                ssem.at[block],
                rsem.at[block],
                sp=y * side + block,
            ).wait_recv()

        return carry

    lax.fori_loop(0, side, finish, 0)


def clear_halo(y, ks, vs):
    @pl.when(y == 0)
    def _():
        ks[pl.ds(0, REACH), :] = jnp.zeros((REACH, ks.shape[1]), BF)
        vs[pl.ds(0, REACH), :] = jnp.zeros((REACH, vs.shape[1]), BF)


def first_kernel(
    side, q_ref, k_ref, v_ref, diag_ref, wq_ref, wk_ref, wv_ref, mixed_ref, wall_ref,
    qs, ks, vs, outs, mixed, wall, band, s_a2a, r_a2a, s_up, r_up, s_down, r_down,
    s_halo, r_halo, s_back, r_back,
):
    x, y, _ = place(side)
    tok, head = q_ref.shape[0], qs.shape[1]
    wrow = wq_ref.shape[0]
    group = side * wrow
    greet(side, x, y, True, False)

    mine = pl.ds(pl.multiple_of(x * tok, tok), tok)
    mine_late = pl.ds(pl.multiple_of(REACH + x * tok, tok), tok)
    wmine = pl.ds(pl.multiple_of(y * group + x * wrow, wrow), wrow)
    kinds = [
        (wq_ref, lambda: wall.at[wmine, pl.ds(0, head)]),
        (wk_ref, lambda: wall.at[wmine, pl.ds(head, head)]),
        (wv_ref, lambda: wall.at[wmine, pl.ds(2 * head, head)]),
        (k_ref, lambda: ks.at[mine_late, :]),
        (v_ref, lambda: vs.at[mine_late, :]),
        (q_ref, lambda: qs.at[mine, :]),
    ]

    def piece(kind, d):
        peer = lax.rem(x + d, side)
        src, dst = kinds[kind]
        cut = src.at[:, pl.ds(pl.multiple_of(peer * head, head), head)]
        if d == 0:
            return pltpu.make_async_copy(cut, dst(), r_a2a.at[kind, 0])
        return remote(cut, dst(), s_a2a.at[kind, d], r_a2a.at[kind, d], sp=y * side + peer)

    pieces = [[piece(kind, d) for d in range(side)] for kind in range(6)]
    for kind in range(6):
        for d in range(side):
            pieces[kind][d].start()

    def take(kind):
        pieces[kind][0].wait()
        for d in range(1, side):
            pieces[kind][d].wait_recv()

    up = lax.rem(y + 1, side) * side + x
    down = lax.rem(y + side - 1, side) * side + x

    def ring(step, going_up):
        owner = lax.rem(y - step + side, side) if going_up else lax.rem(y + step, side)
        rows = pl.ds(pl.multiple_of(owner * group, group), group)
        ss, rs = (s_up, r_up) if going_up else (s_down, r_down)
        return remote(
            wall.at[rows, :], wall.at[rows, :], ss.at[step], rs.at[step],
            sp=up if going_up else down,
        )

    ups, downs = side // 2, side // 2 - 1

    def relay(step):
        if 0 < step <= ups:
            ring(step - 1, True).wait_recv()
        if step < ups:
            ring(step, True).start()
        if 0 < step <= downs:
            ring(step - 1, False).wait_recv()
        if step < downs:
            ring(step, False).start()

    clear_halo(y, ks, vs)
    spread_bias(diag_ref, band, x)
    for kind in (0, 1, 2):
        take(kind)
    relay(0)
    for kind in (3, 4):
        take(kind)

    late = pl.ds(REACH + side * tok - REACH, REACH)
    halo = [
        remote(a.at[late, :], a.at[pl.ds(0, REACH), :], s_halo.at[i], r_halo.at[i], sp=up)
        for i, a in enumerate((ks, vs))
    ]

    @pl.when(y < side - 1)
    def _():
        for copy in halo:
            copy.start()

    relay(1)
    take(5)

    def halo_wait():
        relay(2)

        @pl.when(y > 0)
        def _():
            for copy in halo:
                copy.wait_recv()

    attend_rows(side, x, y, qs, ks, vs, band, outs, mixed, s_back, r_back, halo_wait)
    for step in range(3, ups + 1):
        relay(step)
    mixed_ref[...] = mixed[...]
    wall_ref[...] = wall[...]

    for kind in range(6):
        for d in range(1, side):
            pieces[kind][d].wait_send()
    for step in range(ups):
        ring(step, True).wait_send()
    for step in range(downs):
        ring(step, False).wait_send()

    @pl.when(y < side - 1)
    def _():
        for copy in halo:
            copy.wait_send()


def project(mixed_ref, w_any, wbuf, wsem, part, cuts):
    n = w_any.shape[0] // cuts
    loads = [
        pltpu.make_async_copy(
            w_any.at[pl.ds(i * n, n), :], wbuf.at[pl.ds(i * n, n), :], wsem.at[i]
        )
        for i in range(cuts)
    ]
    for load in loads:
        load.start()

    def piece(i):
        loads[i].wait()
        done = lax.dot_general(
            mixed_ref[...], wbuf[pl.ds(i * n, n), :], NT, preferred_element_type=F32
        )
        part[:, pl.ds(i * n, n)] = done.astype(BF)

    return piece, n


CUTS = 4


def second_kernel(
    side, mixed_ref, w_any, resid_any, post_ref, pre_ref, wall_ref, diag_ref, out_ref, hid_ref,
    wbuf, part, theirs, resid, inp, qs, ks, vs, outs, mixed, band, wsem, rsem,
    s_part, r_part, s_right, r_right, s_left, r_left, s_d2d, r_d2d, s_halo, r_halo,
    s_back, r_back, s_hid, r_hid, hid,
):
    x, y, c = place(side)
    tok = mixed_ref.shape[0]
    head = qs.shape[1]
    half = tok // 2
    chunk = half // 2
    other = 1 - c
    load_resid = pltpu.make_async_copy(
        resid_any.at[pl.ds(pl.multiple_of(c * half, half), half), :], resid, rsem.at[0]
    )
    piece, n = project(mixed_ref, w_any, wbuf, wsem, part, CUTS)
    load_resid.start()
    greet(side, x, y, True, True)

    swaps = [
        remote(
            part.at[pl.ds(pl.multiple_of(other * half, half), half), pl.ds(i * n, n)],
            theirs.at[:, pl.ds(i * n, n)],
            s_part.at[i],
            r_part.at[i],
            tp=other,
        )
        for i in range(CUTS)
    ]
    for i in range(CUTS):
        piece(i)
        swaps[i].start()
    clear_halo(y, ks, vs)
    spread_bias(diag_ref, band, x)
    load_resid.wait()
    for copy in swaps:
        copy.wait_recv()

    def rows_of(owner, core, r):
        return pl.ds(pl.multiple_of(owner * tok + core * half + r * chunk, chunk), chunk)

    right = y * side + lax.rem(x + 1, side)
    left = y * side + lax.rem(x + side - 1, side)

    def owner_right(step):
        return lax.rem(x - step + side, side)

    def owner_left(step):
        return lax.rem(x + step, side)

    def pass_right(step, r):
        rows = rows_of(owner_right(step), c, r)
        return remote(
            inp.at[rows, :], inp.at[rows, :], s_right.at[step, r], r_right.at[step, r], sp=right
        )

    def pass_left(step, r):
        rows = rows_of(owner_left(step), c, r)
        return remote(
            inp.at[rows, :], inp.at[rows, :], s_left.at[step, r], r_left.at[step, r], sp=left
        )

    def share(owner, slot, r, core):
        rows = rows_of(owner, core, r)
        return remote(
            inp.at[rows, :], inp.at[rows, :], s_d2d.at[slot, r], r_d2d.at[slot, r], tp=other
        )

    def send_hid(r):
        rows = pl.ds(pl.multiple_of(c * half + r * chunk, chunk), chunk)
        return remote(hid.at[rows, :], hid.at[rows, :], s_hid.at[r], r_hid.at[r], tp=other)

    last = side // 2 - 1
    for r in range(2):
        rows = pl.ds(pl.multiple_of(c * half + r * chunk, chunk), chunk)
        sub = pl.ds(r * chunk, chunk)
        branch = part[rows, :].astype(F32) + theirs[sub, :].astype(F32)
        branch = branch.astype(BF).astype(F32)
        scale = lax.rsqrt(jnp.mean(branch * branch, axis=-1, keepdims=True) + EPS)
        hidden = (resid[sub, :].astype(F32) + branch * scale * post_ref[...]).astype(BF)
        hid[rows, :] = hidden
        wide = hidden.astype(F32)
        scale = lax.rsqrt(jnp.mean(wide * wide, axis=-1, keepdims=True) + EPS)
        inp[rows_of(x, c, r), :] = (wide * scale * pre_ref[...]).astype(BF)
        pass_right(0, r).start()
        pass_left(0, r).start()
        share(x, 0, r, c).start()
        send_hid(r).start()

    up = lax.rem(y + 1, side) * side + x
    shift = REACH // tok

    def halo(owner):
        slot = owner - (side - shift)
        rows = pl.ds(pl.multiple_of(REACH + owner * tok, tok), tok)
        dest = pl.ds(pl.multiple_of(slot * tok, tok), tok)
        return [
            remote(a.at[rows, :], a.at[dest, :], s_halo.at[i, slot], r_halo.at[i, slot], sp=up)
            for i, a in enumerate((ks, vs))
        ]

    def qkv(owner):
        rows = pl.ds(pl.multiple_of(owner * tok, tok), tok)
        late = pl.ds(pl.multiple_of(REACH + owner * tok, tok), tok)
        done = jnp.dot(inp[rows, :], wall_ref[...], preferred_element_type=F32).astype(BF)
        qs[rows, :] = done[:, :head]
        ks[late, :] = done[:, head : 2 * head]
        vs[late, :] = done[:, 2 * head :]

        @pl.when(jnp.logical_and(owner >= side - shift, y < side - 1))
        def _():
            for copy in halo(owner):
                copy.start()

    for r in range(2):
        share(x, 0, r, other).wait_recv()
    qkv(x)
    for step in range(1, last + 1):
        for r in range(2):
            rows = rows_of(owner_right(step), c, r)
            remote(
                inp.at[rows, :], inp.at[rows, :], s_right.at[step - 1, r],
                r_right.at[step - 1, r], sp=right,
            ).wait_recv()
            if not (step == last and r == 1):
                pass_right(step, r).start()
            share(owner_right(step), step, r, c).start()
            rows = rows_of(owner_left(step), c, r)
            remote(
                inp.at[rows, :], inp.at[rows, :], s_left.at[step - 1, r],
                r_left.at[step - 1, r], sp=left,
            ).wait_recv()
            if not (step == last and r == 0):
                pass_left(step, r).start()
            share(owner_left(step), last + 1 + step, r, c).start()
        for r in range(2):
            share(owner_right(step), step, r, other).wait_recv()
        qkv(owner_right(step))
        for r in range(2):
            share(owner_left(step), last + 1 + step, r, other).wait_recv()
        qkv(owner_left(step))
    far = lax.rem(x + side // 2, side)
    step = last + 1
    rows = rows_of(far, c, 0)
    remote(
        inp.at[rows, :], inp.at[rows, :], s_right.at[last, 0], r_right.at[last, 0], sp=right
    ).wait_recv()
    share(far, step, 0, c).start()
    rows = rows_of(far, c, 1)
    remote(
        inp.at[rows, :], inp.at[rows, :], s_left.at[last, 1], r_left.at[last, 1], sp=left
    ).wait_recv()
    share(far, step, 1, c).start()
    for r in range(2):
        share(far, step, r, other).wait_recv()
    qkv(far)

    def halo_wait():
        @pl.when(y > 0)
        def _():
            for k in range(shift):
                for copy in halo(side - shift + k):
                    copy.wait_recv()

    attend_rows(side, x, y, qs, ks, vs, band, outs, mixed, s_back, r_back, halo_wait)
    out_ref[...] = mixed[...]
    for r in range(2):
        rows = pl.ds(pl.multiple_of(other * half + r * chunk, chunk), chunk)
        remote(hid.at[rows, :], hid.at[rows, :], s_hid.at[r], r_hid.at[r], tp=other).wait_recv()
    hid_ref[...] = hid[...]

    for copy in swaps:
        copy.wait_send()
    for step in range(last + 1):
        for r in range(2):
            if not (step == last and r == 1):
                pass_right(step, r).wait_send()
            if not (step == last and r == 0):
                pass_left(step, r).wait_send()
    for r in range(2):
        send_hid(r).wait_send()
        share(x, 0, r, c).wait_send()
        share(far, last + 1, r, c).wait_send()
        for step in range(1, last + 1):
            share(owner_right(step), step, r, c).wait_send()
            share(owner_left(step), last + 1 + step, r, c).wait_send()

    @pl.when(y < side - 1)
    def _():
        for k in range(shift):
            for copy in halo(side - shift + k):
                copy.wait_send()


def third_kernel(
    side, mixed_ref, w_any, hid_ref, post_ref, out_ref, wbuf, part, theirs, wsem, s_part, r_part
):
    x, y, c = place(side)
    piece, n = project(mixed_ref, w_any, wbuf, wsem, part, CUTS)
    greet(side, x, y, False, True)
    swaps = [
        remote(
            part.at[:, pl.ds(i * n, n)],
            theirs.at[:, pl.ds(i * n, n)],
            s_part.at[i],
            r_part.at[i],
            tp=1 - c,
        )
        for i in range(CUTS)
    ]
    for i in range(CUTS):
        piece(i)
        swaps[i].start()
    for copy in swaps:
        copy.wait_recv()
    rows = 32
    for r in range(part.shape[0] // rows):
        sub = pl.ds(r * rows, rows)
        branch = part[sub, :].astype(F32) + theirs[sub, :].astype(F32)
        branch = branch.astype(BF).astype(F32)
        scale = lax.rsqrt(jnp.mean(branch * branch, axis=-1, keepdims=True) + EPS)
        out_ref[sub, :] = (hid_ref[sub, :].astype(F32) + branch * scale * post_ref[...]).astype(BF)
    for copy in swaps:
        copy.wait_send()


def diagonals(table, tok):
    window = tok + REACH
    far = table[:, 2 * REL_CLIP :]
    heads = table.shape[0]
    before = jnp.broadcast_to(far, (heads, REACH - REL_CLIP))
    near = table[:, :0:-1]
    after = jnp.broadcast_to(far, (heads, window + tok - REACH - REL_CLIP))
    return jnp.concatenate([before, near, after], axis=1)


def shards(
    side, resid, queries_first, keys_first, values_first, rel_first, post_first, out_first,
    pre_second, query_weight, key_weight, value_weight, rel_second, post_second, out_second,
):
    tok, width = queries_first.shape
    model = resid.shape[1]
    heads = rel_first.shape[0]
    head = width // heads
    rows = side * tok
    dma = pltpu.SemaphoreType.DMA
    params = functools.partial(pltpu.CompilerParams, has_side_effects=True)

    def shape(*dims):
        return jax.ShapeDtypeStruct(dims, BF)

    def vmem(*dims):
        return pltpu.VMEM(dims, BF)

    w_first = lax.all_gather(out_first.T, "sp", axis=0, tiled=True)
    w_second = lax.all_gather(out_second.T, "sp", axis=0, tiled=True)
    attention = [
        vmem(rows, head),
        vmem(rows + REACH, head),
        vmem(rows + REACH, head),
        vmem(rows, head),
        vmem(tok, width),
    ]
    band = pltpu.VMEM((tok, tok + REACH), F32)
    steps = side // 2
    mixed, wall = pl.pallas_call(
        functools.partial(first_kernel, side),
        out_shape=(shape(tok, width), shape(model, 3 * head)),
        in_specs=[ANY] * 3 + [VM] + [ANY] * 3,
        out_specs=(VM, VM),
        scratch_shapes=attention
        + [vmem(model, 3 * head), band]
        + [dma((6, side))] * 2
        + [dma((steps,))] * 4
        + [dma((2,))] * 2
        + [dma((side,))] * 2,
        compiler_params=params(collective_id=0),
        cost_estimate=pl.CostEstimate(
            flops=20_000_000_000, bytes_accessed=4_000_000, transcendentals=0
        ),
    )(
        queries_first,
        keys_first,
        values_first,
        diagonals(rel_first, tok),
        query_weight,
        key_weight,
        value_weight,
    )
    mixed, hidden = pl.pallas_call(
        functools.partial(second_kernel, side),
        out_shape=(shape(tok, width), shape(tok, model)),
        in_specs=[VM, ANY, ANY, VM, VM, VM, VM],
        out_specs=(VM, VM),
        scratch_shapes=[
            vmem(model, width),
            vmem(tok, model),
            vmem(tok // 2, model),
            vmem(tok // 2, model),
            vmem(rows, model),
        ]
        + attention
        + [band]
        + [dma((CUTS,)), dma((1,))]
        + [dma((CUTS,))] * 2
        + [dma((steps, 2))] * 4
        + [dma((side, 2))] * 2
        + [dma((2, REACH // tok))] * 2
        + [dma((side,))] * 2
        + [dma((2,))] * 2
        + [vmem(tok, model)],
        compiler_params=params(collective_id=1),
        cost_estimate=pl.CostEstimate(
            flops=30_000_000_000, bytes_accessed=8_000_000, transcendentals=0
        ),
    )(
        mixed,
        w_first,
        resid,
        post_first[None],
        pre_second[None],
        wall,
        diagonals(rel_second, tok),
    )
    return pl.pallas_call(
        functools.partial(third_kernel, side),
        out_shape=shape(tok, model),
        in_specs=[VM, ANY, VM, VM],
        out_specs=VM,
        scratch_shapes=[vmem(model, width), vmem(tok, model), vmem(tok, model)]
        + [dma((CUTS,))] * 3,
        compiler_params=params(collective_id=2),
        cost_estimate=pl.CostEstimate(
            flops=5_000_000_000, bytes_accessed=5_000_000, transcendentals=0
        ),
    )(mixed, w_second, hidden, post_second[None])


def solution(mesh):
    side = math.isqrt(mesh.shape["sp"])
    in_specs = (
        P(("grp", "sp"), None),
        P(("grp", "sp"), "tp"),
        P(("grp", "sp"), "tp"),
        P(("grp", "sp"), "tp"),
        P("tp", None),
        P(),
        P("tp", "sp"),
        P(),
        P("sp", "tp"),
        P("sp", "tp"),
        P("sp", "tp"),
        P("tp", None),
        P(),
        P("tp", "sp"),
    )
    out_specs = P(("grp", "sp"), None)
    return jax.shard_map(
        functools.partial(shards, side),
        mesh=mesh,
        in_specs=in_specs,
        out_specs=out_specs,
        check_vma=False,
    )
```

```python
import functools
import math

import jax
import jax.numpy as jnp
from jax import lax
from jax.experimental import pallas as pl
from jax.experimental.pallas import tpu as pltpu
from jax.sharding import PartitionSpec as P

SEG = 64
LEFT = 8
REACH = 512
REL_CLIP = 128
EPS = 1e-06
NEG_FILL = -1e30
LOG2E = 1.4426950408889634
BF = jnp.bfloat16
F32 = jnp.float32
MESH = pl.DeviceIdType.MESH
VM = pl.BlockSpec(memory_space=pltpu.VMEM)
ANY = pl.BlockSpec(memory_space=pl.ANY)
NT = (((1,), (1,)), ((), ()))


def place(side):
    sp = lax.axis_index("sp")
    return lax.rem(sp, side), lax.div(sp, side), lax.axis_index("tp")


def remote(src, dst, send, recv, **where):
    return pltpu.make_async_remote_copy(
        src_ref=src,
        dst_ref=dst,
        send_sem=send,
        recv_sem=recv,
        device_id=dict(where),
        device_id_type=MESH,
    )


def greet(side, x, y, c, grp):
    barrier = pltpu.get_barrier_semaphore()
    peers = [{"sp": y * side + lax.rem(x + d, side)} for d in range(1, side)]
    peers += [{"sp": lax.rem(y + d, side) * side + x} for d in (1, side - 1)]
    peers += [{"tp": 1 - c}, {"grp": other_plane(grp)}]
    for peer in peers:
        pl.semaphore_signal(barrier, inc=1, device_id=peer, device_id_type=MESH)
    return lambda: pl.semaphore_wait(barrier, len(peers))


def other_plane(grp):
    return grp + 1 - 2 * lax.rem(grp, 2)


def spread_bias(table_ref, band_ref, x):
    tok, window = band_ref.shape
    length = window + tok
    near = table_ref[:, : 2 * REL_CLIP]
    far = table_ref[:, 2 * REL_CLIP :]
    end = REACH + REL_CLIP
    slot = end - lax.broadcasted_iota(jnp.int32, (2 * REL_CLIP, length), 1)
    pick = slot == lax.broadcasted_iota(jnp.int32, (2 * REL_CLIP, length), 0)
    lines = jnp.dot(
        near, pick.astype(F32), preferred_element_type=F32, precision=lax.Precision.HIGHEST
    )
    where = lax.broadcasted_iota(jnp.int32, lines.shape, 1)
    lines = jnp.where((where > end - 2 * REL_CLIP) & (where < end), lines, far)
    chosen = lax.broadcasted_iota(jnp.int32, lines.shape, 0) == x
    line = jnp.sum(jnp.where(chosen, lines, 0.0), axis=0, keepdims=True)
    wide = jnp.broadcast_to(line, (tok, length))
    wide = pltpu.roll(wide, 0, 1, stride=1, stride_axis=0)[:, :window] * LOG2E
    qseg = lax.broadcasted_iota(jnp.int32, (tok, window), 0) // SEG
    kseg = lax.broadcasted_iota(jnp.int32, (tok, window), 1) // SEG
    band_ref[...] = jnp.where((kseg >= qseg) & (kseg <= qseg + LEFT), wide, NEG_FILL)


def attend(block, first_row, qs, ks, vs, band_ref):
    tok, window = band_ref.shape
    head = qs.shape[1]
    at = pl.multiple_of(block * tok, tok)
    query = qs[pl.ds(at, tok), :]
    keys = ks[pl.ds(at, window), :]
    values = vs[pl.ds(at, window), :]
    scores = lax.dot_general(query, keys, NT, preferred_element_type=F32)
    scores = scores * (head**-0.5 * LOG2E) + band_ref[...]
    if first_row is not None:
        column = lax.broadcasted_iota(jnp.int32, (1, window), 1) + block * tok
        hidden = jnp.logical_and(column < REACH, first_row)
        scores = scores + jnp.where(hidden, NEG_FILL, 0.0)
    largest = jnp.max(scores, axis=-1, keepdims=True)
    weights = jnp.exp2(scores - largest)
    total = jnp.sum(weights, axis=-1, keepdims=True)
    mixed = jnp.dot(weights.astype(BF), values, preferred_element_type=F32)
    return (mixed / total).astype(BF)


def attend_rows(side, x, y, qs, ks, vs, band, outs, mixed, ssem, rsem, between):
    tok, head = band.shape[0], qs.shape[1]
    here = pl.ds(pl.multiple_of(x * head, head), head)

    def hand_back(block):
        rows = pl.ds(pl.multiple_of(block * tok, tok), tok)
        return remote(
            outs.at[rows, :], mixed.at[:, here], ssem.at[block], rsem.at[x], sp=y * side + block
        )

    def run(block, first_row):
        result = attend(block, first_row, qs, ks, vs, band)
        outs[pl.ds(pl.multiple_of(block * tok, tok), tok), :] = result

        @pl.when(block != x)
        def _():
            hand_back(block).start()

        @pl.when(block == x)
        def _():
            mixed[:, here] = result

    half = REACH // tok

    def late(i, carry):
        run(i + half, None)
        return carry

    lax.fori_loop(0, side - half, late, 0)
    between()

    def early(i, carry):
        run(i, y == 0)
        return carry

    lax.fori_loop(0, half, early, 0)

    def take_back():
        def finish(block, carry):
            @pl.when(block != x)
            def _():
                there = pl.ds(pl.multiple_of(block * head, head), head)
                remote(
                    outs.at[pl.ds(0, tok), :],
                    mixed.at[:, there],
                    ssem.at[block],
                    rsem.at[block],
                    sp=y * side + block,
                ).wait_recv()

            return carry

        lax.fori_loop(0, side, finish, 0)

    def sent():
        def finish(block, carry):
            @pl.when(block != x)
            def _():
                hand_back(block).wait_send()

            return carry

        lax.fori_loop(0, side, finish, 0)

    return take_back, sent


def clear_halo(y, ks, vs):
    @pl.when(y == 0)
    def _():
        ks[pl.ds(0, REACH), :] = jnp.zeros((REACH, ks.shape[1]), BF)
        vs[pl.ds(0, REACH), :] = jnp.zeros((REACH, vs.shape[1]), BF)


class Gather:
    def __init__(self, side, x, y, grp, buf, xr, xl, yu, yd, z):
        self.side, self.x, self.y, self.grp, self.buf = side, x, y, grp, buf
        self.xr, self.xl, self.yu, self.yd, self.z = xr, xl, yu, yd, z
        self.rows = buf.shape[0] // (side * side)
        quarter = buf.shape[1] // 4
        parity = lax.rem(grp, 2)
        self.inside = pl.ds(pl.multiple_of(parity * quarter, quarter), 3 * quarter)
        self.across = pl.ds(pl.multiple_of(parity * 3 * quarter, quarter), quarter)
        self.theirs = pl.ds(pl.multiple_of((1 - parity) * 3 * quarter, quarter), quarter)

    def slab(self, xp, yp, columns):
        at = pl.multiple_of((yp * self.side + xp) * self.rows, self.rows)
        return self.buf.at[pl.ds(at, self.rows), columns]

    def column(self, k):
        if isinstance(k, int):
            off = -(k + 1) // 2 if k % 2 else k // 2
        else:
            off = jnp.where(lax.rem(k, 2) == 1, -lax.div(k + 1, 2), lax.div(k, 2))
        return lax.rem(self.x + off + self.side, self.side)

    def xcopy(self, step, right):
        owner = lax.rem(self.x + (-step if right else step) + self.side, self.side)
        to = lax.rem(self.x + (1 if right else self.side - 1), self.side)
        part = self.slab(owner, self.y, self.inside)
        send, recv = self.xr if right else self.xl
        return remote(part, part, send.at[step], recv.at[step], sp=self.y * self.side + to)

    def xarrival(self, step, right):
        owner = lax.rem(self.x + (-step - 1 if right else step + 1) + self.side, self.side)
        part = self.slab(owner, self.y, self.inside)
        send, recv = self.xr if right else self.xl
        return remote(part, part, send.at[step], recv.at[step], sp=self.y * self.side + self.x)

    def ycopy(self, step, k, upward):
        owner = lax.rem(self.y + (-step if upward else step) + self.side, self.side)
        to = lax.rem(self.y + (1 if upward else self.side - 1), self.side)
        part = self.slab(self.column(k), owner, self.inside)
        send, recv = self.yu if upward else self.yd
        return remote(part, part, send.at[step, k], recv.at[step, k], sp=to * self.side + self.x)

    def yarrival(self, step, k, upward):
        owner = lax.rem(self.y + (-step - 1 if upward else step + 1) + self.side, self.side)
        part = self.slab(self.column(k), owner, self.inside)
        send, recv = self.yu if upward else self.yd
        return remote(part, part, send.at[step, k], recv.at[step, k], sp=self.x)

    def zcopy(self, t, k, columns):
        owner = lax.rem(self.y - t + self.side, self.side)
        part = self.slab(self.column(k), owner, columns)
        send, recv = self.z
        return remote(part, part, send.at[t, k], recv.at[t, k], grp=other_plane(self.grp))

    def begin(self):
        self.xcopy(0, True).start()
        self.xcopy(0, False).start()
        self.ycopy(0, 0, True).start()
        self.ycopy(0, 0, False).start()

    def xevent(self, k):
        right = k % 2 == 1
        step = (k + 1) // 2 if right else k // 2
        self.xarrival(step - 1, right).wait_recv()
        if step < self.side // 2 - (0 if right else 1):
            self.xcopy(step, right).start()
        self.ycopy(0, k, True).start()
        self.ycopy(0, k, False).start()
        self.zcopy(0, k, self.across).start()

    def yevent(self, step, lower):
        side = self.side
        half = side // 2
        far = step == half
        base = 0 if lower else half

        def one(k, carry):
            if not far or lower:
                self.yarrival(step - 1, k, True).wait_recv()
                if step < half - 1 or (step == half - 1 and lower):
                    self.ycopy(step, k, True).start()
                self.zcopy(step, k, self.across).start()
            if not far or not lower:
                self.yarrival(step - 1, k, False).wait_recv()
                if step < half - 1 or (step == half - 1 and not lower):
                    self.ycopy(step, k, False).start()
                self.zcopy(side - step, k, self.across).start()
            return carry

        lax.fori_loop(base, base + half, one, 0)

    def zevent(self):
        side = self.side

        def one(i, carry):
            t, k = lax.div(i, side), lax.rem(i, side)
            self.zcopy(t, k, self.theirs).wait_recv()
            return carry

        lax.fori_loop(1, side * side, one, 0)

    def sent(self):
        side = self.side
        half = side // 2
        for step in range(half):
            self.xcopy(step, True).wait_send()
            if step < half - 1:
                self.xcopy(step, False).wait_send()

            def one(k, carry, step=step):
                if step < half - 1:
                    self.ycopy(step, k, True).wait_send()
                    self.ycopy(step, k + half, True).wait_send()
                    self.ycopy(step, k, False).wait_send()
                else:
                    self.ycopy(step, k, True).wait_send()
                self.ycopy(step, k + half, False).wait_send()
                return carry

            lax.fori_loop(0, half, one, 0)

        def one(i, carry):
            self.zcopy(lax.div(i, side), lax.rem(i, side), self.across).wait_send()
            return carry

        lax.fori_loop(1, side * side, one, 0)


CUTS = 4


def layers_kernel(side, names, *refs):
    r = dict(zip(names, refs))
    x, y, c = place(side)
    grp = lax.axis_index("grp")
    plane = lax.rem(grp, 2)
    q_ref, k_ref, v_ref = r["q"], r["k"], r["v"]
    tok, width = q_ref.shape
    head = width // side
    wall = r["wall"]
    wrow = r["wq"].shape[0]
    group = side * wrow
    model = r["w1"].shape[0]
    other = 1 - c
    half = tok // 2
    steps = side // 2
    up = lax.rem(y + 1, side) * side + x
    down = lax.rem(y + side - 1, side) * side + x
    right = y * side + lax.rem(x + 1, side)
    left = y * side + lax.rem(x + side - 1, side)

    meet = greet(side, x, y, c, grp)
    own = pl.ds(pl.multiple_of((y * side + x) * wrow, wrow), wrow)
    loads = [
        pltpu.make_async_copy(r["o1"], r["w1"].at[own, :], r["loads"].at[0]),
        pltpu.make_async_copy(r["o2"], r["w2"].at[own, :], r["loads"].at[1]),
        pltpu.make_async_copy(
            r["resid_any"].at[pl.ds(pl.multiple_of(c * half, half), half), :],
            r["resid"],
            r["loads"].at[2],
        ),
    ]
    for load in loads:
        load.start()
    g1, g2 = [
        Gather(
            side, x, y, grp, r[f"w{i}"],
            *((r[f"s{kind}{i}"], r[f"r{kind}{i}"]) for kind in ("xr", "xl", "yu", "yd", "z")),
        )
        for i in (1, 2)
    ]

    mine = pl.ds(pl.multiple_of(x * tok, tok), tok)
    mine_late = pl.ds(pl.multiple_of(REACH + x * tok, tok), tok)
    kinds = [
        (k_ref, r["ks1"].at[mine_late, :]),
        (v_ref, r["vs1"].at[mine_late, :]),
        (q_ref, r["qs1"].at[mine, :]),
    ] + [(r[f"w{n}"], wall.at[own, pl.ds(i * head, head)]) for i, n in enumerate("qkv")]

    def piece(kind, d):
        peer = lax.rem(x + d, side)
        src, dst = kinds[kind]
        cut = src.at[:, pl.ds(pl.multiple_of(peer * head, head), head)]
        if d == 0:
            return pltpu.make_async_copy(cut, dst, r["ra2a"].at[kind, 0])
        send, recv = r["sa2a"].at[kind, d], r["ra2a"].at[kind, d]
        return remote(cut, dst, send, recv, sp=y * side + peer)

    for kind in range(3):
        piece(kind, 0).start()
    in_plane = lax.div(x, steps) == plane

    @pl.when(in_plane)
    def _():
        for kind in range(3, 6):
            piece(kind, 0).start()

    spread_bias(r["rel1"], r["band1"], x)
    spread_bias(r["rel2"], r["band2"], x)
    clear_halo(y, r["ks1"], r["vs1"])
    clear_halo(y, r["ks2"], r["vs2"])
    for load in loads:
        load.wait()
    meet()

    g1.begin()
    near, wide = [1, side - 1, 2, side - 2], [3, side - 3, 4]
    for d in near:
        piece(0, d).start()
        piece(1, d).start()
    g1.xevent(1)
    g1.xevent(2)
    for d in wide:
        piece(0, d).start()
        piece(1, d).start()
    g1.xevent(3)
    g1.xevent(4)
    for d in near:
        piece(2, d).start()
    g1.xevent(5)
    g1.xevent(6)
    for d in wide:
        piece(2, d).start()

    @pl.when(in_plane)
    def _():
        for kind in range(3, 6):
            for d in range(1, side):
                piece(kind, d).start()

    g1.xevent(7)

    def take(kind):
        piece(kind, 0).wait()
        for d in range(1, side):
            piece(kind, d).wait_recv()

    def ring_rows(owner, parity):
        return pl.ds(pl.multiple_of(owner * group + parity * (group // 2), group // 2), group // 2)

    def ring(step, upward):
        owner = lax.rem(y + (-step if upward else step) + side, side)
        part = wall.at[ring_rows(owner, plane), :]
        send, recv = (r["squ"], r["rqu"]) if upward else (r["sqd"], r["rqd"])
        return remote(part, part, send.at[step], recv.at[step], sp=up if upward else down)

    def cross(t, parity):
        owner = lax.rem(y - t + side, side)
        part = wall.at[ring_rows(owner, parity), :]
        return remote(part, part, r["sqz"].at[t], r["rqz"].at[t], grp=other_plane(grp))

    def relay(step):
        if step == 0:
            @pl.when(in_plane)
            def _():
                for kind in range(3, 6):
                    piece(kind, 0).wait()

            for d in range(1, side):
                @pl.when(lax.div(lax.rem(x - d + side, side), steps) == plane)
                def _(d=d):
                    for kind in range(3, 6):
                        piece(kind, d).wait_recv()

        if step > 0:
            ring(step - 1, True).wait_recv()
        if step < steps:
            ring(step, True).start()
        cross(step, plane).start()
        if 0 < step < steps:
            ring(step - 1, False).wait_recv()
            cross(side - step, plane).start()
        if step < steps - 1:
            ring(step, False).start()

    take(0)
    take(1)
    halo1 = [
        remote(
            a.at[pl.ds(side * tok, REACH), :], a.at[pl.ds(0, REACH), :],
            r["sh1"].at[i], r["rh1"].at[i], sp=up,
        )
        for i, a in enumerate((r["ks1"], r["vs1"]))
    ]

    @pl.when(y < side - 1)
    def _():
        for copy in halo1:
            copy.start()

    g1.yevent(1, True)
    take(2)
    g1.yevent(1, False)
    relay(0)

    def between():
        g1.yevent(2, True)
        relay(1)

        @pl.when(y > 0)
        def _():
            for copy in halo1:
                copy.wait_recv()

    take_back, back1 = attend_rows(
        side, x, y, r["qs1"], r["ks1"], r["vs1"], r["band1"], r["outs1"], r["mixed1"],
        r["sb1"], r["rb1"], between,
    )
    g1.yevent(2, False)
    relay(2)
    g2.begin()
    take_back()
    g1.yevent(3, True)
    g1.yevent(3, False)
    relay(3)
    g2.xevent(1)
    g2.xevent(2)
    g2.xevent(3)
    g2.xevent(4)
    g1.yevent(4, True)
    g1.yevent(4, False)
    relay(4)
    g1.zevent()

    n = model // CUTS
    part1, theirs1 = r["part1"], r["theirs1"]
    swaps = [
        remote(
            part1.at[pl.ds(pl.multiple_of(other * half, half), half), pl.ds(i * n, n)],
            theirs1.at[:, pl.ds(i * n, n)],
            r["sp1"].at[i],
            r["rp1"].at[i],
            tp=other,
        )
        for i in range(CUTS)
    ]
    for i in range(CUTS):
        done = lax.dot_general(
            r["mixed1"][...], r["w1"][pl.ds(i * n, n), :], NT, preferred_element_type=F32
        )
        part1[:, pl.ds(i * n, n)] = done.astype(BF)
        swaps[i].start()
    g2.xevent(5)
    g2.xevent(6)
    g2.xevent(7)
    for copy in swaps:
        copy.wait_recv()

    inp, hid = r["inp"], r["hid"]
    chunk = half // 2

    def rows_of(owner, core, i):
        return pl.ds(pl.multiple_of(owner * tok + core * half + i * chunk, chunk), chunk)

    def away(step):
        return lax.rem(x + step + side, side)

    def spread(owner, send, recv, **to):
        return lambda step, i: remote(
            inp.at[rows_of(owner(step), c, i), :], inp.at[rows_of(owner(step), c, i), :],
            send.at[step, i], recv.at[step, i], **to,
        )

    pass_right = spread(lambda s: away(-s), r["sr"], r["rr"], sp=right)
    pass_left = spread(lambda s: away(s), r["sl"], r["rl"], sp=left)
    from_left = spread(lambda s: away(-s - 1), r["sr"], r["rr"], sp=right)
    from_right = spread(lambda s: away(s + 1), r["sl"], r["rl"], sp=left)

    def share(offset, i, core):
        rows = rows_of(away(offset), core, i)
        slot = offset % side
        return remote(
            inp.at[rows, :], inp.at[rows, :], r["sd"].at[slot, i], r["rd"].at[slot, i], tp=other
        )

    def show(i, core):
        rows = rows_of(0, core, i)
        return remote(hid.at[rows, :], hid.at[rows, :], r["sw"].at[i], r["rw"].at[i], tp=other)

    for i in range(2):
        rows = rows_of(0, c, i)
        sub = pl.ds(i * chunk, chunk)
        branch = part1[rows, :].astype(F32) + theirs1[sub, :].astype(F32)
        branch = branch.astype(BF).astype(F32)
        scale = lax.rsqrt(jnp.mean(branch * branch, axis=-1, keepdims=True) + EPS)
        hidden = (r["resid"][sub, :].astype(F32) + branch * scale * r["post1"][...]).astype(BF)
        hid[rows, :] = hidden
        long = hidden.astype(F32)
        scale = lax.rsqrt(jnp.mean(long * long, axis=-1, keepdims=True) + EPS)
        inp[rows_of(x, c, i), :] = (long * scale * r["pre2"][...]).astype(BF)
        pass_right(0, i).start()
        pass_left(0, i).start()
        share(0, i, c).start()
        show(i, c).start()

    shift = REACH // tok
    qs2, ks2, vs2 = r["qs2"], r["ks2"], r["vs2"]

    def halo2(owner):
        slot = owner - (side - shift)
        rows = pl.ds(pl.multiple_of(REACH + owner * tok, tok), tok)
        dest = pl.ds(pl.multiple_of(slot * tok, tok), tok)
        return [
            remote(
                a.at[rows, :], a.at[dest, :], r["sh2"].at[i, slot], r["rh2"].at[i, slot], sp=up
            )
            for i, a in enumerate((ks2, vs2))
        ]

    def qkv(offset):
        for i in range(2):
            share(offset, i, other).wait_recv()
        owner = away(offset)
        rows = pl.ds(pl.multiple_of(owner * tok, tok), tok)
        late = pl.ds(pl.multiple_of(REACH + owner * tok, tok), tok)
        done = jnp.dot(inp[rows, :], wall[...], preferred_element_type=F32).astype(BF)
        qs2[rows, :] = done[:, :head]
        ks2[late, :] = done[:, head : 2 * head]
        vs2[late, :] = done[:, 2 * head :]

        @pl.when(jnp.logical_and(owner >= side - shift, y < side - 1))
        def _():
            for copy in halo2(owner):
                copy.start()

    for t in range(side):
        cross(t, 1 - plane).wait_recv()
    qkv(0)
    last = steps - 1
    for step in range(1, steps):
        for i in range(2):
            from_left(step - 1, i).wait_recv()
            if step < last or i == 0:
                pass_right(step, i).start()
            share(-step, i, c).start()
            from_right(step - 1, i).wait_recv()
            if step < last or i == 1:
                pass_left(step, i).start()
            share(step, i, c).start()
        g2.yevent(step, True)
        qkv(-step)
        g2.yevent(step, False)
        qkv(step)
    from_left(last, 0).wait_recv()
    share(steps, 0, c).start()
    from_right(last, 1).wait_recv()
    share(steps, 1, c).start()
    qkv(steps)

    def between2():
        @pl.when(y > 0)
        def _():
            for k in range(shift):
                for copy in halo2(side - shift + k):
                    copy.wait_recv()

    take_back, back2 = attend_rows(
        side, x, y, qs2, ks2, vs2, r["band2"], r["outs2"], r["mixed2"], r["sb2"], r["rb2"],
        between2,
    )
    g2.yevent(4, True)
    g2.yevent(4, False)
    for i in range(2):
        show(i, other).wait_recv()
    take_back()
    g2.zevent()

    part2, theirs2 = r["part2"], r["theirs2"]
    swaps2 = [
        remote(
            part2.at[:, pl.ds(i * n, n)], theirs2.at[:, pl.ds(i * n, n)],
            r["sp2"].at[i], r["rp2"].at[i], tp=other,
        )
        for i in range(CUTS)
    ]
    for i in range(CUTS):
        done = lax.dot_general(
            r["mixed2"][...], r["w2"][pl.ds(i * n, n), :], NT, preferred_element_type=F32
        )
        part2[:, pl.ds(i * n, n)] = done.astype(BF)
        swaps2[i].start()
    for copy in swaps2:
        copy.wait_recv()
    for i in range(tok // chunk):
        sub = pl.ds(i * chunk, chunk)
        branch = part2[sub, :].astype(F32) + theirs2[sub, :].astype(F32)
        branch = branch.astype(BF).astype(F32)
        scale = lax.rsqrt(jnp.mean(branch * branch, axis=-1, keepdims=True) + EPS)
        done = hid[sub, :].astype(F32) + branch * scale * r["post2"][...]
        r["out"][sub, :] = done.astype(BF)

    for kind in range(3):
        for d in range(1, side):
            piece(kind, d).wait_send()

    @pl.when(in_plane)
    def _():
        for kind in range(3, 6):
            for d in range(1, side):
                piece(kind, d).wait_send()

    for step in range(steps):
        ring(step, True).wait_send()
        if step < last:
            ring(step, False).wait_send()
    for t in range(side):
        cross(t, plane).wait_send()
    g1.sent()
    g2.sent()
    back1()
    back2()
    for copy in swaps + swaps2:
        copy.wait_send()
    for step in range(steps):
        for i in range(2):
            if step < last or i == 0:
                pass_right(step, i).wait_send()
            if step < last or i == 1:
                pass_left(step, i).wait_send()
    for i in range(2):
        show(i, c).wait_send()
        for offset in range(side):
            share(offset, i, c).wait_send()

    @pl.when(y < side - 1)
    def _():
        for copy in halo1:
            copy.wait_send()
        for k in range(shift):
            for copy in halo2(side - shift + k):
                copy.wait_send()


def shards(
    side, resid, queries_first, keys_first, values_first, rel_first, post_first, out_first,
    pre_second, query_weight, key_weight, value_weight, rel_second, post_second, out_second,
):
    tok, width = queries_first.shape
    model = resid.shape[1]
    head = width // rel_first.shape[0]
    rows = side * tok
    steps = side // 2
    inputs = {
        "q": (queries_first, ANY),
        "k": (keys_first, ANY),
        "v": (values_first, ANY),
        "rel1": (rel_first, VM),
        "rel2": (rel_second, VM),
        "o1": (out_first.T, ANY),
        "o2": (out_second.T, ANY),
        "resid_any": (resid, ANY),
        "post1": (post_first[None], VM),
        "pre2": (pre_second[None], VM),
        "post2": (post_second[None], VM),
        "wq": (query_weight, ANY),
        "wk": (key_weight, ANY),
        "wv": (value_weight, ANY),
    }

    def vmem(*dims):
        return pltpu.VMEM(dims, BF)

    def dma(*dims):
        return pltpu.SemaphoreType.DMA(dims)

    scratch = {
        "wall": vmem(model, 3 * head),
        "inp": vmem(rows, model),
        "hid": vmem(tok, model),
        "resid": vmem(tok // 2, model),
        "theirs1": vmem(tok // 2, model),
        "theirs2": vmem(tok, model),
        "loads": dma(3),
        "sa2a": dma(6, side),
        "ra2a": dma(6, side),
    }
    for i in (1, 2):
        scratch[f"w{i}"] = vmem(model, width)
        scratch[f"qs{i}"] = vmem(rows, head)
        scratch[f"ks{i}"] = vmem(rows + REACH, head)
        scratch[f"vs{i}"] = vmem(rows + REACH, head)
        scratch[f"outs{i}"] = vmem(rows, head)
        scratch[f"mixed{i}"] = vmem(tok, width)
        scratch[f"part{i}"] = vmem(tok, model)
        scratch[f"band{i}"] = pltpu.VMEM((tok, tok + REACH), F32)
    for d in "sr":
        for i in (1, 2):
            scratch[f"{d}xr{i}"] = dma(steps)
            scratch[f"{d}xl{i}"] = dma(steps)
            scratch[f"{d}yu{i}"] = dma(steps, side)
            scratch[f"{d}yd{i}"] = dma(steps, side)
            scratch[f"{d}z{i}"] = dma(side, side)
            scratch[f"{d}b{i}"] = dma(side)
            scratch[f"{d}p{i}"] = dma(CUTS)
        scratch[f"{d}qu"] = dma(steps)
        scratch[f"{d}qd"] = dma(steps)
        scratch[f"{d}qz"] = dma(side)
        scratch[f"{d}h1"] = dma(2)
        scratch[f"{d}h2"] = dma(2, REACH // tok)
        scratch[f"{d}r"] = dma(steps, 2)
        scratch[f"{d}l"] = dma(steps, 2)
        scratch[f"{d}d"] = dma(side, 2)
        scratch[f"{d}w"] = dma(2)
    return pl.pallas_call(
        functools.partial(layers_kernel, side, [*inputs, "out", *scratch]),
        out_shape=jax.ShapeDtypeStruct((tok, model), BF),
        in_specs=[spec for _, spec in inputs.values()],
        out_specs=VM,
        scratch_shapes=list(scratch.values()),
        compiler_params=pltpu.CompilerParams(has_side_effects=True, collective_id=0),
    )(*(value for value, _ in inputs.values()))


def solution(mesh):
    side = math.isqrt(mesh.shape["sp"])
    in_specs = (
        P(("grp", "sp"), None),
        P(("grp", "sp"), "tp"),
        P(("grp", "sp"), "tp"),
        P(("grp", "sp"), "tp"),
        P("tp", None),
        P(),
        P("tp", "sp"),
        P(),
        P("sp", "tp"),
        P("sp", "tp"),
        P("sp", "tp"),
        P("tp", None),
        P(),
        P("tp", "sp"),
    )
    out_specs = P(("grp", "sp"), None)
    return jax.shard_map(
        functools.partial(shards, side),
        mesh=mesh,
        in_specs=in_specs,
        out_specs=out_specs,
        check_vma=False,
    )
```

```python
import functools
import math

import jax
import jax.numpy as jnp
from jax import lax
from jax.experimental import pallas as pl
from jax.experimental.pallas import tpu as pltpu
from jax.sharding import PartitionSpec as P

SEG = 64
LEFT = 8
REACH = 512
REL_CLIP = 128
EPS = 1e-06
NEG_FILL = -1e30
LOG2E = 1.4426950408889634
BF = jnp.bfloat16
F32 = jnp.float32
MESH = pl.DeviceIdType.MESH
VM = pl.BlockSpec(memory_space=pltpu.VMEM)
ANY = pl.BlockSpec(memory_space=pl.ANY)
NT = (((1,), (1,)), ((), ()))


def place(side):
    sp = lax.axis_index("sp")
    return lax.rem(sp, side), lax.div(sp, side), lax.axis_index("tp")


def remote(src, dst, send, recv, **where):
    return pltpu.make_async_remote_copy(
        src_ref=src,
        dst_ref=dst,
        send_sem=send,
        recv_sem=recv,
        device_id=dict(where),
        device_id_type=MESH,
    )


def greet(side, x, y, c, grp):
    barrier = pltpu.get_barrier_semaphore()
    peers = [{"sp": y * side + lax.rem(x + d, side)} for d in range(1, side)]
    peers += [{"sp": lax.rem(y + d, side) * side + x} for d in (1, side - 1)]
    peers += [{"tp": 1 - c}]
    peers += [{"grp": other_plane(grp)}, {"grp": other_plane(grp), "tp": 1 - c}]
    for peer in peers:
        pl.semaphore_signal(barrier, inc=1, device_id=peer, device_id_type=MESH)
    return lambda: pl.semaphore_wait(barrier, len(peers))


def other_plane(grp):
    return grp + 1 - 2 * lax.rem(grp, 2)


def spread_bias(table_ref, band_ref, x):
    tok, window = band_ref.shape
    length = window + tok
    near = table_ref[:, : 2 * REL_CLIP]
    far = table_ref[:, 2 * REL_CLIP :]
    end = REACH + REL_CLIP
    slot = end - lax.broadcasted_iota(jnp.int32, (2 * REL_CLIP, length), 1)
    pick = slot == lax.broadcasted_iota(jnp.int32, (2 * REL_CLIP, length), 0)
    lines = jnp.dot(
        near, pick.astype(F32), preferred_element_type=F32, precision=lax.Precision.HIGHEST
    )
    where = lax.broadcasted_iota(jnp.int32, lines.shape, 1)
    lines = jnp.where((where > end - 2 * REL_CLIP) & (where < end), lines, far)
    chosen = lax.broadcasted_iota(jnp.int32, lines.shape, 0) == x
    line = jnp.sum(jnp.where(chosen, lines, 0.0), axis=0, keepdims=True)
    wide = jnp.broadcast_to(line, (tok, length))
    wide = pltpu.roll(wide, 0, 1, stride=1, stride_axis=0)[:, :window] * LOG2E
    qseg = lax.broadcasted_iota(jnp.int32, (tok, window), 0) // SEG
    kseg = lax.broadcasted_iota(jnp.int32, (tok, window), 1) // SEG
    band_ref[...] = jnp.where((kseg >= qseg) & (kseg <= qseg + LEFT), wide, NEG_FILL)


def attend(block, first_row, qs, ks, vs, band_ref):
    tok, window = band_ref.shape
    head = qs.shape[1]
    at = pl.multiple_of(block * tok, tok)
    query = qs[pl.ds(at, tok), :]
    keys = ks[pl.ds(at, window), :]
    values = vs[pl.ds(at, window), :]
    scores = lax.dot_general(query, keys, NT, preferred_element_type=F32)
    scores = scores * (head**-0.5 * LOG2E) + band_ref[...]
    if first_row is not None:
        column = lax.broadcasted_iota(jnp.int32, (1, window), 1) + block * tok
        hidden = jnp.logical_and(column < REACH, first_row)
        scores = scores + jnp.where(hidden, NEG_FILL, 0.0)
    largest = jnp.max(scores, axis=-1, keepdims=True)
    weights = jnp.exp2(scores - largest)
    total = jnp.sum(weights, axis=-1, keepdims=True)
    mixed = jnp.dot(weights.astype(BF), values, preferred_element_type=F32)
    return (mixed / total).astype(BF)


def attend_rows(side, x, y, qs, ks, vs, band, outs, mixed, ssem, rsem, between):
    tok, head = band.shape[0], qs.shape[1]
    here = pl.ds(pl.multiple_of(x * head, head), head)

    def hand_back(block):
        rows = pl.ds(pl.multiple_of(block * tok, tok), tok)
        return remote(
            outs.at[rows, :], mixed.at[:, here], ssem.at[block], rsem.at[x], sp=y * side + block
        )

    def run(block, first_row):
        result = attend(block, first_row, qs, ks, vs, band)
        outs[pl.ds(pl.multiple_of(block * tok, tok), tok), :] = result

        @pl.when(block != x)
        def _():
            hand_back(block).start()

        @pl.when(block == x)
        def _():
            mixed[:, here] = result

    half = REACH // tok

    def late(i, carry):
        run(i + half, None)
        return carry

    lax.fori_loop(0, side - half, late, 0)
    between()

    def early(i, carry):
        run(i, y == 0)
        return carry

    lax.fori_loop(0, half, early, 0)

    def take_back(then):
        def finish(block, carry):
            @pl.when(block != x)
            def _():
                there = pl.ds(pl.multiple_of(block * head, head), head)
                remote(
                    outs.at[pl.ds(0, tok), :],
                    mixed.at[:, there],
                    ssem.at[block],
                    rsem.at[block],
                    sp=y * side + block,
                ).wait_recv()
                then(block)

            return carry

        lax.fori_loop(0, side, finish, 0)

    def sent():
        def finish(block, carry):
            @pl.when(block != x)
            def _():
                hand_back(block).wait_send()

            return carry

        lax.fori_loop(0, side, finish, 0)

    return take_back, sent


def clear_halo(y, ks, vs):
    @pl.when(y == 0)
    def _():
        ks[pl.ds(0, REACH), :] = jnp.zeros((REACH, ks.shape[1]), BF)
        vs[pl.ds(0, REACH), :] = jnp.zeros((REACH, vs.shape[1]), BF)


class Gather:
    def __init__(self, side, x, y, grp, buf, shared, xr, xl, yu, yd, z):
        self.side, self.x, self.y, self.grp, self.buf = side, x, y, grp, buf
        self.xr, self.xl, self.yu, self.yd, self.z = xr, xl, yu, yd, z
        self.shared = shared
        self.rows = buf.shape[0] // (side * side)
        quarter = buf.shape[1] // 4
        self.plane = lax.rem(grp, 2)
        self.inside = pl.ds(0, buf.shape[1])
        if not shared:
            self.inside = pl.ds(pl.multiple_of(self.plane * quarter, quarter), 3 * quarter)
        self.across = pl.ds(pl.multiple_of(self.plane * 3 * quarter, quarter), quarter)
        self.theirs = pl.ds(pl.multiple_of((1 - self.plane) * 3 * quarter, quarter), quarter)

    def guard(self, step):
        if self.shared:
            return pl.when(lax.rem(self.y + step, 2) == self.plane)
        return lambda run: run()

    def slab(self, xp, yp, columns):
        at = pl.multiple_of((yp * self.side + xp) * self.rows, self.rows)
        return self.buf.at[pl.ds(at, self.rows), columns]

    def column(self, k):
        if isinstance(k, int):
            off = -(k + 1) // 2 if k % 2 else k // 2
        else:
            off = jnp.where(lax.rem(k, 2) == 1, -lax.div(k + 1, 2), lax.div(k, 2))
        return lax.rem(self.x + off + self.side, self.side)

    def xcopy(self, step, right):
        owner = lax.rem(self.x + (-step if right else step) + self.side, self.side)
        to = lax.rem(self.x + (1 if right else self.side - 1), self.side)
        part = self.slab(owner, self.y, self.inside)
        send, recv = self.xr if right else self.xl
        return remote(part, part, send.at[step], recv.at[step], sp=self.y * self.side + to)

    def xarrival(self, step, right):
        owner = lax.rem(self.x + (-step - 1 if right else step + 1) + self.side, self.side)
        part = self.slab(owner, self.y, self.inside)
        send, recv = self.xr if right else self.xl
        return remote(part, part, send.at[step], recv.at[step], sp=self.y * self.side + self.x)

    def ycopy(self, step, k, upward):
        owner = lax.rem(self.y + (-step if upward else step) + self.side, self.side)
        to = lax.rem(self.y + (1 if upward else self.side - 1), self.side)
        part = self.slab(self.column(k), owner, self.inside)
        send, recv = self.yu if upward else self.yd
        return remote(part, part, send.at[step, k], recv.at[step, k], sp=to * self.side + self.x)

    def yarrival(self, step, k, upward):
        owner = lax.rem(self.y + (-step - 1 if upward else step + 1) + self.side, self.side)
        part = self.slab(self.column(k), owner, self.inside)
        send, recv = self.yu if upward else self.yd
        return remote(part, part, send.at[step, k], recv.at[step, k], sp=self.x)

    def zcopy(self, t, k, columns):
        owner = lax.rem(self.y - t + self.side, self.side)
        part = self.slab(self.column(k), owner, columns)
        send, recv = self.z
        return remote(part, part, send.at[t, k], recv.at[t, k], grp=other_plane(self.grp))

    def begin(self):
        @self.guard(0)
        def _():
            self.xcopy(0, True).start()
            self.xcopy(0, False).start()
            if self.shared:
                self.ycopy(0, 0, True).start()
                self.ycopy(0, 0, False).start()

    def xevent(self, k):
        right = k % 2 == 1
        step = (k + 1) // 2 if right else k // 2

        @self.guard(0)
        def _():
            self.xarrival(step - 1, right).wait_recv()
            if step < self.side // 2 - (0 if right else 1):
                self.xcopy(step, right).start()
            if self.shared:
                self.ycopy(0, k, True).start()
                self.ycopy(0, k, False).start()
            else:
                self.zcopy(0, k, self.across).start()

    def ybegin(self):
        def one(k, carry):
            self.ycopy(0, k, True).start()
            self.ycopy(0, k, False).start()
            return carry

        lax.fori_loop(0, self.side, one, 0)

    def yevent(self, step, base, count):
        side = self.side
        half = side // 2
        far = step == half
        lower = base < half

        def one(k, carry):
            if not far or lower:
                self.yarrival(step - 1, k, True).wait_recv()
                if step < half - 1 or (step == half - 1 and lower):
                    self.ycopy(step, k, True).start()
                if not self.shared:
                    self.zcopy(step, k, self.across).start()
            if not far or not lower:
                self.yarrival(step - 1, k, False).wait_recv()
                if step < half - 1 or (step == half - 1 and not lower):
                    self.ycopy(step, k, False).start()
                if not self.shared:
                    self.zcopy(side - step, k, self.across).start()
            return carry

        @self.guard(step)
        def _():
            lax.fori_loop(base, base + count, one, 0)

    def zevent(self):
        side = self.side

        def one(i, carry):
            t, k = lax.div(i, side), lax.rem(i, side)
            self.zcopy(t, k, self.theirs).wait_recv()
            return carry

        lax.fori_loop(1, side * side, one, 0)

    def sent(self):
        side = self.side
        half = side // 2

        @self.guard(0)
        def _():
            for step in range(half):
                self.xcopy(step, True).wait_send()
                if step < half - 1:
                    self.xcopy(step, False).wait_send()

        for step in range(half):

            def one(k, carry, step=step):
                if step < half - 1:
                    self.ycopy(step, k, True).wait_send()
                    self.ycopy(step, k + half, True).wait_send()
                    self.ycopy(step, k, False).wait_send()
                else:
                    self.ycopy(step, k, True).wait_send()
                self.ycopy(step, k + half, False).wait_send()
                return carry

            @self.guard(step)
            def _(one=one):
                lax.fori_loop(0, half, one, 0)

        def one(i, carry):
            self.zcopy(lax.div(i, side), lax.rem(i, side), self.across).wait_send()
            return carry

        if not self.shared:
            lax.fori_loop(1, side * side, one, 0)


CUTS = 4


def layers_kernel(side, names, *refs):
    r = dict(zip(names, refs))
    x, y, c = place(side)
    grp = lax.axis_index("grp")
    plane = lax.rem(grp, 2)
    q_ref, k_ref, v_ref = r["q"], r["k"], r["v"]
    tok, width = q_ref.shape
    head = width // side
    wall = r["wall"]
    wrow = r["wq"].shape[0]
    group = side * wrow
    model = r["w1"].shape[0]
    other = 1 - c
    half = tok // 2
    steps = side // 2
    up = lax.rem(y + 1, side) * side + x
    down = lax.rem(y + side - 1, side) * side + x
    right = y * side + lax.rem(x + 1, side)
    left = y * side + lax.rem(x + side - 1, side)

    meet = greet(side, x, y, c, grp)
    own = pl.ds(pl.multiple_of((y * side + x) * wrow, wrow), wrow)
    loads = [
        pltpu.make_async_copy(r["o1"], r["w1"].at[own, :], r["loads"].at[0]),
        pltpu.make_async_copy(r["o2"], r["w2"].at[own, :], r["loads"].at[1]),
        pltpu.make_async_copy(
            r["resid_any"].at[pl.ds(pl.multiple_of(c * half, half), half), :],
            r["resid"],
            r["loads"].at[2],
        ),
    ]
    for load in loads:
        load.start()
    g1, g2 = [
        Gather(
            side, x, y, grp, r[f"w{i}"], i == 1,
            *((r[f"s{kind}{i}"], r[f"r{kind}{i}"]) for kind in ("xr", "xl", "yu", "yd", "z")),
        )
        for i in (1, 2)
    ]

    mine = pl.ds(pl.multiple_of(x * tok, tok), tok)
    mine_late = pl.ds(pl.multiple_of(REACH + x * tok, tok), tok)
    kinds = [
        (k_ref, r["ks1"].at[mine_late, :]),
        (v_ref, r["vs1"].at[mine_late, :]),
        (q_ref, r["qs1"].at[mine, :]),
    ] + [(r[f"w{n}"], wall.at[own, pl.ds(i * head, head)]) for i, n in enumerate("qkv")]

    def piece(kind, d):
        peer = lax.rem(x + d, side)
        src, dst = kinds[kind]
        cut = src.at[:, pl.ds(pl.multiple_of(peer * head, head), head)]
        if d == 0:
            return pltpu.make_async_copy(cut, dst, r["ra2a"].at[kind, 0])
        send, recv = r["sa2a"].at[kind, d], r["ra2a"].at[kind, d]
        return remote(cut, dst, send, recv, sp=y * side + peer)

    for kind in range(3):
        piece(kind, 0).start()
    in_plane = lax.div(x, steps) == plane

    @pl.when(in_plane)
    def _():
        for kind in range(3, 6):
            piece(kind, 0).start()

    spread_bias(r["rel1"], r["band1"], x)
    spread_bias(r["rel2"], r["band2"], x)
    clear_halo(y, r["ks1"], r["vs1"])
    clear_halo(y, r["ks2"], r["vs2"])
    for load in loads:
        load.wait()
    meet()

    g1.begin()
    near, wide = [1, side - 1, 2, side - 2], [3, side - 3, 4]
    for d in near:
        piece(0, d).start()
        piece(1, d).start()
    g1.xevent(1)
    g1.xevent(2)
    g1.yevent(1, 0, 2)
    for d in wide:
        piece(0, d).start()
        piece(1, d).start()
    g1.xevent(3)
    g1.xevent(4)
    g1.yevent(1, 2, 2)
    g1.yevent(2, 0, 2)
    for d in near:
        piece(2, d).start()
    g1.xevent(5)
    g1.xevent(6)
    g1.yevent(1, 4, 2)
    g1.yevent(2, 2, 2)
    g1.yevent(3, 0, 2)
    for d in wide:
        piece(2, d).start()

    @pl.when(in_plane)
    def _():
        for kind in range(3, 6):
            for d in range(1, side):
                piece(kind, d).start()

    g1.xevent(7)
    g1.yevent(1, 6, 2)
    g1.yevent(2, 4, 2)
    g1.yevent(3, 2, 2)
    g2.begin()

    def take(kind):
        piece(kind, 0).wait()
        for d in range(1, side):
            piece(kind, d).wait_recv()

    def ring_rows(owner, parity):
        return pl.ds(pl.multiple_of(owner * group + parity * (group // 2), group // 2), group // 2)

    def ring(step, upward):
        owner = lax.rem(y + (-step if upward else step) + side, side)
        part = wall.at[ring_rows(owner, plane), :]
        send, recv = (r["squ"], r["rqu"]) if upward else (r["sqd"], r["rqd"])
        return remote(part, part, send.at[step], recv.at[step], sp=up if upward else down)

    def cross(t, parity):
        owner = lax.rem(y - t + side, side)
        part = wall.at[ring_rows(owner, parity), :]
        return remote(part, part, r["sqz"].at[t], r["rqz"].at[t], grp=other_plane(grp))

    def relay(step):
        if step == 0:
            @pl.when(in_plane)
            def _():
                for kind in range(3, 6):
                    piece(kind, 0).wait()

            for d in range(1, side):
                @pl.when(lax.div(lax.rem(x - d + side, side), steps) == plane)
                def _(d=d):
                    for kind in range(3, 6):
                        piece(kind, d).wait_recv()

        if step > 0:
            ring(step - 1, True).wait_recv()
        if step < steps:
            ring(step, True).start()
        cross(step, plane).start()
        if 0 < step < steps:
            ring(step - 1, False).wait_recv()
            cross(side - step, plane).start()
        if step < steps - 1:
            ring(step, False).start()

    take(0)
    take(1)
    halo1 = [
        remote(
            a.at[pl.ds(side * tok, REACH), :], a.at[pl.ds(0, REACH), :],
            r["sh1"].at[i], r["rh1"].at[i], sp=up,
        )
        for i, a in enumerate((r["ks1"], r["vs1"]))
    ]

    @pl.when(y < side - 1)
    def _():
        for copy in halo1:
            copy.start()

    take(2)
    g1.yevent(2, 6, 2)
    g1.yevent(3, 4, 2)
    relay(0)
    g2.xevent(1)
    g2.xevent(2)

    def between():
        g1.yevent(3, 6, 2)
        g1.yevent(4, 0, 4)
        relay(1)
        @pl.when(y > 0)
        def _():
            for copy in halo1:
                copy.wait_recv()


    take_back, back1 = attend_rows(
        side, x, y, r["qs1"], r["ks1"], r["vs1"], r["band1"], r["outs1"], r["mixed1"],
        r["sb1"], r["rb1"], between,
    )
    g1.yevent(4, 4, 4)
    relay(2)
    g2.xevent(3)
    g2.xevent(4)
    mixed1, mixedz = r["mixed1"], r["mixedz"]

    def lend(block):
        there = pl.ds(pl.multiple_of(block * head, head), head)
        return remote(
            mixed1.at[:, there], mixedz.at[:, there], r["smz"].at[block], r["rmz"].at[block],
            grp=other_plane(grp),
        )

    lend(x).start()
    take_back(lambda block: lend(block).start())
    relay(3)
    g2.xevent(5)
    g2.xevent(6)

    n = group
    part1, partz, terms = r["part1"], r["partz"], r["terms1"]
    my_half = pl.ds(pl.multiple_of(c * half, half), half)
    their_half = pl.ds(pl.multiple_of(other * half, half), half)

    def columns(j):
        return pl.ds(pl.multiple_of((2 * j + plane) * n, n), n)

    swaps, same, diagonal = [], [], []
    for j in range(steps):
        at, lent = columns(j), (r["srz"], r["rrz"])
        swaps.append(
            remote(
                part1.at[their_half, at], terms.at[1, :, at], r["sp1"].at[j], r["rp1"].at[j],
                tp=other,
            )
        )
        same.append(
            remote(
                partz.at[my_half, at], terms.at[0, :, at], lent[0].at[0, j], lent[1].at[0, j],
                grp=other_plane(grp),
            )
        )
        diagonal.append(
            remote(
                partz.at[their_half, at], terms.at[1, :, at], lent[0].at[1, j], lent[1].at[1, j],
                grp=other_plane(grp), tp=other,
            )
        )

    def out1(rows, j):
        return lax.dot_general(
            rows[...], r["w1"][columns(j), :], NT, preferred_element_type=F32
        ).astype(BF)

    for j in range(steps):
        part1[:, columns(j)] = out1(mixed1, j)
        swaps[j].start()
        terms[0, :, columns(j)] = part1[my_half, columns(j)]
    for block in range(side):
        lend(block).wait_recv()
    for j in range(steps):
        partz[:, columns(j)] = out1(mixedz, j)
        same[j].start()
        diagonal[j].start()
    relay(4)
    g2.xevent(7)
    g2.ybegin()
    for copy in swaps + same + diagonal:
        copy.wait_recv()

    inp, hid = r["inp"], r["hid"]
    chunk = half // 2

    def rows_of(owner, core, i):
        return pl.ds(pl.multiple_of(owner * tok + core * half + i * chunk, chunk), chunk)

    def away(step):
        return lax.rem(x + step + side, side)

    def spread(owner, send, recv, **to):
        return lambda step, i: remote(
            inp.at[rows_of(owner(step), c, i), :], inp.at[rows_of(owner(step), c, i), :],
            send.at[step, i], recv.at[step, i], **to,
        )

    pass_right = spread(lambda s: away(-s), r["sr"], r["rr"], sp=right)
    pass_left = spread(lambda s: away(s), r["sl"], r["rl"], sp=left)
    from_left = spread(lambda s: away(-s - 1), r["sr"], r["rr"], sp=right)
    from_right = spread(lambda s: away(s + 1), r["sl"], r["rl"], sp=left)

    def share(offset, i, core):
        rows = rows_of(away(offset), core, i)
        slot = offset % side
        return remote(
            inp.at[rows, :], inp.at[rows, :], r["sd"].at[slot, i], r["rd"].at[slot, i], tp=other
        )

    def show(i, core):
        rows = rows_of(0, core, i)
        return remote(hid.at[rows, :], hid.at[rows, :], r["sw"].at[i], r["rw"].at[i], tp=other)

    for i in range(2):
        rows = rows_of(0, c, i)
        sub = pl.ds(i * chunk, chunk)
        branch = terms[0, sub, :].astype(F32) + terms[1, sub, :].astype(F32)
        branch = branch.astype(BF).astype(F32)
        scale = lax.rsqrt(jnp.mean(branch * branch, axis=-1, keepdims=True) + EPS)
        hidden = (r["resid"][sub, :].astype(F32) + branch * scale * r["post1"][...]).astype(BF)
        hid[rows, :] = hidden
        long = hidden.astype(F32)
        scale = lax.rsqrt(jnp.mean(long * long, axis=-1, keepdims=True) + EPS)
        inp[rows_of(x, c, i), :] = (long * scale * r["pre2"][...]).astype(BF)
        pass_right(0, i).start()
        pass_left(0, i).start()
        share(0, i, c).start()
        show(i, c).start()

    shift = REACH // tok
    qs2, ks2, vs2 = r["qs2"], r["ks2"], r["vs2"]

    def halo2(owner):
        slot = owner - (side - shift)
        rows = pl.ds(pl.multiple_of(REACH + owner * tok, tok), tok)
        dest = pl.ds(pl.multiple_of(slot * tok, tok), tok)
        return [
            remote(
                a.at[rows, :], a.at[dest, :], r["sh2"].at[i, slot], r["rh2"].at[i, slot], sp=up
            )
            for i, a in enumerate((ks2, vs2))
        ]

    def qkv(offset):
        for i in range(2):
            share(offset, i, other).wait_recv()
        owner = away(offset)
        rows = pl.ds(pl.multiple_of(owner * tok, tok), tok)
        late = pl.ds(pl.multiple_of(REACH + owner * tok, tok), tok)
        done = jnp.dot(inp[rows, :], wall[...], preferred_element_type=F32).astype(BF)
        qs2[rows, :] = done[:, :head]
        ks2[late, :] = done[:, head : 2 * head]
        vs2[late, :] = done[:, 2 * head :]

        @pl.when(jnp.logical_and(owner >= side - shift, y < side - 1))
        def _():
            for copy in halo2(owner):
                copy.start()

    for t in range(side):
        cross(t, 1 - plane).wait_recv()
    qkv(0)
    last = steps - 1
    for step in range(1, steps):
        for i in range(2):
            from_left(step - 1, i).wait_recv()
            if step < last or i == 0:
                pass_right(step, i).start()
            share(-step, i, c).start()
            from_right(step - 1, i).wait_recv()
            if step < last or i == 1:
                pass_left(step, i).start()
            share(step, i, c).start()
        g2.yevent(step, 0, 4)
        qkv(-step)
        g2.yevent(step, 4, 4)
        qkv(step)
    from_left(last, 0).wait_recv()
    share(steps, 0, c).start()
    from_right(last, 1).wait_recv()
    share(steps, 1, c).start()
    qkv(steps)

    def between2():
        @pl.when(y > 0)
        def _():
            for k in range(shift):
                for copy in halo2(side - shift + k):
                    copy.wait_recv()

    take_back, back2 = attend_rows(
        side, x, y, qs2, ks2, vs2, r["band2"], r["outs2"], r["mixed2"], r["sb2"], r["rb2"],
        between2,
    )
    g2.yevent(4, 0, 4)
    g2.yevent(4, 4, 4)
    for i in range(2):
        show(i, other).wait_recv()
    take_back(lambda block: None)
    g2.zevent()

    part2, theirs2 = r["part2"], r["theirs2"]
    n = model // CUTS
    swaps2 = [
        remote(
            part2.at[:, pl.ds(i * n, n)], theirs2.at[:, pl.ds(i * n, n)],
            r["sp2"].at[i], r["rp2"].at[i], tp=other,
        )
        for i in range(CUTS)
    ]
    for i in range(CUTS):
        done = lax.dot_general(
            r["mixed2"][...], r["w2"][pl.ds(i * n, n), :], NT, preferred_element_type=F32
        )
        part2[:, pl.ds(i * n, n)] = done.astype(BF)
        swaps2[i].start()
    for copy in swaps2:
        copy.wait_recv()
    for i in range(tok // chunk):
        sub = pl.ds(i * chunk, chunk)
        branch = part2[sub, :].astype(F32) + theirs2[sub, :].astype(F32)
        branch = branch.astype(BF).astype(F32)
        scale = lax.rsqrt(jnp.mean(branch * branch, axis=-1, keepdims=True) + EPS)
        done = hid[sub, :].astype(F32) + branch * scale * r["post2"][...]
        r["out"][sub, :] = done.astype(BF)

    for kind in range(3):
        for d in range(1, side):
            piece(kind, d).wait_send()

    @pl.when(in_plane)
    def _():
        for kind in range(3, 6):
            for d in range(1, side):
                piece(kind, d).wait_send()

    for step in range(steps):
        ring(step, True).wait_send()
        if step < last:
            ring(step, False).wait_send()
    for t in range(side):
        cross(t, plane).wait_send()
    g1.sent()
    g2.sent()
    back1()
    back2()
    for copy in swaps + same + diagonal + swaps2:
        copy.wait_send()
    for block in range(side):
        lend(block).wait_send()
    for step in range(steps):
        for i in range(2):
            if step < last or i == 0:
                pass_right(step, i).wait_send()
            if step < last or i == 1:
                pass_left(step, i).wait_send()
    for i in range(2):
        show(i, c).wait_send()
        for offset in range(side):
            share(offset, i, c).wait_send()

    @pl.when(y < side - 1)
    def _():
        for copy in halo1:
            copy.wait_send()
        for k in range(shift):
            for copy in halo2(side - shift + k):
                copy.wait_send()


def shards(
    side, resid, queries_first, keys_first, values_first, rel_first, post_first, out_first,
    pre_second, query_weight, key_weight, value_weight, rel_second, post_second, out_second,
):
    tok, width = queries_first.shape
    model = resid.shape[1]
    head = width // rel_first.shape[0]
    rows = side * tok
    steps = side // 2
    inputs = {
        "q": (queries_first, ANY),
        "k": (keys_first, ANY),
        "v": (values_first, ANY),
        "rel1": (rel_first, VM),
        "rel2": (rel_second, VM),
        "o1": (out_first.T, ANY),
        "o2": (out_second.T, ANY),
        "resid_any": (resid, ANY),
        "post1": (post_first[None], VM),
        "pre2": (pre_second[None], VM),
        "post2": (post_second[None], VM),
        "wq": (query_weight, ANY),
        "wk": (key_weight, ANY),
        "wv": (value_weight, ANY),
    }

    def vmem(*dims):
        return pltpu.VMEM(dims, BF)

    def dma(*dims):
        return pltpu.SemaphoreType.DMA(dims)

    scratch = {
        "wall": vmem(model, 3 * head),
        "inp": vmem(rows, model),
        "hid": vmem(tok, model),
        "resid": vmem(tok // 2, model),
        "terms1": vmem(2, tok // 2, model),
        "mixedz": vmem(tok, width),
        "partz": vmem(tok, model),
        "theirs2": vmem(tok, model),
        "loads": dma(3),
        "sa2a": dma(6, side),
        "ra2a": dma(6, side),
    }
    for i in (1, 2):
        scratch[f"w{i}"] = vmem(model, width)
        scratch[f"qs{i}"] = vmem(rows, head)
        scratch[f"ks{i}"] = vmem(rows + REACH, head)
        scratch[f"vs{i}"] = vmem(rows + REACH, head)
        scratch[f"outs{i}"] = vmem(rows, head)
        scratch[f"mixed{i}"] = vmem(tok, width)
        scratch[f"part{i}"] = vmem(tok, model)
        scratch[f"band{i}"] = pltpu.VMEM((tok, tok + REACH), F32)
    for d in "sr":
        for i in (1, 2):
            scratch[f"{d}xr{i}"] = dma(steps)
            scratch[f"{d}xl{i}"] = dma(steps)
            scratch[f"{d}yu{i}"] = dma(steps, side)
            scratch[f"{d}yd{i}"] = dma(steps, side)
            scratch[f"{d}z{i}"] = dma(side, side)
            scratch[f"{d}b{i}"] = dma(side)
            scratch[f"{d}p{i}"] = dma(CUTS)
        scratch[f"{d}mz"] = dma(side)
        scratch[f"{d}rz"] = dma(2, steps)
        scratch[f"{d}qu"] = dma(steps)
        scratch[f"{d}qd"] = dma(steps)
        scratch[f"{d}qz"] = dma(side)
        scratch[f"{d}h1"] = dma(2)
        scratch[f"{d}h2"] = dma(2, REACH // tok)
        scratch[f"{d}r"] = dma(steps, 2)
        scratch[f"{d}l"] = dma(steps, 2)
        scratch[f"{d}d"] = dma(side, 2)
        scratch[f"{d}w"] = dma(2)
    return pl.pallas_call(
        functools.partial(layers_kernel, side, [*inputs, "out", *scratch]),
        out_shape=jax.ShapeDtypeStruct((tok, model), BF),
        in_specs=[spec for _, spec in inputs.values()],
        out_specs=VM,
        scratch_shapes=list(scratch.values()),
        compiler_params=pltpu.CompilerParams(has_side_effects=True, collective_id=0),
    )(*(value for value, _ in inputs.values()))


def solution(mesh):
    side = math.isqrt(mesh.shape["sp"])
    in_specs = (
        P(("grp", "sp"), None),
        P(("grp", "sp"), "tp"),
        P(("grp", "sp"), "tp"),
        P(("grp", "sp"), "tp"),
        P("tp", None),
        P(),
        P("tp", "sp"),
        P(),
        P("sp", "tp"),
        P("sp", "tp"),
        P("sp", "tp"),
        P("tp", None),
        P(),
        P("tp", "sp"),
    )
    out_specs = P(("grp", "sp"), None)
    return jax.shard_map(
        functools.partial(shards, side),
        mesh=mesh,
        in_specs=in_specs,
        out_specs=out_specs,
        check_vma=False,
    )
```

```python
import functools
import math

import jax
import jax.numpy as jnp
from jax import lax
from jax.experimental import pallas as pl
from jax.experimental.pallas import tpu as pltpu
from jax.sharding import PartitionSpec as P

SEG = 64
LEFT = 8
REACH = 512
REL_CLIP = 128
EPS = 1e-06
NEG_FILL = -1e30
LOG2E = 1.4426950408889634
BF = jnp.bfloat16
F32 = jnp.float32
MESH = pl.DeviceIdType.MESH
VM = pl.BlockSpec(memory_space=pltpu.VMEM)
ANY = pl.BlockSpec(memory_space=pl.ANY)
NT = (((1,), (1,)), ((), ()))


def place(side):
    sp = lax.axis_index("sp")
    return lax.rem(sp, side), lax.div(sp, side), lax.axis_index("tp")


def remote(src, dst, send, recv, **where):
    return pltpu.make_async_remote_copy(
        src_ref=src,
        dst_ref=dst,
        send_sem=send,
        recv_sem=recv,
        device_id=dict(where),
        device_id_type=MESH,
    )


def greet(side, x, y, c, grp):
    barrier = pltpu.get_barrier_semaphore()
    peers = [{"sp": y * side + lax.rem(x + d, side)} for d in range(1, side)]
    peers += [{"sp": lax.rem(y + d, side) * side + x} for d in (1, side - 1)]
    peers += [{"tp": 1 - c}]
    peers += [{"grp": other_plane(grp)}, {"grp": other_plane(grp), "tp": 1 - c}]
    for peer in peers:
        pl.semaphore_signal(barrier, inc=1, device_id=peer, device_id_type=MESH)
    return lambda: pl.semaphore_wait(barrier, len(peers))


def other_plane(grp):
    return grp + 1 - 2 * lax.rem(grp, 2)


def spread_bias(table_ref, band_ref, x):
    tok, window = band_ref.shape
    length = window + tok
    near = table_ref[:, : 2 * REL_CLIP]
    far = table_ref[:, 2 * REL_CLIP :]
    end = REACH + REL_CLIP
    slot = end - lax.broadcasted_iota(jnp.int32, (2 * REL_CLIP, length), 1)
    pick = slot == lax.broadcasted_iota(jnp.int32, (2 * REL_CLIP, length), 0)
    lines = jnp.dot(
        near, pick.astype(F32), preferred_element_type=F32, precision=lax.Precision.HIGHEST
    )
    where = lax.broadcasted_iota(jnp.int32, lines.shape, 1)
    lines = jnp.where((where > end - 2 * REL_CLIP) & (where < end), lines, far)
    chosen = lax.broadcasted_iota(jnp.int32, lines.shape, 0) == x
    line = jnp.sum(jnp.where(chosen, lines, 0.0), axis=0, keepdims=True)
    wide = jnp.broadcast_to(line, (tok, length))
    wide = pltpu.roll(wide, 0, 1, stride=1, stride_axis=0)[:, :window] * LOG2E
    qseg = lax.broadcasted_iota(jnp.int32, (tok, window), 0) // SEG
    kseg = lax.broadcasted_iota(jnp.int32, (tok, window), 1) // SEG
    band_ref[...] = jnp.where((kseg >= qseg) & (kseg <= qseg + LEFT), wide, NEG_FILL)


def attend(block, first_row, qs, ks, vs, band_ref):
    tok, window = band_ref.shape
    head = qs.shape[1]
    at = pl.multiple_of(block * tok, tok)
    query = qs[pl.ds(at, tok), :]
    keys = ks[pl.ds(at, window), :]
    values = vs[pl.ds(at, window), :]
    scores = lax.dot_general(query, keys, NT, preferred_element_type=F32)
    scores = scores * (head**-0.5 * LOG2E) + band_ref[...]
    if first_row is not None:
        column = lax.broadcasted_iota(jnp.int32, (1, window), 1) + block * tok
        hidden = jnp.logical_and(column < REACH, first_row)
        scores = scores + jnp.where(hidden, NEG_FILL, 0.0)
    largest = jnp.max(scores, axis=-1, keepdims=True)
    weights = jnp.exp2(scores - largest)
    total = jnp.sum(weights, axis=-1, keepdims=True)
    mixed = jnp.dot(weights.astype(BF), values, preferred_element_type=F32)
    return (mixed / total).astype(BF)


def attend_rows(side, x, y, qs, ks, vs, band, outs, mixed, ssem, rsem, between):
    tok, head = band.shape[0], qs.shape[1]
    here = pl.ds(pl.multiple_of(x * head, head), head)

    def hand_back(block):
        rows = pl.ds(pl.multiple_of(block * tok, tok), tok)
        return remote(
            outs.at[rows, :], mixed.at[:, here], ssem.at[block], rsem.at[x], sp=y * side + block
        )

    def run(block, first_row):
        result = attend(block, first_row, qs, ks, vs, band)
        outs[pl.ds(pl.multiple_of(block * tok, tok), tok), :] = result

        @pl.when(block != x)
        def _():
            hand_back(block).start()

        @pl.when(block == x)
        def _():
            mixed[:, here] = result

    half = REACH // tok

    def late(i, carry):
        run(i + half, None)
        return carry

    lax.fori_loop(0, side - half, late, 0)
    between()

    def early(i, carry):
        run(i, y == 0)
        return carry

    lax.fori_loop(0, half, early, 0)

    def take_back(then):
        def finish(block, carry):
            @pl.when(block != x)
            def _():
                there = pl.ds(pl.multiple_of(block * head, head), head)
                remote(
                    outs.at[pl.ds(0, tok), :],
                    mixed.at[:, there],
                    ssem.at[block],
                    rsem.at[block],
                    sp=y * side + block,
                ).wait_recv()
                then(block)

            return carry

        lax.fori_loop(0, side, finish, 0)

    def sent():
        def finish(block, carry):
            @pl.when(block != x)
            def _():
                hand_back(block).wait_send()

            return carry

        lax.fori_loop(0, side, finish, 0)

    return take_back, sent


def clear_halo(y, ks, vs):
    @pl.when(y == 0)
    def _():
        ks[pl.ds(0, REACH), :] = jnp.zeros((REACH, ks.shape[1]), BF)
        vs[pl.ds(0, REACH), :] = jnp.zeros((REACH, vs.shape[1]), BF)


class Gather:
    def __init__(self, side, x, y, grp, buf, shared, xr, xl, yu, yd, z):
        self.side, self.x, self.y, self.grp, self.buf = side, x, y, grp, buf
        self.xr, self.xl, self.yu, self.yd, self.z = xr, xl, yu, yd, z
        self.shared = shared
        self.rows = buf.shape[0] // (side * side)
        quarter = buf.shape[1] // 4
        self.plane = lax.rem(grp, 2)
        self.inside = pl.ds(0, buf.shape[1])
        if not shared:
            self.inside = pl.ds(pl.multiple_of(self.plane * quarter, quarter), 3 * quarter)
        self.across = pl.ds(pl.multiple_of(self.plane * 3 * quarter, quarter), quarter)
        self.theirs = pl.ds(pl.multiple_of((1 - self.plane) * 3 * quarter, quarter), quarter)

    def guard(self, step):
        if self.shared:
            return pl.when(lax.rem(self.y + step, 2) == self.plane)
        return lambda run: run()

    def slab(self, xp, yp, columns):
        at = pl.multiple_of((yp * self.side + xp) * self.rows, self.rows)
        return self.buf.at[pl.ds(at, self.rows), columns]

    def column(self, k):
        if isinstance(k, int):
            off = -(k + 1) // 2 if k % 2 else k // 2
        else:
            off = jnp.where(lax.rem(k, 2) == 1, -lax.div(k + 1, 2), lax.div(k, 2))
        return lax.rem(self.x + off + self.side, self.side)

    def xcopy(self, step, right):
        owner = lax.rem(self.x + (-step if right else step) + self.side, self.side)
        to = lax.rem(self.x + (1 if right else self.side - 1), self.side)
        part = self.slab(owner, self.y, self.inside)
        send, recv = self.xr if right else self.xl
        return remote(part, part, send.at[step], recv.at[step], sp=self.y * self.side + to)

    def xarrival(self, step, right):
        owner = lax.rem(self.x + (-step - 1 if right else step + 1) + self.side, self.side)
        part = self.slab(owner, self.y, self.inside)
        send, recv = self.xr if right else self.xl
        return remote(part, part, send.at[step], recv.at[step], sp=self.y * self.side + self.x)

    def ycopy(self, step, k, upward):
        owner = lax.rem(self.y + (-step if upward else step) + self.side, self.side)
        to = lax.rem(self.y + (1 if upward else self.side - 1), self.side)
        part = self.slab(self.column(k), owner, self.inside)
        send, recv = self.yu if upward else self.yd
        return remote(part, part, send.at[step, k], recv.at[step, k], sp=to * self.side + self.x)

    def yarrival(self, step, k, upward):
        owner = lax.rem(self.y + (-step - 1 if upward else step + 1) + self.side, self.side)
        part = self.slab(self.column(k), owner, self.inside)
        send, recv = self.yu if upward else self.yd
        return remote(part, part, send.at[step, k], recv.at[step, k], sp=self.x)

    def zcopy(self, t, k, columns):
        owner = lax.rem(self.y - t + self.side, self.side)
        part = self.slab(self.column(k), owner, columns)
        send, recv = self.z
        return remote(part, part, send.at[t, k], recv.at[t, k], grp=other_plane(self.grp))

    def begin(self):
        @self.guard(0)
        def _():
            self.xcopy(0, True).start()
            self.xcopy(0, False).start()
            if self.shared:
                self.ycopy(0, 0, True).start()
                self.ycopy(0, 0, False).start()

    def xevent(self, k):
        right = k % 2 == 1
        step = (k + 1) // 2 if right else k // 2

        @self.guard(0)
        def _():
            self.xarrival(step - 1, right).wait_recv()
            if step < self.side // 2 - (0 if right else 1):
                self.xcopy(step, right).start()
            if self.shared:
                self.ycopy(0, k, True).start()
                self.ycopy(0, k, False).start()
            else:
                self.zcopy(0, k, self.across).start()

    def ybegin(self, *pieces):
        for k in pieces:
            self.ycopy(0, k, True).start()
            self.ycopy(0, k, False).start()

    def yevent(self, step, base, count):
        side = self.side
        half = side // 2
        far = step == half
        lower = base < half

        def one(k, carry):
            if not far or lower:
                self.yarrival(step - 1, k, True).wait_recv()
                if step < half - 1 or (step == half - 1 and lower):
                    self.ycopy(step, k, True).start()
                if not self.shared:
                    self.zcopy(step, k, self.across).start()
            if not far or not lower:
                self.yarrival(step - 1, k, False).wait_recv()
                if step < half - 1 or (step == half - 1 and not lower):
                    self.ycopy(step, k, False).start()
                if not self.shared:
                    self.zcopy(side - step, k, self.across).start()
            return carry

        @self.guard(step)
        def _():
            lax.fori_loop(base, base + count, one, 0)

    def zevent(self):
        side = self.side

        def one(i, carry):
            t, k = lax.div(i, side), lax.rem(i, side)
            self.zcopy(t, k, self.theirs).wait_recv()
            return carry

        lax.fori_loop(1, side * side, one, 0)

    def sent(self):
        side = self.side
        half = side // 2

        @self.guard(0)
        def _():
            for step in range(half):
                self.xcopy(step, True).wait_send()
                if step < half - 1:
                    self.xcopy(step, False).wait_send()

        for step in range(half):

            def one(k, carry, step=step):
                if step < half - 1:
                    self.ycopy(step, k, True).wait_send()
                    self.ycopy(step, k + half, True).wait_send()
                    self.ycopy(step, k, False).wait_send()
                else:
                    self.ycopy(step, k, True).wait_send()
                self.ycopy(step, k + half, False).wait_send()
                return carry

            @self.guard(step)
            def _(one=one):
                lax.fori_loop(0, half, one, 0)

        def one(i, carry):
            self.zcopy(lax.div(i, side), lax.rem(i, side), self.across).wait_send()
            return carry

        if not self.shared:
            lax.fori_loop(1, side * side, one, 0)


CUTS = 4


def layers_kernel(side, names, *refs):
    r = dict(zip(names, refs))
    x, y, c = place(side)
    grp = lax.axis_index("grp")
    plane = lax.rem(grp, 2)
    q_ref, k_ref, v_ref = r["q"], r["k"], r["v"]
    tok, width = q_ref.shape
    head = width // side
    wall = r["wall"]
    wrow = r["wq"].shape[0]
    group = side * wrow
    model = r["w1"].shape[0]
    other = 1 - c
    half = tok // 2
    steps = side // 2
    up = lax.rem(y + 1, side) * side + x
    down = lax.rem(y + side - 1, side) * side + x
    right = y * side + lax.rem(x + 1, side)
    left = y * side + lax.rem(x + side - 1, side)

    meet = greet(side, x, y, c, grp)
    own = pl.ds(pl.multiple_of((y * side + x) * wrow, wrow), wrow)
    loads = [
        pltpu.make_async_copy(r["o1"], r["w1"].at[own, :], r["loads"].at[0]),
        pltpu.make_async_copy(r["o2"], r["w2"].at[own, :], r["loads"].at[1]),
        pltpu.make_async_copy(
            r["resid_any"].at[pl.ds(pl.multiple_of(c * half, half), half), :],
            r["resid"],
            r["loads"].at[2],
        ),
    ]
    for load in loads:
        load.start()
    g1, g2 = [
        Gather(
            side, x, y, grp, r[f"w{i}"], i == 1,
            *((r[f"s{kind}{i}"], r[f"r{kind}{i}"]) for kind in ("xr", "xl", "yu", "yd", "z")),
        )
        for i in (1, 2)
    ]

    mine = pl.ds(pl.multiple_of(x * tok, tok), tok)
    mine_late = pl.ds(pl.multiple_of(REACH + x * tok, tok), tok)
    kinds = [
        (k_ref, r["ks1"].at[mine_late, :]),
        (v_ref, r["vs1"].at[mine_late, :]),
        (q_ref, r["qs1"].at[mine, :]),
    ] + [(r[f"w{n}"], wall.at[own, pl.ds(i * head, head)]) for i, n in enumerate("qkv")]

    def piece(kind, d):
        peer = lax.rem(x + d, side)
        src, dst = kinds[kind]
        cut = src.at[:, pl.ds(pl.multiple_of(peer * head, head), head)]
        if d == 0:
            return pltpu.make_async_copy(cut, dst, r["ra2a"].at[kind, 0])
        send, recv = r["sa2a"].at[kind, d], r["ra2a"].at[kind, d]
        return remote(cut, dst, send, recv, sp=y * side + peer)

    for kind in range(3):
        piece(kind, 0).start()
    in_plane = lax.div(x, steps) == plane

    @pl.when(in_plane)
    def _():
        for kind in range(3, 6):
            piece(kind, 0).start()

    spread_bias(r["rel1"], r["band1"], x)
    spread_bias(r["rel2"], r["band2"], x)
    clear_halo(y, r["ks1"], r["vs1"])
    clear_halo(y, r["ks2"], r["vs2"])
    for load in loads:
        load.wait()
    meet()

    def take(kind):
        piece(kind, 0).wait()
        for d in range(1, side):
            piece(kind, d).wait_recv()

    def ring_rows(owner, parity):
        return pl.ds(pl.multiple_of(owner * group + parity * (group // 2), group // 2), group // 2)

    def ring(step, upward):
        owner = lax.rem(y + (-step if upward else step) + side, side)
        part = wall.at[ring_rows(owner, plane), :]
        send, recv = (r["squ"], r["rqu"]) if upward else (r["sqd"], r["rqd"])
        return remote(part, part, send.at[step], recv.at[step], sp=up if upward else down)

    def cross(t, parity):
        owner = lax.rem(y - t + side, side)
        part = wall.at[ring_rows(owner, parity), :]
        return remote(part, part, r["sqz"].at[t], r["rqz"].at[t], grp=other_plane(grp))

    def relay(step):
        if step == 0:
            @pl.when(in_plane)
            def _():
                for kind in range(3, 6):
                    piece(kind, 0).wait()

            for d in range(1, side):
                @pl.when(lax.div(lax.rem(x - d + side, side), steps) == plane)
                def _(d=d):
                    for kind in range(3, 6):
                        piece(kind, d).wait_recv()

        if step > 0:
            ring(step - 1, True).wait_recv()
        if step < steps:
            ring(step, True).start()
        if step > 0:
            cross(step, plane).start()
        if 0 < step < steps:
            ring(step - 1, False).wait_recv()
        if 0 < step < steps:
            cross(side - step, plane).start()
        if step < steps - 1:
            ring(step, False).start()

    g1.begin()

    opposite = side // 2
    odd = lax.rem(x, 2) == 1
    far_x = lax.rem(x + opposite, side)
    far_cut = pl.ds(pl.multiple_of(far_x * head, head), head)
    behind = pl.ds(pl.multiple_of(REACH + lax.rem(x + 1, side) * tok, tok), tok)
    behind_q = pl.ds(pl.multiple_of(lax.rem(x + 1, side) * tok, tok), tok)

    def detour(kind):
        src = v_ref if kind == 1 else q_ref
        return remote(
            src.at[:, far_cut], r["via"].at[kind - 1], r["sv"].at[kind, 0], r["rv"].at[kind - 1],
            sp=left,
        )

    def onward(kind):
        dst = r["vs1"].at[behind, :] if kind == 1 else r["qs1"].at[behind_q, :]
        return remote(
            r["via"].at[kind - 1], dst, r["sv"].at[kind, 1], r["ra2a"].at[kind, opposite],
            sp=y * side + lax.rem(x + opposite + 1, side),
        )

    def hand_out(kinds, distances):
        for d in distances:
            for kind in kinds:
                piece(kind, d).start()

    near, third = [1, side - 1, 2, side - 2], [3, side - 3]
    hand_out([0], near)
    g1.xevent(1)
    g1.xevent(2)
    hand_out([1], near)
    detour(1).start()
    g1.xevent(3)
    g1.xevent(4)
    hand_out([0], third + [opposite])
    g1.yevent(1, 0, 2)
    g1.xevent(5)
    g1.xevent(6)
    hand_out([1], third)
    detour(1).wait_recv()
    onward(1).start()

    @pl.when(odd)
    def _():
        detour(2).start()

    g1.yevent(1, 2, 2)
    g1.yevent(2, 0, 2)
    g1.xevent(7)

    @pl.when(jnp.logical_not(odd))
    def _():
        hand_out([2], [opposite])

    hand_out([2], third + near)

    @pl.when(in_plane)
    def _():
        hand_out([3, 4, 5], range(1, side))

    @pl.when(jnp.logical_not(odd))
    def _():
        detour(2).wait_recv()
        onward(2).start()

    g1.yevent(1, 4, 2)
    g1.yevent(2, 2, 2)
    g1.yevent(3, 0, 2)
    g1.yevent(1, 6, 2)
    g1.yevent(2, 4, 2)
    g1.yevent(3, 2, 2)
    take(0)
    take(1)
    halo1 = [
        remote(
            a.at[pl.ds(side * tok, REACH), :], a.at[pl.ds(0, REACH), :],
            r["sh1"].at[i], r["rh1"].at[i], sp=up,
        )
        for i, a in enumerate((r["ks1"], r["vs1"]))
    ]

    @pl.when(y < side - 1)
    def _():
        for copy in halo1:
            copy.start()

    take(2)
    g2.begin()

    def between():
        g1.yevent(2, 6, 2)
        g1.yevent(3, 4, 2)
        @pl.when(y > 0)
        def _():
            for copy in halo1:
                copy.wait_recv()


    take_back, back1 = attend_rows(
        side, x, y, r["qs1"], r["ks1"], r["vs1"], r["band1"], r["outs1"], r["mixed1"],
        r["sb1"], r["rb1"], between,
    )
    g1.yevent(3, 6, 2)
    relay(0)
    g2.xevent(1)
    g2.xevent(2)
    g1.yevent(4, 0, 4)
    g1.yevent(4, 4, 4)
    mixed1, mixedz = r["mixed1"], r["mixedz"]

    def lend(block):
        there = pl.ds(pl.multiple_of(block * head, head), head)
        return remote(
            mixed1.at[:, there], mixedz.at[:, there], r["smz"].at[block], r["rmz"].at[block],
            grp=other_plane(grp),
        )

    lend(x).start()
    take_back(lambda block: lend(block).start())

    n = group
    part1, partz, terms = r["part1"], r["partz"], r["terms1"]
    my_half = pl.ds(pl.multiple_of(c * half, half), half)
    their_half = pl.ds(pl.multiple_of(other * half, half), half)

    def columns(j):
        return pl.ds(pl.multiple_of((2 * j + plane) * n, n), n)

    swaps, same, diagonal = [], [], []
    for j in range(steps):
        at, lent = columns(j), (r["srz"], r["rrz"])
        swaps.append(
            remote(
                part1.at[their_half, at], terms.at[1, :, at], r["sp1"].at[j], r["rp1"].at[j],
                tp=other,
            )
        )
        same.append(
            remote(
                partz.at[my_half, at], terms.at[0, :, at], lent[0].at[0, j], lent[1].at[0, j],
                grp=other_plane(grp),
            )
        )
        diagonal.append(
            remote(
                partz.at[their_half, at], terms.at[1, :, at], lent[0].at[1, j], lent[1].at[1, j],
                grp=other_plane(grp), tp=other,
            )
        )

    def out1(rows, j):
        return lax.dot_general(
            rows[...], r["w1"][columns(j), :], NT, preferred_element_type=F32
        ).astype(BF)

    for j in range(steps):
        part1[:, columns(j)] = out1(mixed1, j)
        swaps[j].start()
        terms[0, :, columns(j)] = part1[my_half, columns(j)]
    g2.xevent(3)
    g2.xevent(4)
    for block in range(side):
        lend(block).wait_recv()
    for j in range(steps):
        partz[:, columns(j)] = out1(mixedz, j)
        same[j].start()
        diagonal[j].start()
    cross(0, plane).start()
    relay(1)
    g2.ybegin(0, 1, 2)
    for copy in swaps + same + diagonal:
        copy.wait_recv()

    inp, hid = r["inp"], r["hid"]
    chunk = half // 2

    def rows_of(owner, core, i):
        return pl.ds(pl.multiple_of(owner * tok + core * half + i * chunk, chunk), chunk)

    def away(step):
        return lax.rem(x + step + side, side)

    def spread(owner, send, recv, **to):
        return lambda step, i: remote(
            inp.at[rows_of(owner(step), c, i), :], inp.at[rows_of(owner(step), c, i), :],
            send.at[step, i], recv.at[step, i], **to,
        )

    pass_right = spread(lambda s: away(-s), r["sr"], r["rr"], sp=right)
    pass_left = spread(lambda s: away(s), r["sl"], r["rl"], sp=left)
    from_left = spread(lambda s: away(-s - 1), r["sr"], r["rr"], sp=right)
    from_right = spread(lambda s: away(s + 1), r["sl"], r["rl"], sp=left)

    def share(offset, i, core):
        rows = rows_of(away(offset), core, i)
        slot = offset % side
        return remote(
            inp.at[rows, :], inp.at[rows, :], r["sd"].at[slot, i], r["rd"].at[slot, i], tp=other
        )

    def show(i, core):
        rows = rows_of(0, core, i)
        return remote(hid.at[rows, :], hid.at[rows, :], r["sw"].at[i], r["rw"].at[i], tp=other)

    for i in range(2):
        rows = rows_of(0, c, i)
        sub = pl.ds(i * chunk, chunk)
        branch = terms[0, sub, :].astype(F32) + terms[1, sub, :].astype(F32)
        branch = branch.astype(BF).astype(F32)
        scale = lax.rsqrt(jnp.mean(branch * branch, axis=-1, keepdims=True) + EPS)
        hidden = (r["resid"][sub, :].astype(F32) + branch * scale * r["post1"][...]).astype(BF)
        hid[rows, :] = hidden
        long = hidden.astype(F32)
        scale = lax.rsqrt(jnp.mean(long * long, axis=-1, keepdims=True) + EPS)
        inp[rows_of(x, c, i), :] = (long * scale * r["pre2"][...]).astype(BF)
        pass_right(0, i).start()
        pass_left(0, i).start()
        share(0, i, c).start()
        show(i, c).start()

    shift = REACH // tok
    qs2, ks2, vs2 = r["qs2"], r["ks2"], r["vs2"]

    def halo2(owner):
        slot = owner - (side - shift)
        rows = pl.ds(pl.multiple_of(REACH + owner * tok, tok), tok)
        dest = pl.ds(pl.multiple_of(slot * tok, tok), tok)
        return [
            remote(
                a.at[rows, :], a.at[dest, :], r["sh2"].at[i, slot], r["rh2"].at[i, slot], sp=up
            )
            for i, a in enumerate((ks2, vs2))
        ]

    def qkv(offset):
        for i in range(2):
            share(offset, i, other).wait_recv()
        owner = away(offset)
        rows = pl.ds(pl.multiple_of(owner * tok, tok), tok)
        late = pl.ds(pl.multiple_of(REACH + owner * tok, tok), tok)
        done = jnp.dot(inp[rows, :], wall[...], preferred_element_type=F32).astype(BF)
        qs2[rows, :] = done[:, :head]
        ks2[late, :] = done[:, head : 2 * head]
        vs2[late, :] = done[:, 2 * head :]

        @pl.when(jnp.logical_and(owner >= side - shift, y < side - 1))
        def _():
            for copy in halo2(owner):
                copy.start()

    relay(2)
    g2.ybegin(3, 4)
    g2.xevent(5)
    g2.xevent(6)
    last = steps - 1

    def fill(step, i):
        if (step, i) == (1, 0):
            relay(3)
            g2.ybegin(5, 6)
        elif (step, i) == (1, 1):
            relay(4)
            g2.xevent(7)
            g2.ybegin(7)
        elif (step, i) == (2, 0):
            g2.yevent(1, 0, 4)
        elif (step, i) == (2, 1):
            g2.yevent(1, 4, 4)
        elif (step, i) == (3, 0):
            g2.yevent(2, 0, 4)

    for step in range(1, steps):
        for i in range(2):
            from_left(step - 1, i).wait_recv()
            if step < last or i == 0:
                pass_right(step, i).start()
            share(-step, i, c).start()
            from_right(step - 1, i).wait_recv()
            if step < last or i == 1:
                pass_left(step, i).start()
            share(step, i, c).start()
            fill(step, i)
    for t in range(side):
        cross(t, 1 - plane).wait_recv()
    qkv(0)
    for d in range(1, steps):
        qkv(-d)
        qkv(d)
    g2.yevent(2, 4, 4)
    from_left(last, 0).wait_recv()
    share(steps, 0, c).start()
    from_right(last, 1).wait_recv()
    share(steps, 1, c).start()
    qkv(steps)

    g2.yevent(3, 0, 4)

    def between2():
        @pl.when(y > 0)
        def _():
            for k in range(shift):
                for copy in halo2(side - shift + k):
                    copy.wait_recv()

        g2.yevent(3, 4, 4)

    take_back, back2 = attend_rows(
        side, x, y, qs2, ks2, vs2, r["band2"], r["outs2"], r["mixed2"], r["sb2"], r["rb2"],
        between2,
    )
    g2.yevent(4, 0, 4)
    for i in range(2):
        show(i, other).wait_recv()
    take_back(lambda block: None)
    g2.yevent(4, 4, 4)
    g2.zevent()

    part2, theirs2 = r["part2"], r["theirs2"]
    n = model // CUTS
    swaps2 = [
        remote(
            part2.at[:, pl.ds(i * n, n)], theirs2.at[:, pl.ds(i * n, n)],
            r["sp2"].at[i], r["rp2"].at[i], tp=other,
        )
        for i in range(CUTS)
    ]
    for i in range(CUTS):
        done = lax.dot_general(
            r["mixed2"][...], r["w2"][pl.ds(i * n, n), :], NT, preferred_element_type=F32
        )
        part2[:, pl.ds(i * n, n)] = done.astype(BF)
        swaps2[i].start()
    for copy in swaps2:
        copy.wait_recv()
    for i in range(tok // chunk):
        sub = pl.ds(i * chunk, chunk)
        branch = part2[sub, :].astype(F32) + theirs2[sub, :].astype(F32)
        branch = branch.astype(BF).astype(F32)
        scale = lax.rsqrt(jnp.mean(branch * branch, axis=-1, keepdims=True) + EPS)
        done = hid[sub, :].astype(F32) + branch * scale * r["post2"][...]
        r["out"][sub, :] = done.astype(BF)

    for kind in range(3):
        for d in range(1, side):
            if kind == 0 or d != opposite:
                piece(kind, d).wait_send()
    detour(1).wait_send()
    onward(1).wait_send()

    @pl.when(odd)
    def _():
        detour(2).wait_send()

    @pl.when(jnp.logical_not(odd))
    def _():
        onward(2).wait_send()
        piece(2, opposite).wait_send()

    @pl.when(in_plane)
    def _():
        for kind in range(3, 6):
            for d in range(1, side):
                piece(kind, d).wait_send()

    for step in range(steps):
        ring(step, True).wait_send()
        if step < last:
            ring(step, False).wait_send()
    for t in range(side):
        cross(t, plane).wait_send()
    g1.sent()
    g2.sent()
    back1()
    back2()
    for copy in swaps + same + diagonal + swaps2:
        copy.wait_send()
    for block in range(side):
        lend(block).wait_send()
    for step in range(steps):
        for i in range(2):
            if step < last or i == 0:
                pass_right(step, i).wait_send()
            if step < last or i == 1:
                pass_left(step, i).wait_send()
    for i in range(2):
        show(i, c).wait_send()
        for offset in range(side):
            share(offset, i, c).wait_send()

    @pl.when(y < side - 1)
    def _():
        for copy in halo1:
            copy.wait_send()
        for k in range(shift):
            for copy in halo2(side - shift + k):
                copy.wait_send()


def shards(
    side, resid, queries_first, keys_first, values_first, rel_first, post_first, out_first,
    pre_second, query_weight, key_weight, value_weight, rel_second, post_second, out_second,
):
    tok, width = queries_first.shape
    model = resid.shape[1]
    head = width // rel_first.shape[0]
    rows = side * tok
    steps = side // 2
    inputs = {
        "q": (queries_first, ANY),
        "k": (keys_first, ANY),
        "v": (values_first, ANY),
        "rel1": (rel_first, VM),
        "rel2": (rel_second, VM),
        "o1": (out_first.T, ANY),
        "o2": (out_second.T, ANY),
        "resid_any": (resid, ANY),
        "post1": (post_first[None], VM),
        "pre2": (pre_second[None], VM),
        "post2": (post_second[None], VM),
        "wq": (query_weight, ANY),
        "wk": (key_weight, ANY),
        "wv": (value_weight, ANY),
    }

    def vmem(*dims):
        return pltpu.VMEM(dims, BF)

    def dma(*dims):
        return pltpu.SemaphoreType.DMA(dims)

    scratch = {
        "wall": vmem(model, 3 * head),
        "inp": vmem(rows, model),
        "hid": vmem(tok, model),
        "resid": vmem(tok // 2, model),
        "terms1": vmem(2, tok // 2, model),
        "mixedz": vmem(tok, width),
        "partz": vmem(tok, model),
        "theirs2": vmem(tok, model),
        "loads": dma(3),
        "via": vmem(2, tok, head),
        "sv": dma(3, 2),
        "rv": dma(2),
        "sa2a": dma(6, side),
        "ra2a": dma(6, side),
    }
    for i in (1, 2):
        scratch[f"w{i}"] = vmem(model, width)
        scratch[f"qs{i}"] = vmem(rows, head)
        scratch[f"ks{i}"] = vmem(rows + REACH, head)
        scratch[f"vs{i}"] = vmem(rows + REACH, head)
        scratch[f"outs{i}"] = vmem(rows, head)
        scratch[f"mixed{i}"] = vmem(tok, width)
        scratch[f"part{i}"] = vmem(tok, model)
        scratch[f"band{i}"] = pltpu.VMEM((tok, tok + REACH), F32)
    for d in "sr":
        for i in (1, 2):
            scratch[f"{d}xr{i}"] = dma(steps)
            scratch[f"{d}xl{i}"] = dma(steps)
            scratch[f"{d}yu{i}"] = dma(steps, side)
            scratch[f"{d}yd{i}"] = dma(steps, side)
            scratch[f"{d}z{i}"] = dma(side, side)
            scratch[f"{d}b{i}"] = dma(side)
            scratch[f"{d}p{i}"] = dma(CUTS)
        scratch[f"{d}mz"] = dma(side)
        scratch[f"{d}rz"] = dma(2, steps)
        scratch[f"{d}qu"] = dma(steps)
        scratch[f"{d}qd"] = dma(steps)
        scratch[f"{d}qz"] = dma(side)
        scratch[f"{d}h1"] = dma(2)
        scratch[f"{d}h2"] = dma(2, REACH // tok)
        scratch[f"{d}r"] = dma(steps, 2)
        scratch[f"{d}l"] = dma(steps, 2)
        scratch[f"{d}d"] = dma(side, 2)
        scratch[f"{d}w"] = dma(2)
    return pl.pallas_call(
        functools.partial(layers_kernel, side, [*inputs, "out", *scratch]),
        out_shape=jax.ShapeDtypeStruct((tok, model), BF),
        in_specs=[spec for _, spec in inputs.values()],
        out_specs=VM,
        scratch_shapes=list(scratch.values()),
        compiler_params=pltpu.CompilerParams(has_side_effects=True, collective_id=0),
    )(*(value for value, _ in inputs.values()))


def solution(mesh):
    side = math.isqrt(mesh.shape["sp"])
    in_specs = (
        P(("grp", "sp"), None),
        P(("grp", "sp"), "tp"),
        P(("grp", "sp"), "tp"),
        P(("grp", "sp"), "tp"),
        P("tp", None),
        P(),
        P("tp", "sp"),
        P(),
        P("sp", "tp"),
        P("sp", "tp"),
        P("sp", "tp"),
        P("tp", None),
        P(),
        P("tp", "sp"),
    )
    out_specs = P(("grp", "sp"), None)
    return jax.shard_map(
        functools.partial(shards, side),
        mesh=mesh,
        in_specs=in_specs,
        out_specs=out_specs,
        check_vma=False,
    )
```

```python
import functools
import math

import jax
import jax.numpy as jnp
from jax import lax
from jax.experimental import pallas as pl
from jax.experimental.pallas import tpu as pltpu
from jax.sharding import PartitionSpec as P

SEG = 64
LEFT = 8
REACH = 512
REL_CLIP = 128
EPS = 1e-06
NEG_FILL = -1e30
LOG2E = 1.4426950408889634
BF = jnp.bfloat16
F32 = jnp.float32
MESH = pl.DeviceIdType.MESH
VM = pl.BlockSpec(memory_space=pltpu.VMEM)
ANY = pl.BlockSpec(memory_space=pl.ANY)
NT = (((1,), (1,)), ((), ()))


def place(side):
    sp = lax.axis_index("sp")
    return lax.rem(sp, side), lax.div(sp, side), lax.axis_index("tp")


def remote(src, dst, send, recv, **where):
    return pltpu.make_async_remote_copy(
        src_ref=src,
        dst_ref=dst,
        send_sem=send,
        recv_sem=recv,
        device_id=dict(where),
        device_id_type=MESH,
    )


def greet(side, x, y, c, grp):
    barrier = pltpu.get_barrier_semaphore()
    peers = [{"sp": y * side + lax.rem(x + d, side)} for d in range(1, side)]
    peers += [{"sp": lax.rem(y + d, side) * side + x} for d in (1, side - 1)]
    peers += [{"tp": 1 - c}]
    peers += [{"grp": other_plane(grp)}, {"grp": other_plane(grp), "tp": 1 - c}]
    for peer in peers:
        pl.semaphore_signal(barrier, inc=1, device_id=peer, device_id_type=MESH)
    return lambda: pl.semaphore_wait(barrier, len(peers))


def other_plane(grp):
    return grp + 1 - 2 * lax.rem(grp, 2)


def spread_bias(table_ref, band_ref, x):
    tok, window = band_ref.shape
    length = window + tok
    near = table_ref[:, : 2 * REL_CLIP]
    far = table_ref[:, 2 * REL_CLIP :]
    end = REACH + REL_CLIP
    slot = end - lax.broadcasted_iota(jnp.int32, (2 * REL_CLIP, length), 1)
    pick = slot == lax.broadcasted_iota(jnp.int32, (2 * REL_CLIP, length), 0)
    lines = jnp.dot(
        near, pick.astype(F32), preferred_element_type=F32, precision=lax.Precision.HIGHEST
    )
    where = lax.broadcasted_iota(jnp.int32, lines.shape, 1)
    lines = jnp.where((where > end - 2 * REL_CLIP) & (where < end), lines, far)
    chosen = lax.broadcasted_iota(jnp.int32, lines.shape, 0) == x
    line = jnp.sum(jnp.where(chosen, lines, 0.0), axis=0, keepdims=True)
    wide = jnp.broadcast_to(line, (tok, length))
    wide = pltpu.roll(wide, 0, 1, stride=1, stride_axis=0)[:, :window] * LOG2E
    qseg = lax.broadcasted_iota(jnp.int32, (tok, window), 0) // SEG
    kseg = lax.broadcasted_iota(jnp.int32, (tok, window), 1) // SEG
    band_ref[...] = jnp.where((kseg >= qseg) & (kseg <= qseg + LEFT), wide, NEG_FILL)


def attend(block, first_row, qs, ks, vs, band_ref):
    tok, window = band_ref.shape
    head = qs.shape[1]
    at = pl.multiple_of(block * tok, tok)
    query = qs[pl.ds(at, tok), :]
    keys = ks[pl.ds(at, window), :]
    values = vs[pl.ds(at, window), :]
    scores = lax.dot_general(query, keys, NT, preferred_element_type=F32)
    scores = scores * (head**-0.5 * LOG2E) + band_ref[...]
    if first_row is not None:
        column = lax.broadcasted_iota(jnp.int32, (1, window), 1) + block * tok
        hidden = jnp.logical_and(column < REACH, first_row)
        scores = scores + jnp.where(hidden, NEG_FILL, 0.0)
    largest = jnp.max(scores, axis=-1, keepdims=True)
    weights = jnp.exp2(scores - largest)
    total = jnp.sum(weights, axis=-1, keepdims=True)
    mixed = jnp.dot(weights.astype(BF), values, preferred_element_type=F32)
    return (mixed / total).astype(BF)


def attend_rows(side, x, y, qs, ks, vs, band, outs, mixed, ssem, rsem, between):
    tok, head = band.shape[0], qs.shape[1]
    here = pl.ds(pl.multiple_of(x * head, head), head)

    def hand_back(block):
        rows = pl.ds(pl.multiple_of(block * tok, tok), tok)
        return remote(
            outs.at[rows, :], mixed.at[:, here], ssem.at[block], rsem.at[x], sp=y * side + block
        )

    def run(block, first_row):
        result = attend(block, first_row, qs, ks, vs, band)
        outs[pl.ds(pl.multiple_of(block * tok, tok), tok), :] = result

        @pl.when(block != x)
        def _():
            hand_back(block).start()

        @pl.when(block == x)
        def _():
            mixed[:, here] = result

    half = REACH // tok

    def late(i, carry):
        run(i + half, None)
        return carry

    lax.fori_loop(0, side - half, late, 0)
    between()

    def early(i, carry):
        run(i, y == 0)
        return carry

    lax.fori_loop(0, half, early, 0)

    def take_back(then):
        def finish(block, carry):
            @pl.when(block != x)
            def _():
                there = pl.ds(pl.multiple_of(block * head, head), head)
                remote(
                    outs.at[pl.ds(0, tok), :],
                    mixed.at[:, there],
                    ssem.at[block],
                    rsem.at[block],
                    sp=y * side + block,
                ).wait_recv()
                then(block)

            return carry

        lax.fori_loop(0, side, finish, 0)

    def sent():
        def finish(block, carry):
            @pl.when(block != x)
            def _():
                hand_back(block).wait_send()

            return carry

        lax.fori_loop(0, side, finish, 0)

    return take_back, sent


def clear_halo(y, ks, vs):
    @pl.when(y == 0)
    def _():
        ks[pl.ds(0, REACH), :] = jnp.zeros((REACH, ks.shape[1]), BF)
        vs[pl.ds(0, REACH), :] = jnp.zeros((REACH, vs.shape[1]), BF)


class Gather:
    def __init__(self, side, x, y, grp, buf, shared, xr, xl, yu, yd, z):
        self.side, self.x, self.y, self.grp, self.buf = side, x, y, grp, buf
        self.xr, self.xl, self.yu, self.yd, self.z = xr, xl, yu, yd, z
        self.shared = shared
        self.rows = buf.shape[0] // (side * side)
        quarter = buf.shape[1] // 4
        self.plane = lax.rem(grp, 2)
        self.inside = pl.ds(0, buf.shape[1])
        if not shared:
            self.inside = pl.ds(pl.multiple_of(self.plane * quarter, quarter), 3 * quarter)
        self.across = pl.ds(pl.multiple_of(self.plane * 3 * quarter, quarter), quarter)
        self.theirs = pl.ds(pl.multiple_of((1 - self.plane) * 3 * quarter, quarter), quarter)

    def guard(self, step):
        if self.shared:
            return pl.when(lax.rem(self.y + step, 2) == self.plane)
        return lambda run: run()

    def slab(self, xp, yp, columns):
        at = pl.multiple_of((yp * self.side + xp) * self.rows, self.rows)
        return self.buf.at[pl.ds(at, self.rows), columns]

    def column(self, k):
        if isinstance(k, int):
            off = -(k + 1) // 2 if k % 2 else k // 2
        else:
            off = jnp.where(lax.rem(k, 2) == 1, -lax.div(k + 1, 2), lax.div(k, 2))
        return lax.rem(self.x + off + self.side, self.side)

    def xcopy(self, step, right):
        owner = lax.rem(self.x + (-step if right else step) + self.side, self.side)
        to = lax.rem(self.x + (1 if right else self.side - 1), self.side)
        part = self.slab(owner, self.y, self.inside)
        send, recv = self.xr if right else self.xl
        return remote(part, part, send.at[step], recv.at[step], sp=self.y * self.side + to)

    def xarrival(self, step, right):
        owner = lax.rem(self.x + (-step - 1 if right else step + 1) + self.side, self.side)
        part = self.slab(owner, self.y, self.inside)
        send, recv = self.xr if right else self.xl
        return remote(part, part, send.at[step], recv.at[step], sp=self.y * self.side + self.x)

    def ycopy(self, step, k, upward):
        owner = lax.rem(self.y + (-step if upward else step) + self.side, self.side)
        to = lax.rem(self.y + (1 if upward else self.side - 1), self.side)
        part = self.slab(self.column(k), owner, self.inside)
        send, recv = self.yu if upward else self.yd
        return remote(part, part, send.at[step, k], recv.at[step, k], sp=to * self.side + self.x)

    def yarrival(self, step, k, upward):
        owner = lax.rem(self.y + (-step - 1 if upward else step + 1) + self.side, self.side)
        part = self.slab(self.column(k), owner, self.inside)
        send, recv = self.yu if upward else self.yd
        return remote(part, part, send.at[step, k], recv.at[step, k], sp=self.x)

    def zcopy(self, t, k, columns):
        owner = lax.rem(self.y - t + self.side, self.side)
        part = self.slab(self.column(k), owner, columns)
        send, recv = self.z
        return remote(part, part, send.at[t, k], recv.at[t, k], grp=other_plane(self.grp))

    def begin(self):
        @self.guard(0)
        def _():
            self.xcopy(0, True).start()
            self.xcopy(0, False).start()
            if self.shared:
                self.ycopy(0, 0, True).start()
                self.ycopy(0, 0, False).start()

    def xevent(self, k):
        right = k % 2 == 1
        step = (k + 1) // 2 if right else k // 2

        @self.guard(0)
        def _():
            self.xarrival(step - 1, right).wait_recv()
            if step < self.side // 2 - (0 if right else 1):
                self.xcopy(step, right).start()
            if self.shared:
                self.ycopy(0, k, True).start()
                self.ycopy(0, k, False).start()
            else:
                self.zcopy(0, k, self.across).start()

    def ybegin(self, *pieces):
        for k in pieces:
            self.ycopy(0, k, True).start()
            self.ycopy(0, k, False).start()

    def yevent(self, step, base, count):
        side = self.side
        half = side // 2
        far = step == half
        lower = base < half

        def one(k, carry):
            if not far or lower:
                self.yarrival(step - 1, k, True).wait_recv()
                if step < half - 1 or (step == half - 1 and lower):
                    self.ycopy(step, k, True).start()
                if not self.shared:
                    self.zcopy(step, k, self.across).start()
            if not far or not lower:
                self.yarrival(step - 1, k, False).wait_recv()
                if step < half - 1 or (step == half - 1 and not lower):
                    self.ycopy(step, k, False).start()
                if not self.shared:
                    self.zcopy(side - step, k, self.across).start()
            return carry

        @self.guard(step)
        def _():
            lax.fori_loop(base, base + count, one, 0)

    def zevent(self):
        side = self.side

        def one(i, carry):
            t, k = lax.div(i, side), lax.rem(i, side)
            self.zcopy(t, k, self.theirs).wait_recv()
            return carry

        lax.fori_loop(1, side * side, one, 0)

    def sent(self):
        side = self.side
        half = side // 2

        @self.guard(0)
        def _():
            for step in range(half):
                self.xcopy(step, True).wait_send()
                if step < half - 1:
                    self.xcopy(step, False).wait_send()

        for step in range(half):

            def one(k, carry, step=step):
                if step < half - 1:
                    self.ycopy(step, k, True).wait_send()
                    self.ycopy(step, k + half, True).wait_send()
                    self.ycopy(step, k, False).wait_send()
                else:
                    self.ycopy(step, k, True).wait_send()
                self.ycopy(step, k + half, False).wait_send()
                return carry

            @self.guard(step)
            def _(one=one):
                lax.fori_loop(0, half, one, 0)

        def one(i, carry):
            self.zcopy(lax.div(i, side), lax.rem(i, side), self.across).wait_send()
            return carry

        if not self.shared:
            lax.fori_loop(1, side * side, one, 0)


CUTS = 4


def layers_kernel(side, names, *refs):
    r = dict(zip(names, refs))
    x, y, c = place(side)
    grp = lax.axis_index("grp")
    plane = lax.rem(grp, 2)
    q_ref, k_ref, v_ref = r["q"], r["k"], r["v"]
    tok, width = q_ref.shape
    head = width // side
    wall = r["wall"]
    wrow = r["wq"].shape[0]
    group = side * wrow
    model = r["w1"].shape[0]
    other = 1 - c
    half = tok // 2
    steps = side // 2
    up = lax.rem(y + 1, side) * side + x
    down = lax.rem(y + side - 1, side) * side + x
    right = y * side + lax.rem(x + 1, side)
    left = y * side + lax.rem(x + side - 1, side)

    meet = greet(side, x, y, c, grp)
    own = pl.ds(pl.multiple_of((y * side + x) * wrow, wrow), wrow)
    loads = [
        pltpu.make_async_copy(r["o1"], r["w1"].at[own, :], r["loads"].at[0]),
        pltpu.make_async_copy(r["o2"], r["w2"].at[own, :], r["loads"].at[1]),
        pltpu.make_async_copy(
            r["resid_any"].at[pl.ds(pl.multiple_of(c * half, half), half), :],
            r["resid"],
            r["loads"].at[2],
        ),
    ]
    for load in loads:
        load.start()
    g1, g2 = [
        Gather(
            side, x, y, grp, r[f"w{i}"], i == 1,
            *((r[f"s{kind}{i}"], r[f"r{kind}{i}"]) for kind in ("xr", "xl", "yu", "yd", "z")),
        )
        for i in (1, 2)
    ]

    mine = pl.ds(pl.multiple_of(x * tok, tok), tok)
    mine_late = pl.ds(pl.multiple_of(REACH + x * tok, tok), tok)
    kinds = [
        (k_ref, r["ks1"].at[mine_late, :]),
        (v_ref, r["vs1"].at[mine_late, :]),
        (q_ref, r["qs1"].at[mine, :]),
    ] + [(r[f"w{n}"], wall.at[own, pl.ds(i * head, head)]) for i, n in enumerate("qkv")]

    def piece(kind, d):
        peer = lax.rem(x + d, side)
        src, dst = kinds[kind]
        cut = src.at[:, pl.ds(pl.multiple_of(peer * head, head), head)]
        if d == 0:
            return pltpu.make_async_copy(cut, dst, r["ra2a"].at[kind, 0])
        send, recv = r["sa2a"].at[kind, d], r["ra2a"].at[kind, d]
        return remote(cut, dst, send, recv, sp=y * side + peer)

    for kind in range(3):
        piece(kind, 0).start()
    in_plane = lax.div(x, steps) == plane

    @pl.when(in_plane)
    def _():
        for kind in range(3, 6):
            piece(kind, 0).start()

    spread_bias(r["rel1"], r["band1"], x)
    spread_bias(r["rel2"], r["band2"], x)
    clear_halo(y, r["ks1"], r["vs1"])
    clear_halo(y, r["ks2"], r["vs2"])
    for load in loads:
        load.wait()
    meet()

    def take(kind):
        piece(kind, 0).wait()
        for d in range(1, side):
            piece(kind, d).wait_recv()

    def ring_rows(owner, parity):
        return pl.ds(pl.multiple_of(owner * group + parity * (group // 2), group // 2), group // 2)

    def ring(step, upward):
        owner = lax.rem(y + (-step if upward else step) + side, side)
        part = wall.at[ring_rows(owner, plane), :]
        send, recv = (r["squ"], r["rqu"]) if upward else (r["sqd"], r["rqd"])
        return remote(part, part, send.at[step], recv.at[step], sp=up if upward else down)

    def cross(t, parity):
        owner = lax.rem(y - t + side, side)
        part = wall.at[ring_rows(owner, parity), :]
        return remote(part, part, r["sqz"].at[t], r["rqz"].at[t], grp=other_plane(grp))

    def relay(step):
        if step == 0:
            @pl.when(in_plane)
            def _():
                for kind in range(3, 6):
                    piece(kind, 0).wait()

            for d in range(1, side):
                @pl.when(lax.div(lax.rem(x - d + side, side), steps) == plane)
                def _(d=d):
                    for kind in range(3, 6):
                        piece(kind, d).wait_recv()

        if step > 0:
            ring(step - 1, True).wait_recv()
        if step < steps:
            ring(step, True).start()
        if step > 0:
            cross(step, plane).start()
        if 0 < step < steps:
            ring(step - 1, False).wait_recv()
        if 0 < step < steps:
            cross(side - step, plane).start()
        if step < steps - 1:
            ring(step, False).start()

    g1.begin()

    opposite = side // 2
    odd = lax.rem(x, 2) == 1
    far_x = lax.rem(x + opposite, side)
    far_cut = pl.ds(pl.multiple_of(far_x * head, head), head)
    behind = pl.ds(pl.multiple_of(REACH + lax.rem(x + 1, side) * tok, tok), tok)
    behind_q = pl.ds(pl.multiple_of(lax.rem(x + 1, side) * tok, tok), tok)

    def detour(kind):
        src = v_ref if kind == 1 else q_ref
        return remote(
            src.at[:, far_cut], r["via"].at[kind - 1], r["sv"].at[kind, 0], r["rv"].at[kind - 1],
            sp=left,
        )

    def onward(kind):
        dst = r["vs1"].at[behind, :] if kind == 1 else r["qs1"].at[behind_q, :]
        return remote(
            r["via"].at[kind - 1], dst, r["sv"].at[kind, 1], r["ra2a"].at[kind, opposite],
            sp=y * side + lax.rem(x + opposite + 1, side),
        )

    def hand_out(kinds, distances):
        for d in distances:
            for kind in kinds:
                piece(kind, d).start()

    near, third = [1, side - 1, 2, side - 2], [3, side - 3]
    hand_out([0], near)
    g1.xevent(1)
    g1.xevent(2)
    hand_out([1], near)
    detour(1).start()
    g1.xevent(3)
    g1.xevent(4)
    hand_out([0], third + [opposite])
    g1.yevent(1, 0, 2)
    g1.xevent(5)
    g1.xevent(6)
    hand_out([1], third)
    detour(1).wait_recv()
    onward(1).start()

    @pl.when(odd)
    def _():
        detour(2).start()

    @pl.when(jnp.logical_not(odd))
    def _():
        hand_out([2], [opposite])

    hand_out([2], third + near)

    @pl.when(in_plane)
    def _():
        hand_out([3, 4, 5], range(1, side))

    g1.yevent(1, 2, 2)
    g1.yevent(2, 0, 2)
    g1.xevent(7)

    @pl.when(jnp.logical_not(odd))
    def _():
        detour(2).wait_recv()
        onward(2).start()

    g2.begin()

    g1.yevent(1, 4, 2)
    g1.yevent(2, 2, 2)
    g1.yevent(3, 0, 2)
    g1.yevent(1, 6, 2)
    g1.yevent(2, 4, 2)
    g1.yevent(3, 2, 2)
    take(0)
    take(1)
    halo1 = [
        remote(
            a.at[pl.ds(side * tok, REACH), :], a.at[pl.ds(0, REACH), :],
            r["sh1"].at[i], r["rh1"].at[i], sp=up,
        )
        for i, a in enumerate((r["ks1"], r["vs1"]))
    ]

    @pl.when(y < side - 1)
    def _():
        for copy in halo1:
            copy.start()

    take(2)

    def between():
        g1.yevent(2, 6, 2)
        g1.yevent(3, 4, 2)
        g2.xevent(1)
        g2.xevent(2)
        @pl.when(y > 0)
        def _():
            for copy in halo1:
                copy.wait_recv()


    take_back, back1 = attend_rows(
        side, x, y, r["qs1"], r["ks1"], r["vs1"], r["band1"], r["outs1"], r["mixed1"],
        r["sb1"], r["rb1"], between,
    )
    g1.yevent(3, 6, 2)
    relay(0)
    g2.xevent(3)
    g2.xevent(4)
    g1.yevent(4, 0, 4)
    g1.yevent(4, 4, 4)
    mixed1, mixedz = r["mixed1"], r["mixedz"]

    def lend(block):
        there = pl.ds(pl.multiple_of(block * head, head), head)
        return remote(
            mixed1.at[:, there], mixedz.at[:, there], r["smz"].at[block], r["rmz"].at[block],
            grp=other_plane(grp),
        )

    lend(x).start()
    take_back(lambda block: lend(block).start())

    n = group
    part1, partz, terms = r["part1"], r["partz"], r["terms1"]
    my_half = pl.ds(pl.multiple_of(c * half, half), half)
    their_half = pl.ds(pl.multiple_of(other * half, half), half)

    def columns(j):
        return pl.ds(pl.multiple_of((2 * j + plane) * n, n), n)

    swaps, same, diagonal = [], [], []
    for j in range(steps):
        at, lent = columns(j), (r["srz"], r["rrz"])
        swaps.append(
            remote(
                part1.at[their_half, at], terms.at[1, :, at], r["sp1"].at[j], r["rp1"].at[j],
                tp=other,
            )
        )
        same.append(
            remote(
                partz.at[my_half, at], terms.at[0, :, at], lent[0].at[0, j], lent[1].at[0, j],
                grp=other_plane(grp),
            )
        )
        diagonal.append(
            remote(
                partz.at[their_half, at], terms.at[1, :, at], lent[0].at[1, j], lent[1].at[1, j],
                grp=other_plane(grp), tp=other,
            )
        )

    def out1(rows, j):
        return lax.dot_general(
            rows[...], r["w1"][columns(j), :], NT, preferred_element_type=F32
        ).astype(BF)

    for j in range(steps):
        part1[:, columns(j)] = out1(mixed1, j)
        swaps[j].start()
        terms[0, :, columns(j)] = part1[my_half, columns(j)]
    g2.xevent(5)
    g2.xevent(6)
    for block in range(side):
        lend(block).wait_recv()
    for j in range(steps):
        partz[:, columns(j)] = out1(mixedz, j)
        same[j].start()
        diagonal[j].start()
    cross(0, plane).start()
    relay(1)
    g2.ybegin(0, 1, 2, 3)
    for copy in swaps + same + diagonal:
        copy.wait_recv()

    inp, hid = r["inp"], r["hid"]
    chunk = half // 2

    def rows_of(owner, core, i):
        return pl.ds(pl.multiple_of(owner * tok + core * half + i * chunk, chunk), chunk)

    def away(step):
        return lax.rem(x + step + side, side)

    def spread(owner, send, recv, **to):
        return lambda step, i: remote(
            inp.at[rows_of(owner(step), c, i), :], inp.at[rows_of(owner(step), c, i), :],
            send.at[step, i], recv.at[step, i], **to,
        )

    pass_right = spread(lambda s: away(-s), r["sr"], r["rr"], sp=right)
    pass_left = spread(lambda s: away(s), r["sl"], r["rl"], sp=left)
    from_left = spread(lambda s: away(-s - 1), r["sr"], r["rr"], sp=right)
    from_right = spread(lambda s: away(s + 1), r["sl"], r["rl"], sp=left)

    def share(offset, i, core):
        rows = rows_of(away(offset), core, i)
        slot = offset % side
        return remote(
            inp.at[rows, :], inp.at[rows, :], r["sd"].at[slot, i], r["rd"].at[slot, i], tp=other
        )

    def show(i, core):
        rows = rows_of(0, core, i)
        return remote(hid.at[rows, :], hid.at[rows, :], r["sw"].at[i], r["rw"].at[i], tp=other)

    for i in range(2):
        rows = rows_of(0, c, i)
        sub = pl.ds(i * chunk, chunk)
        branch = terms[0, sub, :].astype(F32) + terms[1, sub, :].astype(F32)
        branch = branch.astype(BF).astype(F32)
        scale = lax.rsqrt(jnp.mean(branch * branch, axis=-1, keepdims=True) + EPS)
        hidden = (r["resid"][sub, :].astype(F32) + branch * scale * r["post1"][...]).astype(BF)
        hid[rows, :] = hidden
        long = hidden.astype(F32)
        scale = lax.rsqrt(jnp.mean(long * long, axis=-1, keepdims=True) + EPS)
        inp[rows_of(x, c, i), :] = (long * scale * r["pre2"][...]).astype(BF)
        pass_right(0, i).start()
        pass_left(0, i).start()
        share(0, i, c).start()
        show(i, c).start()

    shift = REACH // tok
    qs2, ks2, vs2 = r["qs2"], r["ks2"], r["vs2"]

    def halo2(owner):
        slot = owner - (side - shift)
        rows = pl.ds(pl.multiple_of(REACH + owner * tok, tok), tok)
        dest = pl.ds(pl.multiple_of(slot * tok, tok), tok)
        return [
            remote(
                a.at[rows, :], a.at[dest, :], r["sh2"].at[i, slot], r["rh2"].at[i, slot], sp=up
            )
            for i, a in enumerate((ks2, vs2))
        ]

    def qkv(offset):
        for i in range(2):
            share(offset, i, other).wait_recv()
        owner = away(offset)
        rows = pl.ds(pl.multiple_of(owner * tok, tok), tok)
        late = pl.ds(pl.multiple_of(REACH + owner * tok, tok), tok)
        done = jnp.dot(inp[rows, :], wall[...], preferred_element_type=F32).astype(BF)
        qs2[rows, :] = done[:, :head]
        ks2[late, :] = done[:, head : 2 * head]
        vs2[late, :] = done[:, 2 * head :]

        @pl.when(jnp.logical_and(owner >= side - shift, y < side - 1))
        def _():
            for copy in halo2(owner):
                copy.start()

    relay(2)
    g2.ybegin(4, 5, 6)
    g2.xevent(7)
    last = steps - 1

    def fill(step, i):
        if (step, i) == (1, 0):
            relay(3)
            g2.ybegin(7)
        elif (step, i) == (1, 1):
            relay(4)
        elif (step, i) == (2, 0):
            g2.yevent(1, 0, 4)
        elif (step, i) == (2, 1):
            g2.yevent(1, 4, 4)
            for t in range(side):
                cross(t, 1 - plane).wait_recv()
            qkv(0)
            qkv(-1)
            qkv(1)
        elif (step, i) == (3, 0):
            qkv(-2)
            qkv(2)
            g2.yevent(2, 0, 4)

    for step in range(1, steps):
        for i in range(2):
            from_left(step - 1, i).wait_recv()
            if step < last or i == 0:
                pass_right(step, i).start()
            share(-step, i, c).start()
            from_right(step - 1, i).wait_recv()
            if step < last or i == 1:
                pass_left(step, i).start()
            share(step, i, c).start()
            fill(step, i)
    qkv(-last)
    qkv(last)
    from_left(last, 0).wait_recv()
    share(steps, 0, c).start()
    from_right(last, 1).wait_recv()
    share(steps, 1, c).start()
    qkv(steps)

    g2.yevent(2, 4, 4)

    def between2():
        @pl.when(y > 0)
        def _():
            for k in range(shift):
                for copy in halo2(side - shift + k):
                    copy.wait_recv()

        g2.yevent(3, 0, 4)

    take_back, back2 = attend_rows(
        side, x, y, qs2, ks2, vs2, r["band2"], r["outs2"], r["mixed2"], r["sb2"], r["rb2"],
        between2,
    )
    g2.yevent(3, 4, 4)
    g2.yevent(4, 0, 4)
    for i in range(2):
        show(i, other).wait_recv()
    take_back(lambda block: None)
    g2.yevent(4, 4, 4)
    for kind in range(3):
        for d in range(1, side):
            if kind == 0 or d != opposite:
                piece(kind, d).wait_send()
    detour(1).wait_send()
    onward(1).wait_send()

    @pl.when(odd)
    def _():
        detour(2).wait_send()

    @pl.when(jnp.logical_not(odd))
    def _():
        onward(2).wait_send()
        piece(2, opposite).wait_send()

    @pl.when(in_plane)
    def _():
        for kind in range(3, 6):
            for d in range(1, side):
                piece(kind, d).wait_send()

    for step in range(steps):
        ring(step, True).wait_send()
        if step < last:
            ring(step, False).wait_send()
    for t in range(side):
        cross(t, plane).wait_send()
    g1.sent()
    back1()
    for copy in swaps + same + diagonal:
        copy.wait_send()
    for block in range(side):
        lend(block).wait_send()
    for step in range(steps):
        for i in range(2):
            if step < last or i == 0:
                pass_right(step, i).wait_send()
            if step < last or i == 1:
                pass_left(step, i).wait_send()
    for i in range(2):
        show(i, c).wait_send()
        for offset in range(side):
            share(offset, i, c).wait_send()

    @pl.when(y < side - 1)
    def _():
        for copy in halo1:
            copy.wait_send()
        for k in range(shift):
            for copy in halo2(side - shift + k):
                copy.wait_send()

    g2.sent()
    back2()
    g2.zevent()

    part2, theirs2 = r["part2"], r["theirs2"]
    n = model // CUTS
    swaps2 = [
        remote(
            part2.at[:, pl.ds(i * n, n)], theirs2.at[:, pl.ds(i * n, n)],
            r["sp2"].at[i], r["rp2"].at[i], tp=other,
        )
        for i in range(CUTS)
    ]
    for i in range(CUTS):
        done = lax.dot_general(
            r["mixed2"][...], r["w2"][pl.ds(i * n, n), :], NT, preferred_element_type=F32
        )
        part2[:, pl.ds(i * n, n)] = done.astype(BF)
        swaps2[i].start()
    for copy in swaps2:
        copy.wait_recv()
    for i in range(tok // chunk):
        sub = pl.ds(i * chunk, chunk)
        branch = part2[sub, :].astype(F32) + theirs2[sub, :].astype(F32)
        branch = branch.astype(BF).astype(F32)
        scale = lax.rsqrt(jnp.mean(branch * branch, axis=-1, keepdims=True) + EPS)
        done = hid[sub, :].astype(F32) + branch * scale * r["post2"][...]
        r["out"][sub, :] = done.astype(BF)

    for copy in swaps2:
        copy.wait_send()


def shards(
    side, resid, queries_first, keys_first, values_first, rel_first, post_first, out_first,
    pre_second, query_weight, key_weight, value_weight, rel_second, post_second, out_second,
):
    tok, width = queries_first.shape
    model = resid.shape[1]
    head = width // rel_first.shape[0]
    rows = side * tok
    steps = side // 2
    inputs = {
        "q": (queries_first, ANY),
        "k": (keys_first, ANY),
        "v": (values_first, ANY),
        "rel1": (rel_first, VM),
        "rel2": (rel_second, VM),
        "o1": (out_first.T, ANY),
        "o2": (out_second.T, ANY),
        "resid_any": (resid, ANY),
        "post1": (post_first[None], VM),
        "pre2": (pre_second[None], VM),
        "post2": (post_second[None], VM),
        "wq": (query_weight, ANY),
        "wk": (key_weight, ANY),
        "wv": (value_weight, ANY),
    }

    def vmem(*dims):
        return pltpu.VMEM(dims, BF)

    def dma(*dims):
        return pltpu.SemaphoreType.DMA(dims)

    scratch = {
        "wall": vmem(model, 3 * head),
        "inp": vmem(rows, model),
        "hid": vmem(tok, model),
        "resid": vmem(tok // 2, model),
        "terms1": vmem(2, tok // 2, model),
        "mixedz": vmem(tok, width),
        "partz": vmem(tok, model),
        "theirs2": vmem(tok, model),
        "loads": dma(3),
        "via": vmem(2, tok, head),
        "sv": dma(3, 2),
        "rv": dma(2),
        "sa2a": dma(6, side),
        "ra2a": dma(6, side),
    }
    for i in (1, 2):
        scratch[f"w{i}"] = vmem(model, width)
        scratch[f"qs{i}"] = vmem(rows, head)
        scratch[f"ks{i}"] = vmem(rows + REACH, head)
        scratch[f"vs{i}"] = vmem(rows + REACH, head)
        scratch[f"outs{i}"] = vmem(rows, head)
        scratch[f"mixed{i}"] = vmem(tok, width)
        scratch[f"part{i}"] = vmem(tok, model)
        scratch[f"band{i}"] = pltpu.VMEM((tok, tok + REACH), F32)
    for d in "sr":
        for i in (1, 2):
            scratch[f"{d}xr{i}"] = dma(steps)
            scratch[f"{d}xl{i}"] = dma(steps)
            scratch[f"{d}yu{i}"] = dma(steps, side)
            scratch[f"{d}yd{i}"] = dma(steps, side)
            scratch[f"{d}z{i}"] = dma(side, side)
            scratch[f"{d}b{i}"] = dma(side)
            scratch[f"{d}p{i}"] = dma(CUTS)
        scratch[f"{d}mz"] = dma(side)
        scratch[f"{d}rz"] = dma(2, steps)
        scratch[f"{d}qu"] = dma(steps)
        scratch[f"{d}qd"] = dma(steps)
        scratch[f"{d}qz"] = dma(side)
        scratch[f"{d}h1"] = dma(2)
        scratch[f"{d}h2"] = dma(2, REACH // tok)
        scratch[f"{d}r"] = dma(steps, 2)
        scratch[f"{d}l"] = dma(steps, 2)
        scratch[f"{d}d"] = dma(side, 2)
        scratch[f"{d}w"] = dma(2)
    return pl.pallas_call(
        functools.partial(layers_kernel, side, [*inputs, "out", *scratch]),
        out_shape=jax.ShapeDtypeStruct((tok, model), BF),
        in_specs=[spec for _, spec in inputs.values()],
        out_specs=VM,
        scratch_shapes=list(scratch.values()),
        compiler_params=pltpu.CompilerParams(has_side_effects=True, collective_id=0),
    )(*(value for value, _ in inputs.values()))


def solution(mesh):
    side = math.isqrt(mesh.shape["sp"])
    in_specs = (
        P(("grp", "sp"), None),
        P(("grp", "sp"), "tp"),
        P(("grp", "sp"), "tp"),
        P(("grp", "sp"), "tp"),
        P("tp", None),
        P(),
        P("tp", "sp"),
        P(),
        P("sp", "tp"),
        P("sp", "tp"),
        P("sp", "tp"),
        P("tp", None),
        P(),
        P("tp", "sp"),
    )
    out_specs = P(("grp", "sp"), None)
    return jax.shard_map(
        functools.partial(shards, side),
        mesh=mesh,
        in_specs=in_specs,
        out_specs=out_specs,
        check_vma=False,
    )
```

```python
import functools
import math

import jax
import jax.numpy as jnp
from jax import lax
from jax.experimental import pallas as pl
from jax.experimental.pallas import tpu as pltpu
from jax.sharding import PartitionSpec as P

SEG = 64
LEFT = 8
REACH = 512
REL_CLIP = 128
EPS = 1e-06
NEG_FILL = -1e30
LOG2E = 1.4426950408889634
BF = jnp.bfloat16
F32 = jnp.float32
MESH = pl.DeviceIdType.MESH
VM = pl.BlockSpec(memory_space=pltpu.VMEM)
ANY = pl.BlockSpec(memory_space=pl.ANY)
NT = (((1,), (1,)), ((), ()))


def place(side):
    sp = lax.axis_index("sp")
    return lax.rem(sp, side), lax.div(sp, side), lax.axis_index("tp")


def remote(src, dst, send, recv, **where):
    return pltpu.make_async_remote_copy(
        src_ref=src,
        dst_ref=dst,
        send_sem=send,
        recv_sem=recv,
        device_id=dict(where),
        device_id_type=MESH,
    )


def greet(side, x, y, c, grp):
    barrier = pltpu.get_barrier_semaphore()
    peers = [{"sp": y * side + lax.rem(x + d, side)} for d in range(1, side)]
    peers += [{"sp": lax.rem(y + d, side) * side + x} for d in (1, side - 1)]
    peers += [{"tp": 1 - c}]
    peers += [{"grp": other_plane(grp)}]
    for peer in peers:
        pl.semaphore_signal(barrier, inc=1, device_id=peer, device_id_type=MESH)
    return lambda: pl.semaphore_wait(barrier, len(peers))


def other_plane(grp):
    return grp + 1 - 2 * lax.rem(grp, 2)


def spread_bias(table_ref, band_ref, x):
    tok, window = band_ref.shape
    length = window + tok
    near = table_ref[:, : 2 * REL_CLIP]
    far = table_ref[:, 2 * REL_CLIP :]
    end = REACH + REL_CLIP
    slot = end - lax.broadcasted_iota(jnp.int32, (2 * REL_CLIP, length), 1)
    pick = slot == lax.broadcasted_iota(jnp.int32, (2 * REL_CLIP, length), 0)
    lines = jnp.dot(
        near, pick.astype(F32), preferred_element_type=F32, precision=lax.Precision.HIGHEST
    )
    where = lax.broadcasted_iota(jnp.int32, lines.shape, 1)
    lines = jnp.where((where > end - 2 * REL_CLIP) & (where < end), lines, far)
    chosen = lax.broadcasted_iota(jnp.int32, lines.shape, 0) == x
    line = jnp.sum(jnp.where(chosen, lines, 0.0), axis=0, keepdims=True)
    wide = jnp.broadcast_to(line, (tok, length))
    wide = pltpu.roll(wide, 0, 1, stride=1, stride_axis=0)[:, :window] * LOG2E
    qseg = lax.broadcasted_iota(jnp.int32, (tok, window), 0) // SEG
    kseg = lax.broadcasted_iota(jnp.int32, (tok, window), 1) // SEG
    band_ref[...] = jnp.where((kseg >= qseg) & (kseg <= qseg + LEFT), wide, NEG_FILL)


def attend(block, first_row, qs, ks, vs, band_ref):
    tok, window = band_ref.shape
    head = qs.shape[1]
    at = pl.multiple_of(block * tok, tok)
    query = qs[pl.ds(at, tok), :]
    keys = ks[pl.ds(at, window), :]
    values = vs[pl.ds(at, window), :]
    scores = lax.dot_general(query, keys, NT, preferred_element_type=F32)
    scores = scores * (head**-0.5 * LOG2E) + band_ref[...]
    if first_row is not None:
        column = lax.broadcasted_iota(jnp.int32, (1, window), 1) + block * tok
        hidden = jnp.logical_and(column < REACH, first_row)
        scores = scores + jnp.where(hidden, NEG_FILL, 0.0)
    largest = jnp.max(scores, axis=-1, keepdims=True)
    weights = jnp.exp2(scores - largest)
    total = jnp.sum(weights, axis=-1, keepdims=True)
    mixed = jnp.dot(weights.astype(BF), values, preferred_element_type=F32)
    return (mixed / total).astype(BF)


def attend_rows(side, x, y, qs, ks, vs, band, outs, mixed, ssem, rsem, between):
    tok, head = band.shape[0], qs.shape[1]
    here = pl.ds(pl.multiple_of(x * head, head), head)

    def hand_back(block):
        rows = pl.ds(pl.multiple_of(block * tok, tok), tok)
        return remote(
            outs.at[rows, :], mixed.at[:, here], ssem.at[block], rsem.at[x], sp=y * side + block
        )

    def run(block, first_row):
        result = attend(block, first_row, qs, ks, vs, band)
        outs[pl.ds(pl.multiple_of(block * tok, tok), tok), :] = result

        @pl.when(block != x)
        def _():
            hand_back(block).start()

        @pl.when(block == x)
        def _():
            mixed[:, here] = result

    half = REACH // tok

    def late(i, carry):
        run(i + half, None)
        return carry

    lax.fori_loop(0, side - half, late, 0)
    between()

    def early(i, carry):
        run(i, y == 0)
        return carry

    lax.fori_loop(0, half, early, 0)

    def take_back(then):
        def finish(block, carry):
            @pl.when(block != x)
            def _():
                there = pl.ds(pl.multiple_of(block * head, head), head)
                remote(
                    outs.at[pl.ds(0, tok), :],
                    mixed.at[:, there],
                    ssem.at[block],
                    rsem.at[block],
                    sp=y * side + block,
                ).wait_recv()
                then(block)

            return carry

        lax.fori_loop(0, side, finish, 0)

    def sent():
        def finish(block, carry):
            @pl.when(block != x)
            def _():
                hand_back(block).wait_send()

            return carry

        lax.fori_loop(0, side, finish, 0)

    return take_back, sent


def clear_halo(y, ks, vs):
    @pl.when(y == 0)
    def _():
        ks[pl.ds(0, REACH), :] = jnp.zeros((REACH, ks.shape[1]), BF)
        vs[pl.ds(0, REACH), :] = jnp.zeros((REACH, vs.shape[1]), BF)


class Gather:
    def __init__(self, side, x, y, grp, buf, shared, xr, xl, yu, yd, z):
        self.side, self.x, self.y, self.grp, self.buf = side, x, y, grp, buf
        self.xr, self.xl, self.yu, self.yd, self.z = xr, xl, yu, yd, z
        self.shared = shared
        self.rows = buf.shape[0] // (side * side)
        quarter = buf.shape[1] // 4
        self.plane = lax.rem(grp, 2)
        self.inside = pl.ds(0, buf.shape[1])
        if not shared:
            self.inside = pl.ds(pl.multiple_of(self.plane * quarter, quarter), 3 * quarter)
        self.across = pl.ds(pl.multiple_of(self.plane * 3 * quarter, quarter), quarter)
        self.theirs = pl.ds(pl.multiple_of((1 - self.plane) * 3 * quarter, quarter), quarter)

    def guard(self, step):
        if self.shared:
            return pl.when(lax.rem(self.y + step, 2) == self.plane)
        return lambda run: run()

    def slab(self, xp, yp, columns):
        at = pl.multiple_of((yp * self.side + xp) * self.rows, self.rows)
        return self.buf.at[pl.ds(at, self.rows), columns]

    def column(self, k):
        if isinstance(k, int):
            off = -(k + 1) // 2 if k % 2 else k // 2
        else:
            off = jnp.where(lax.rem(k, 2) == 1, -lax.div(k + 1, 2), lax.div(k, 2))
        return lax.rem(self.x + off + self.side, self.side)

    def xcopy(self, step, right):
        owner = lax.rem(self.x + (-step if right else step) + self.side, self.side)
        to = lax.rem(self.x + (1 if right else self.side - 1), self.side)
        part = self.slab(owner, self.y, self.inside)
        send, recv = self.xr if right else self.xl
        return remote(part, part, send.at[step], recv.at[step], sp=self.y * self.side + to)

    def xarrival(self, step, right):
        owner = lax.rem(self.x + (-step - 1 if right else step + 1) + self.side, self.side)
        part = self.slab(owner, self.y, self.inside)
        send, recv = self.xr if right else self.xl
        return remote(part, part, send.at[step], recv.at[step], sp=self.y * self.side + self.x)

    def ycopy(self, step, k, upward):
        owner = lax.rem(self.y + (-step if upward else step) + self.side, self.side)
        to = lax.rem(self.y + (1 if upward else self.side - 1), self.side)
        part = self.slab(self.column(k), owner, self.inside)
        send, recv = self.yu if upward else self.yd
        return remote(part, part, send.at[step, k], recv.at[step, k], sp=to * self.side + self.x)

    def yarrival(self, step, k, upward):
        owner = lax.rem(self.y + (-step - 1 if upward else step + 1) + self.side, self.side)
        part = self.slab(self.column(k), owner, self.inside)
        send, recv = self.yu if upward else self.yd
        return remote(part, part, send.at[step, k], recv.at[step, k], sp=self.x)

    def zcopy(self, t, k, columns):
        owner = lax.rem(self.y - t + self.side, self.side)
        part = self.slab(self.column(k), owner, columns)
        send, recv = self.z
        return remote(part, part, send.at[t, k], recv.at[t, k], grp=other_plane(self.grp))

    def begin(self):
        @self.guard(0)
        def _():
            self.xcopy(0, True).start()
            self.xcopy(0, False).start()
            if self.shared:
                self.ycopy(0, 0, True).start()
                self.ycopy(0, 0, False).start()

    def xevent(self, k):
        right = k % 2 == 1
        step = (k + 1) // 2 if right else k // 2

        @self.guard(0)
        def _():
            self.xarrival(step - 1, right).wait_recv()
            if step < self.side // 2 - (0 if right else 1):
                self.xcopy(step, right).start()
            if self.shared:
                self.ycopy(0, k, True).start()
                self.ycopy(0, k, False).start()
            else:
                self.zcopy(0, k, self.across).start()

    def ybegin(self, *pieces):
        for k in pieces:
            self.ycopy(0, k, True).start()
            self.ycopy(0, k, False).start()

    def yevent(self, step, base, count):
        side = self.side
        half = side // 2
        far = step == half
        lower = base < half

        def one(k, carry):
            if not far or lower:
                self.yarrival(step - 1, k, True).wait_recv()
                if step < half - 1 or (step == half - 1 and lower):
                    self.ycopy(step, k, True).start()
                if not self.shared:
                    self.zcopy(step, k, self.across).start()
            if not far or not lower:
                self.yarrival(step - 1, k, False).wait_recv()
                if step < half - 1 or (step == half - 1 and not lower):
                    self.ycopy(step, k, False).start()
                if not self.shared:
                    self.zcopy(side - step, k, self.across).start()
            return carry

        @self.guard(step)
        def _():
            lax.fori_loop(base, base + count, one, 0)

    def zevent(self):
        side = self.side

        def one(i, carry):
            t, k = lax.div(i, side), lax.rem(i, side)
            self.zcopy(t, k, self.theirs).wait_recv()
            return carry

        lax.fori_loop(1, side * side, one, 0)

    def sent(self):
        side = self.side
        half = side // 2

        @self.guard(0)
        def _():
            for step in range(half):
                self.xcopy(step, True).wait_send()
                if step < half - 1:
                    self.xcopy(step, False).wait_send()

        for step in range(half):

            def one(k, carry, step=step):
                if step < half - 1:
                    self.ycopy(step, k, True).wait_send()
                    self.ycopy(step, k + half, True).wait_send()
                    self.ycopy(step, k, False).wait_send()
                else:
                    self.ycopy(step, k, True).wait_send()
                self.ycopy(step, k + half, False).wait_send()
                return carry

            @self.guard(step)
            def _(one=one):
                lax.fori_loop(0, half, one, 0)

        def one(i, carry):
            self.zcopy(lax.div(i, side), lax.rem(i, side), self.across).wait_send()
            return carry

        if not self.shared:
            lax.fori_loop(1, side * side, one, 0)


CUTS = 4


def layers_kernel(side, names, *refs):
    r = dict(zip(names, refs))
    x, y, c = place(side)
    grp = lax.axis_index("grp")
    plane = lax.rem(grp, 2)
    q_ref, k_ref, v_ref = r["q"], r["k"], r["v"]
    tok, width = q_ref.shape
    head = width // side
    wall = r["wall"]
    wrow = r["wq"].shape[0]
    group = side * wrow
    model = r["w1"].shape[0]
    other = 1 - c
    half = tok // 2
    steps = side // 2
    up = lax.rem(y + 1, side) * side + x
    down = lax.rem(y + side - 1, side) * side + x
    right = y * side + lax.rem(x + 1, side)
    left = y * side + lax.rem(x + side - 1, side)

    meet = greet(side, x, y, c, grp)
    own = pl.ds(pl.multiple_of((y * side + x) * wrow, wrow), wrow)
    loads = [
        pltpu.make_async_copy(r["o1"], r["w1"].at[own, :], r["loads"].at[0]),
        pltpu.make_async_copy(r["o2"], r["w2"].at[own, :], r["loads"].at[1]),
        pltpu.make_async_copy(
            r["resid_any"].at[pl.ds(pl.multiple_of(c * half, half), half), :],
            r["resid"],
            r["loads"].at[2],
        ),
    ]
    for load in loads:
        load.start()
    g1, g2 = [
        Gather(
            side, x, y, grp, r[f"w{i}"], i == 1,
            *((r[f"s{kind}{i}"], r[f"r{kind}{i}"]) for kind in ("xr", "xl", "yu", "yd", "z")),
        )
        for i in (1, 2)
    ]

    mine = pl.ds(pl.multiple_of(x * tok, tok), tok)
    mine_late = pl.ds(pl.multiple_of(REACH + x * tok, tok), tok)
    kinds = [
        (k_ref, r["ks1"].at[mine_late, :]),
        (v_ref, r["vs1"].at[mine_late, :]),
        (q_ref, r["qs1"].at[mine, :]),
    ] + [(r[f"w{n}"], wall.at[own, pl.ds(i * head, head)]) for i, n in enumerate("qkv")]

    def piece(kind, d):
        peer = lax.rem(x + d, side)
        src, dst = kinds[kind]
        cut = src.at[:, pl.ds(pl.multiple_of(peer * head, head), head)]
        if d == 0:
            return pltpu.make_async_copy(cut, dst, r["ra2a"].at[kind, 0])
        send, recv = r["sa2a"].at[kind, d], r["ra2a"].at[kind, d]
        return remote(cut, dst, send, recv, sp=y * side + peer)

    for kind in range(3):
        piece(kind, 0).start()
    in_plane = lax.div(x, steps) == plane

    @pl.when(in_plane)
    def _():
        for kind in range(3, 6):
            piece(kind, 0).start()

    spread_bias(r["rel1"], r["band1"], x)
    spread_bias(r["rel2"], r["band2"], x)
    clear_halo(y, r["ks1"], r["vs1"])
    clear_halo(y, r["ks2"], r["vs2"])
    for load in loads:
        load.wait()
    meet()

    def take(kind):
        piece(kind, 0).wait()
        for d in range(1, side):
            piece(kind, d).wait_recv()

    def ring_rows(owner, parity):
        return pl.ds(pl.multiple_of(owner * group + parity * (group // 2), group // 2), group // 2)

    def ring(step, upward):
        owner = lax.rem(y + (-step if upward else step) + side, side)
        part = wall.at[ring_rows(owner, plane), :]
        send, recv = (r["squ"], r["rqu"]) if upward else (r["sqd"], r["rqd"])
        return remote(part, part, send.at[step], recv.at[step], sp=up if upward else down)

    def cross(t, parity):
        owner = lax.rem(y - t + side, side)
        part = wall.at[ring_rows(owner, parity), :]
        return remote(part, part, r["sqz"].at[t], r["rqz"].at[t], grp=other_plane(grp))

    def relay(step):
        if step == 0:
            @pl.when(in_plane)
            def _():
                for kind in range(3, 6):
                    piece(kind, 0).wait()

            for d in range(1, side):
                @pl.when(lax.div(lax.rem(x - d + side, side), steps) == plane)
                def _(d=d):
                    for kind in range(3, 6):
                        piece(kind, d).wait_recv()

        if step > 0:
            ring(step - 1, True).wait_recv()
        if step < steps:
            ring(step, True).start()
        if step > 1:
            cross(step, plane).start()
        if 0 < step < steps:
            ring(step - 1, False).wait_recv()
        if 1 < step < steps:
            cross(side - step, plane).start()
        if step < steps - 1:
            ring(step, False).start()

    g1.begin()

    opposite = side // 2
    odd = lax.rem(x, 2) == 1
    far_x = lax.rem(x + opposite, side)
    far_cut = pl.ds(pl.multiple_of(far_x * head, head), head)
    behind = pl.ds(pl.multiple_of(REACH + lax.rem(x + 1, side) * tok, tok), tok)
    behind_q = pl.ds(pl.multiple_of(lax.rem(x + 1, side) * tok, tok), tok)

    def detour(kind):
        src = v_ref if kind == 1 else q_ref
        return remote(
            src.at[:, far_cut], r["via"].at[kind - 1], r["sv"].at[kind, 0], r["rv"].at[kind - 1],
            sp=left,
        )

    def onward(kind):
        dst = r["vs1"].at[behind, :] if kind == 1 else r["qs1"].at[behind_q, :]
        return remote(
            r["via"].at[kind - 1], dst, r["sv"].at[kind, 1], r["ra2a"].at[kind, opposite],
            sp=y * side + lax.rem(x + opposite + 1, side),
        )

    def hand_out(kinds, distances):
        for d in distances:
            for kind in kinds:
                piece(kind, d).start()

    near, third = [1, side - 1, 2, side - 2], [3, side - 3]
    hand_out([0], near)
    g1.xevent(1)
    g1.xevent(2)
    hand_out([1], near)
    detour(1).start()
    g1.xevent(3)
    g1.xevent(4)
    hand_out([0], third + [opposite])
    g1.yevent(1, 0, 2)
    g1.xevent(5)
    g1.xevent(6)
    hand_out([1], third)
    detour(1).wait_recv()
    onward(1).start()

    @pl.when(odd)
    def _():
        detour(2).start()

    @pl.when(jnp.logical_not(odd))
    def _():
        hand_out([2], [opposite])

    hand_out([2], third + near)

    @pl.when(in_plane)
    def _():
        hand_out([3, 4, 5], range(1, side))

    g1.yevent(1, 2, 2)
    g1.yevent(2, 0, 2)
    g1.xevent(7)

    @pl.when(jnp.logical_not(odd))
    def _():
        detour(2).wait_recv()
        onward(2).start()

    g2.begin()

    g1.yevent(1, 4, 2)
    g1.yevent(2, 2, 2)
    g1.yevent(3, 0, 2)
    g1.yevent(1, 6, 2)
    g1.yevent(2, 4, 2)
    g1.yevent(3, 2, 2)
    take(0)
    take(1)
    halo1 = [
        remote(
            a.at[pl.ds(side * tok, REACH), :], a.at[pl.ds(0, REACH), :],
            r["sh1"].at[i], r["rh1"].at[i], sp=up,
        )
        for i, a in enumerate((r["ks1"], r["vs1"]))
    ]

    @pl.when(y < side - 1)
    def _():
        for copy in halo1:
            copy.start()

    take(2)

    def between():
        g1.yevent(2, 6, 2)
        g1.yevent(3, 4, 2)
        g2.xevent(1)
        g2.xevent(2)
        @pl.when(y > 0)
        def _():
            for copy in halo1:
                copy.wait_recv()


    take_back, back1 = attend_rows(
        side, x, y, r["qs1"], r["ks1"], r["vs1"], r["band1"], r["outs1"], r["mixed1"],
        r["sb1"], r["rb1"], between,
    )
    g1.yevent(3, 6, 2)
    relay(0)
    g2.xevent(3)
    g2.xevent(4)
    g1.yevent(4, 0, 4)
    g1.yevent(4, 4, 4)
    mixed1, mixedz = r["mixed1"], r["mixedz"]

    def lend(block):
        there = pl.ds(pl.multiple_of(block * head, head), head)
        return remote(
            mixed1.at[:, there], mixedz.at[:, there], r["smz"].at[block], r["rmz"].at[block],
            grp=other_plane(grp),
        )

    lend(x).start()
    take_back(lambda block: lend(block).start())

    n = group
    part1, partz, terms = r["part1"], r["partz"], r["terms1"]
    my_half = pl.ds(pl.multiple_of(c * half, half), half)
    their_half = pl.ds(pl.multiple_of(other * half, half), half)

    def columns(j):
        return pl.ds(pl.multiple_of((2 * j + plane) * n, n), n)

    swaps, pooled, given = [], [], []
    for j in range(steps):
        at, lent = columns(j), (r["srz"], r["rrz"])
        swaps.append(
            remote(
                part1.at[their_half, at], terms.at[1, :, at], r["sp1"].at[j], r["rp1"].at[j],
                tp=other,
            )
        )
        pooled.append(
            remote(
                partz.at[their_half, at], r["pool"].at[:, at], lent[0].at[0, j], lent[1].at[0, j],
                tp=other,
            )
        )
        given.append(
            remote(
                r["sums"].at[:, at], terms.at[0, :, at], lent[0].at[1, j], lent[1].at[1, j],
                grp=other_plane(grp),
            )
        )

    def out1(rows, j):
        return lax.dot_general(
            rows[...], r["w1"][columns(j), :], NT, preferred_element_type=F32
        ).astype(BF)

    for j in range(steps):
        part1[:, columns(j)] = out1(mixed1, j)
        swaps[j].start()
        terms[0, :, columns(j)] = part1[my_half, columns(j)]
        rest = pl.ds(pl.multiple_of((2 * j + 1 - plane) * n, n), n)
        terms[1, :, rest] = jnp.zeros((half, n), BF)
    g2.xevent(5)
    g2.xevent(6)
    relay(1)
    g2.ybegin(0, 1, 2, 3)
    for block in range(side):
        lend(block).wait_recv()
    for j in range(steps + 2):
        if j < steps:
            partz[:, columns(j)] = out1(mixedz, j)
            pooled[j].start()
        if j >= 2:
            at = columns(j - 2)
            pooled[j - 2].wait_recv()
            both = partz[my_half, at].astype(F32) + r["pool"][:, at].astype(F32)
            r["sums"][:, at] = both.astype(BF)
            given[j - 2].start()
    for t in (0, 1, side - 1):
        cross(t, plane).start()
    relay(2)
    g2.ybegin(4, 5, 6)
    for copy in swaps + given:
        copy.wait_recv()

    inp, hid = r["inp"], r["hid"]
    chunk = half // 2

    def rows_of(owner, core, i):
        return pl.ds(pl.multiple_of(owner * tok + core * half + i * chunk, chunk), chunk)

    def away(step):
        return lax.rem(x + step + side, side)

    def spread(owner, send, recv, **to):
        return lambda step, i: remote(
            inp.at[rows_of(owner(step), c, i), :], inp.at[rows_of(owner(step), c, i), :],
            send.at[step, i], recv.at[step, i], **to,
        )

    pass_right = spread(lambda s: away(-s), r["sr"], r["rr"], sp=right)
    pass_left = spread(lambda s: away(s), r["sl"], r["rl"], sp=left)
    from_left = spread(lambda s: away(-s - 1), r["sr"], r["rr"], sp=right)
    from_right = spread(lambda s: away(s + 1), r["sl"], r["rl"], sp=left)

    def share(offset, i, core):
        rows = rows_of(away(offset), core, i)
        slot = offset % side
        return remote(
            inp.at[rows, :], inp.at[rows, :], r["sd"].at[slot, i], r["rd"].at[slot, i], tp=other
        )

    def show(i, core):
        rows = rows_of(0, core, i)
        return remote(hid.at[rows, :], hid.at[rows, :], r["sw"].at[i], r["rw"].at[i], tp=other)

    for i in range(2):
        rows = rows_of(0, c, i)
        sub = pl.ds(i * chunk, chunk)
        branch = terms[0, sub, :].astype(F32) + terms[1, sub, :].astype(F32)
        branch = branch.astype(BF).astype(F32)
        scale = lax.rsqrt(jnp.mean(branch * branch, axis=-1, keepdims=True) + EPS)
        hidden = (r["resid"][sub, :].astype(F32) + branch * scale * r["post1"][...]).astype(BF)
        hid[rows, :] = hidden
        long = hidden.astype(F32)
        scale = lax.rsqrt(jnp.mean(long * long, axis=-1, keepdims=True) + EPS)
        inp[rows_of(x, c, i), :] = (long * scale * r["pre2"][...]).astype(BF)
        pass_right(0, i).start()
        pass_left(0, i).start()
        share(0, i, c).start()
        show(i, c).start()

    shift = REACH // tok
    qs2, ks2, vs2 = r["qs2"], r["ks2"], r["vs2"]

    def halo2(owner):
        slot = owner - (side - shift)
        rows = pl.ds(pl.multiple_of(REACH + owner * tok, tok), tok)
        dest = pl.ds(pl.multiple_of(slot * tok, tok), tok)
        return [
            remote(
                a.at[rows, :], a.at[dest, :], r["sh2"].at[i, slot], r["rh2"].at[i, slot], sp=up
            )
            for i, a in enumerate((ks2, vs2))
        ]

    def qkv(offset):
        for i in range(2):
            share(offset, i, other).wait_recv()
        owner = away(offset)
        rows = pl.ds(pl.multiple_of(owner * tok, tok), tok)
        late = pl.ds(pl.multiple_of(REACH + owner * tok, tok), tok)
        done = jnp.dot(inp[rows, :], wall[...], preferred_element_type=F32).astype(BF)
        qs2[rows, :] = done[:, :head]
        ks2[late, :] = done[:, head : 2 * head]
        vs2[late, :] = done[:, 2 * head :]

        @pl.when(jnp.logical_and(owner >= side - shift, y < side - 1))
        def _():
            for copy in halo2(owner):
                copy.start()

    relay(3)
    g2.xevent(7)
    g2.ybegin(7)
    last = steps - 1

    def fill(step, i):
        if (step, i) == (1, 0):
            relay(4)
        elif (step, i) == (1, 1):
            g2.yevent(1, 0, 4)
        elif (step, i) == (2, 0):
            g2.yevent(1, 4, 4)
        elif (step, i) == (2, 1):
            for t in range(side):
                cross(t, 1 - plane).wait_recv()
            qkv(0)
            qkv(-1)
            qkv(1)
            g2.yevent(2, 0, 4)
        elif (step, i) == (3, 0):
            qkv(-2)
            qkv(2)
            g2.yevent(2, 4, 4)

    for step in range(1, steps):
        for i in range(2):
            from_left(step - 1, i).wait_recv()
            if step < last or i == 0:
                pass_right(step, i).start()
            share(-step, i, c).start()
            from_right(step - 1, i).wait_recv()
            if step < last or i == 1:
                pass_left(step, i).start()
            share(step, i, c).start()
            fill(step, i)
    qkv(-last)
    qkv(last)
    from_left(last, 0).wait_recv()
    share(steps, 0, c).start()
    from_right(last, 1).wait_recv()
    share(steps, 1, c).start()
    qkv(steps)

    g2.yevent(3, 0, 4)

    def between2():
        @pl.when(y > 0)
        def _():
            for k in range(shift):
                for copy in halo2(side - shift + k):
                    copy.wait_recv()

        g2.yevent(3, 4, 4)

    take_back, back2 = attend_rows(
        side, x, y, qs2, ks2, vs2, r["band2"], r["outs2"], r["mixed2"], r["sb2"], r["rb2"],
        between2,
    )
    g2.yevent(4, 0, 4)
    for i in range(2):
        show(i, other).wait_recv()
    take_back(lambda block: None)
    g2.yevent(4, 4, 4)
    for kind in range(3):
        for d in range(1, side):
            if kind == 0 or d != opposite:
                piece(kind, d).wait_send()
    detour(1).wait_send()
    onward(1).wait_send()

    @pl.when(odd)
    def _():
        detour(2).wait_send()

    @pl.when(jnp.logical_not(odd))
    def _():
        onward(2).wait_send()
        piece(2, opposite).wait_send()

    @pl.when(in_plane)
    def _():
        for kind in range(3, 6):
            for d in range(1, side):
                piece(kind, d).wait_send()

    for step in range(steps):
        ring(step, True).wait_send()
        if step < last:
            ring(step, False).wait_send()
    for t in range(side):
        cross(t, plane).wait_send()
    g1.sent()
    back1()
    for copy in swaps + pooled + given:
        copy.wait_send()
    for block in range(side):
        lend(block).wait_send()
    for step in range(steps):
        for i in range(2):
            if step < last or i == 0:
                pass_right(step, i).wait_send()
            if step < last or i == 1:
                pass_left(step, i).wait_send()
    for i in range(2):
        show(i, c).wait_send()
        for offset in range(side):
            share(offset, i, c).wait_send()

    @pl.when(y < side - 1)
    def _():
        for copy in halo1:
            copy.wait_send()
        for k in range(shift):
            for copy in halo2(side - shift + k):
                copy.wait_send()

    g2.sent()
    back2()
    g2.zevent()

    part2, theirs2 = r["part2"], r["theirs2"]
    n = model // CUTS
    swaps2 = [
        remote(
            part2.at[:, pl.ds(i * n, n)], theirs2.at[:, pl.ds(i * n, n)],
            r["sp2"].at[i], r["rp2"].at[i], tp=other,
        )
        for i in range(CUTS)
    ]
    for i in range(CUTS):
        done = lax.dot_general(
            r["mixed2"][...], r["w2"][pl.ds(i * n, n), :], NT, preferred_element_type=F32
        )
        part2[:, pl.ds(i * n, n)] = done.astype(BF)
        swaps2[i].start()
    for copy in swaps2:
        copy.wait_recv()
    for i in range(tok // chunk):
        sub = pl.ds(i * chunk, chunk)
        branch = part2[sub, :].astype(F32) + theirs2[sub, :].astype(F32)
        branch = branch.astype(BF).astype(F32)
        scale = lax.rsqrt(jnp.mean(branch * branch, axis=-1, keepdims=True) + EPS)
        done = hid[sub, :].astype(F32) + branch * scale * r["post2"][...]
        r["out"][sub, :] = done.astype(BF)

    for copy in swaps2:
        copy.wait_send()


def shards(
    side, resid, queries_first, keys_first, values_first, rel_first, post_first, out_first,
    pre_second, query_weight, key_weight, value_weight, rel_second, post_second, out_second,
):
    tok, width = queries_first.shape
    model = resid.shape[1]
    head = width // rel_first.shape[0]
    rows = side * tok
    steps = side // 2
    inputs = {
        "q": (queries_first, ANY),
        "k": (keys_first, ANY),
        "v": (values_first, ANY),
        "rel1": (rel_first, VM),
        "rel2": (rel_second, VM),
        "o1": (out_first.T, ANY),
        "o2": (out_second.T, ANY),
        "resid_any": (resid, ANY),
        "post1": (post_first[None], VM),
        "pre2": (pre_second[None], VM),
        "post2": (post_second[None], VM),
        "wq": (query_weight, ANY),
        "wk": (key_weight, ANY),
        "wv": (value_weight, ANY),
    }

    def vmem(*dims):
        return pltpu.VMEM(dims, BF)

    def dma(*dims):
        return pltpu.SemaphoreType.DMA(dims)

    scratch = {
        "wall": vmem(model, 3 * head),
        "inp": vmem(rows, model),
        "hid": vmem(tok, model),
        "resid": vmem(tok // 2, model),
        "terms1": vmem(2, tok // 2, model),
        "mixedz": vmem(tok, width),
        "partz": vmem(tok, model),
        "pool": vmem(tok // 2, model),
        "sums": vmem(tok // 2, model),
        "theirs2": vmem(tok, model),
        "loads": dma(3),
        "via": vmem(2, tok, head),
        "sv": dma(3, 2),
        "rv": dma(2),
        "sa2a": dma(6, side),
        "ra2a": dma(6, side),
    }
    for i in (1, 2):
        scratch[f"w{i}"] = vmem(model, width)
        scratch[f"qs{i}"] = vmem(rows, head)
        scratch[f"ks{i}"] = vmem(rows + REACH, head)
        scratch[f"vs{i}"] = vmem(rows + REACH, head)
        scratch[f"outs{i}"] = vmem(rows, head)
        scratch[f"mixed{i}"] = vmem(tok, width)
        scratch[f"part{i}"] = vmem(tok, model)
        scratch[f"band{i}"] = pltpu.VMEM((tok, tok + REACH), F32)
    for d in "sr":
        for i in (1, 2):
            scratch[f"{d}xr{i}"] = dma(steps)
            scratch[f"{d}xl{i}"] = dma(steps)
            scratch[f"{d}yu{i}"] = dma(steps, side)
            scratch[f"{d}yd{i}"] = dma(steps, side)
            scratch[f"{d}z{i}"] = dma(side, side)
            scratch[f"{d}b{i}"] = dma(side)
            scratch[f"{d}p{i}"] = dma(CUTS)
        scratch[f"{d}mz"] = dma(side)
        scratch[f"{d}rz"] = dma(2, steps)
        scratch[f"{d}qu"] = dma(steps)
        scratch[f"{d}qd"] = dma(steps)
        scratch[f"{d}qz"] = dma(side)
        scratch[f"{d}h1"] = dma(2)
        scratch[f"{d}h2"] = dma(2, REACH // tok)
        scratch[f"{d}r"] = dma(steps, 2)
        scratch[f"{d}l"] = dma(steps, 2)
        scratch[f"{d}d"] = dma(side, 2)
        scratch[f"{d}w"] = dma(2)
    return pl.pallas_call(
        functools.partial(layers_kernel, side, [*inputs, "out", *scratch]),
        out_shape=jax.ShapeDtypeStruct((tok, model), BF),
        in_specs=[spec for _, spec in inputs.values()],
        out_specs=VM,
        scratch_shapes=list(scratch.values()),
        compiler_params=pltpu.CompilerParams(has_side_effects=True, collective_id=0),
    )(*(value for value, _ in inputs.values()))


def solution(mesh):
    side = math.isqrt(mesh.shape["sp"])
    in_specs = (
        P(("grp", "sp"), None),
        P(("grp", "sp"), "tp"),
        P(("grp", "sp"), "tp"),
        P(("grp", "sp"), "tp"),
        P("tp", None),
        P(),
        P("tp", "sp"),
        P(),
        P("sp", "tp"),
        P("sp", "tp"),
        P("sp", "tp"),
        P("tp", None),
        P(),
        P("tp", "sp"),
    )
    out_specs = P(("grp", "sp"), None)
    return jax.shard_map(
        functools.partial(shards, side),
        mesh=mesh,
        in_specs=in_specs,
        out_specs=out_specs,
        check_vma=False,
    )
```

```python
import functools
import math

import jax
import jax.numpy as jnp
from jax import lax
from jax.experimental import pallas as pl
from jax.experimental.pallas import tpu as pltpu
from jax.sharding import PartitionSpec as P

SEG = 64
LEFT = 8
REACH = 512
REL_CLIP = 128
EPS = 1e-06
NEG_FILL = -1e30
LOG2E = 1.4426950408889634
BF = jnp.bfloat16
F32 = jnp.float32
MESH = pl.DeviceIdType.MESH
VM = pl.BlockSpec(memory_space=pltpu.VMEM)
ANY = pl.BlockSpec(memory_space=pl.ANY)
NT = (((1,), (1,)), ((), ()))


def place(side):
    sp = lax.axis_index("sp")
    return lax.rem(sp, side), lax.div(sp, side), lax.axis_index("tp")


def remote(src, dst, send, recv, **where):
    return pltpu.make_async_remote_copy(
        src_ref=src,
        dst_ref=dst,
        send_sem=send,
        recv_sem=recv,
        device_id=dict(where),
        device_id_type=MESH,
    )


def greet(side, x, y, c, grp):
    barrier = pltpu.get_barrier_semaphore()
    peers = [{"sp": y * side + lax.rem(x + d, side)} for d in range(1, side)]
    peers += [{"sp": lax.rem(y + d, side) * side + x} for d in (1, side - 1)]
    peers += [{"tp": 1 - c}]
    peers += [{"grp": other_plane(grp)}]
    for peer in peers:
        pl.semaphore_signal(barrier, inc=1, device_id=peer, device_id_type=MESH)
    return lambda: pl.semaphore_wait(barrier, len(peers))


def other_plane(grp):
    return grp + 1 - 2 * lax.rem(grp, 2)


def spread_bias(table_ref, band_ref, x):
    tok, window = band_ref.shape
    length = window + tok
    near = table_ref[:, : 2 * REL_CLIP]
    far = table_ref[:, 2 * REL_CLIP :]
    end = REACH + REL_CLIP
    slot = end - lax.broadcasted_iota(jnp.int32, (2 * REL_CLIP, length), 1)
    pick = slot == lax.broadcasted_iota(jnp.int32, (2 * REL_CLIP, length), 0)
    lines = jnp.dot(
        near, pick.astype(F32), preferred_element_type=F32, precision=lax.Precision.HIGHEST
    )
    where = lax.broadcasted_iota(jnp.int32, lines.shape, 1)
    lines = jnp.where((where > end - 2 * REL_CLIP) & (where < end), lines, far)
    chosen = lax.broadcasted_iota(jnp.int32, lines.shape, 0) == x
    line = jnp.sum(jnp.where(chosen, lines, 0.0), axis=0, keepdims=True)
    wide = jnp.broadcast_to(line, (tok, length))
    wide = pltpu.roll(wide, 0, 1, stride=1, stride_axis=0)[:, :window] * LOG2E
    qseg = lax.broadcasted_iota(jnp.int32, (tok, window), 0) // SEG
    kseg = lax.broadcasted_iota(jnp.int32, (tok, window), 1) // SEG
    band_ref[...] = jnp.where((kseg >= qseg) & (kseg <= qseg + LEFT), wide, NEG_FILL)


def attend(block, first_row, qs, ks, vs, band_ref):
    tok, window = band_ref.shape
    head = qs.shape[1]
    at = pl.multiple_of(block * tok, tok)
    query = qs[pl.ds(at, tok), :]
    keys = ks[pl.ds(at, window), :]
    values = vs[pl.ds(at, window), :]
    scores = lax.dot_general(query, keys, NT, preferred_element_type=F32)
    scores = scores * (head**-0.5 * LOG2E) + band_ref[...]
    if first_row is not None:
        column = lax.broadcasted_iota(jnp.int32, (1, window), 1) + block * tok
        hidden = jnp.logical_and(column < REACH, first_row)
        scores = scores + jnp.where(hidden, NEG_FILL, 0.0)
    largest = jnp.max(scores, axis=-1, keepdims=True)
    weights = jnp.exp2(scores - largest)
    total = jnp.sum(weights, axis=-1, keepdims=True)
    mixed = jnp.dot(weights.astype(BF), values, preferred_element_type=F32)
    return (mixed / total).astype(BF)


def attend_rows(side, x, y, qs, ks, vs, band, outs, mixed, ssem, rsem, between):
    tok, head = band.shape[0], qs.shape[1]
    here = pl.ds(pl.multiple_of(x * head, head), head)

    def hand_back(block):
        rows = pl.ds(pl.multiple_of(block * tok, tok), tok)
        return remote(
            outs.at[rows, :], mixed.at[:, here], ssem.at[block], rsem.at[x], sp=y * side + block
        )

    def run(block, first_row):
        result = attend(block, first_row, qs, ks, vs, band)
        outs[pl.ds(pl.multiple_of(block * tok, tok), tok), :] = result

        @pl.when(block != x)
        def _():
            hand_back(block).start()

        @pl.when(block == x)
        def _():
            mixed[:, here] = result

    half = REACH // tok

    def late(i, carry):
        run(i + half, None)
        return carry

    lax.fori_loop(0, side - half, late, 0)
    between()

    def early(i, carry):
        run(i, y == 0)
        return carry

    lax.fori_loop(0, half, early, 0)

    def take_back(then):
        def finish(block, carry):
            @pl.when(block != x)
            def _():
                there = pl.ds(pl.multiple_of(block * head, head), head)
                remote(
                    outs.at[pl.ds(0, tok), :],
                    mixed.at[:, there],
                    ssem.at[block],
                    rsem.at[block],
                    sp=y * side + block,
                ).wait_recv()
                then(block)

            return carry

        lax.fori_loop(0, side, finish, 0)

    def sent():
        def finish(block, carry):
            @pl.when(block != x)
            def _():
                hand_back(block).wait_send()

            return carry

        lax.fori_loop(0, side, finish, 0)

    return take_back, sent


def clear_halo(y, ks, vs):
    @pl.when(y == 0)
    def _():
        ks[pl.ds(0, REACH), :] = jnp.zeros((REACH, ks.shape[1]), BF)
        vs[pl.ds(0, REACH), :] = jnp.zeros((REACH, vs.shape[1]), BF)


class Gather:
    def __init__(self, side, x, y, grp, buf, shared, xr, xl, yu, yd, z):
        self.side, self.x, self.y, self.grp, self.buf = side, x, y, grp, buf
        self.xr, self.xl, self.yu, self.yd, self.z = xr, xl, yu, yd, z
        self.shared = shared
        self.rows = buf.shape[0] // (side * side)
        quarter = buf.shape[1] // 4
        self.plane = lax.rem(grp, 2)
        self.inside = pl.ds(0, buf.shape[1])
        if not shared:
            self.inside = pl.ds(pl.multiple_of(self.plane * quarter, quarter), 3 * quarter)
        self.across = pl.ds(pl.multiple_of(self.plane * 3 * quarter, quarter), quarter)
        self.theirs = pl.ds(pl.multiple_of((1 - self.plane) * 3 * quarter, quarter), quarter)

    def guard(self, step):
        if self.shared:
            return pl.when(lax.rem(self.y + step, 2) == self.plane)
        return lambda run: run()

    def slab(self, xp, yp, columns):
        at = pl.multiple_of((yp * self.side + xp) * self.rows, self.rows)
        return self.buf.at[pl.ds(at, self.rows), columns]

    def column(self, k):
        if isinstance(k, int):
            off = -(k + 1) // 2 if k % 2 else k // 2
        else:
            off = jnp.where(lax.rem(k, 2) == 1, -lax.div(k + 1, 2), lax.div(k, 2))
        return lax.rem(self.x + off + self.side, self.side)

    def xcopy(self, step, right):
        owner = lax.rem(self.x + (-step if right else step) + self.side, self.side)
        to = lax.rem(self.x + (1 if right else self.side - 1), self.side)
        part = self.slab(owner, self.y, self.inside)
        send, recv = self.xr if right else self.xl
        return remote(part, part, send.at[step], recv.at[step], sp=self.y * self.side + to)

    def xarrival(self, step, right):
        owner = lax.rem(self.x + (-step - 1 if right else step + 1) + self.side, self.side)
        part = self.slab(owner, self.y, self.inside)
        send, recv = self.xr if right else self.xl
        return remote(part, part, send.at[step], recv.at[step], sp=self.y * self.side + self.x)

    def ycopy(self, step, k, upward):
        owner = lax.rem(self.y + (-step if upward else step) + self.side, self.side)
        to = lax.rem(self.y + (1 if upward else self.side - 1), self.side)
        part = self.slab(self.column(k), owner, self.inside)
        send, recv = self.yu if upward else self.yd
        return remote(part, part, send.at[step, k], recv.at[step, k], sp=to * self.side + self.x)

    def yarrival(self, step, k, upward):
        owner = lax.rem(self.y + (-step - 1 if upward else step + 1) + self.side, self.side)
        part = self.slab(self.column(k), owner, self.inside)
        send, recv = self.yu if upward else self.yd
        return remote(part, part, send.at[step, k], recv.at[step, k], sp=self.x)

    def zcopy(self, t, k, columns):
        owner = lax.rem(self.y - t + self.side, self.side)
        part = self.slab(self.column(k), owner, columns)
        send, recv = self.z
        return remote(part, part, send.at[t, k], recv.at[t, k], grp=other_plane(self.grp))

    def begin(self):
        @self.guard(0)
        def _():
            self.xcopy(0, True).start()
            self.xcopy(0, False).start()
            if self.shared:
                self.ycopy(0, 0, True).start()
                self.ycopy(0, 0, False).start()

    def xevent(self, k):
        right = k % 2 == 1
        step = (k + 1) // 2 if right else k // 2

        @self.guard(0)
        def _():
            self.xarrival(step - 1, right).wait_recv()
            if step < self.side // 2 - (0 if right else 1):
                self.xcopy(step, right).start()
            if self.shared:
                self.ycopy(0, k, True).start()
                self.ycopy(0, k, False).start()
            else:
                self.zcopy(0, k, self.across).start()

    def ybegin(self, *pieces):
        for k in pieces:
            self.ycopy(0, k, True).start()
            self.ycopy(0, k, False).start()

    def yevent(self, step, base, count):
        side = self.side
        half = side // 2
        far = step == half
        lower = base < half

        def one(k, carry):
            if not far or lower:
                self.yarrival(step - 1, k, True).wait_recv()
                if step < half - 1 or (step == half - 1 and lower):
                    self.ycopy(step, k, True).start()
                if not self.shared:
                    self.zcopy(step, k, self.across).start()
            if not far or not lower:
                self.yarrival(step - 1, k, False).wait_recv()
                if step < half - 1 or (step == half - 1 and not lower):
                    self.ycopy(step, k, False).start()
                if not self.shared:
                    self.zcopy(side - step, k, self.across).start()
            return carry

        @self.guard(step)
        def _():
            lax.fori_loop(base, base + count, one, 0)

    def zevent(self):
        side = self.side

        def one(i, carry):
            t, k = lax.div(i, side), lax.rem(i, side)
            self.zcopy(t, k, self.theirs).wait_recv()
            return carry

        lax.fori_loop(1, side * side, one, 0)

    def sent(self):
        side = self.side
        half = side // 2

        @self.guard(0)
        def _():
            for step in range(half):
                self.xcopy(step, True).wait_send()
                if step < half - 1:
                    self.xcopy(step, False).wait_send()

        for step in range(half):

            def one(k, carry, step=step):
                if step < half - 1:
                    self.ycopy(step, k, True).wait_send()
                    self.ycopy(step, k + half, True).wait_send()
                    self.ycopy(step, k, False).wait_send()
                else:
                    self.ycopy(step, k, True).wait_send()
                self.ycopy(step, k + half, False).wait_send()
                return carry

            @self.guard(step)
            def _(one=one):
                lax.fori_loop(0, half, one, 0)

        def one(i, carry):
            self.zcopy(lax.div(i, side), lax.rem(i, side), self.across).wait_send()
            return carry

        if not self.shared:
            lax.fori_loop(1, side * side, one, 0)


CUTS = 4


def layers_kernel(side, names, *refs):
    r = dict(zip(names, refs))
    x, y, c = place(side)
    grp = lax.axis_index("grp")
    plane = lax.rem(grp, 2)
    q_ref, k_ref, v_ref = r["q"], r["k"], r["v"]
    tok, width = q_ref.shape
    head = width // side
    wall = r["wall"]
    wrow = r["wq"].shape[0]
    group = side * wrow
    model = r["w1"].shape[0]
    other = 1 - c
    half = tok // 2
    steps = side // 2
    up = lax.rem(y + 1, side) * side + x
    down = lax.rem(y + side - 1, side) * side + x
    right = y * side + lax.rem(x + 1, side)
    left = y * side + lax.rem(x + side - 1, side)

    meet = greet(side, x, y, c, grp)
    own = pl.ds(pl.multiple_of((y * side + x) * wrow, wrow), wrow)
    loads = [
        pltpu.make_async_copy(r["o1"], r["w1"].at[own, :], r["loads"].at[0]),
        pltpu.make_async_copy(r["o2"], r["w2"].at[own, :], r["loads"].at[1]),
        pltpu.make_async_copy(
            r["resid_any"].at[pl.ds(pl.multiple_of(c * half, half), half), :],
            r["resid"],
            r["loads"].at[2],
        ),
    ]
    for load in loads:
        load.start()
    g1, g2 = [
        Gather(
            side, x, y, grp, r[f"w{i}"], i == 1,
            *((r[f"s{kind}{i}"], r[f"r{kind}{i}"]) for kind in ("xr", "xl", "yu", "yd", "z")),
        )
        for i in (1, 2)
    ]

    mine = pl.ds(pl.multiple_of(x * tok, tok), tok)
    mine_late = pl.ds(pl.multiple_of(REACH + x * tok, tok), tok)
    kinds = [
        (k_ref, r["ks1"].at[mine_late, :]),
        (v_ref, r["vs1"].at[mine_late, :]),
        (q_ref, r["qs1"].at[mine, :]),
    ] + [(r[f"w{n}"], wall.at[own, pl.ds(i * head, head)]) for i, n in enumerate("qkv")]

    def piece(kind, d):
        peer = lax.rem(x + d, side)
        src, dst = kinds[kind]
        cut = src.at[:, pl.ds(pl.multiple_of(peer * head, head), head)]
        if d == 0:
            return pltpu.make_async_copy(cut, dst, r["ra2a"].at[kind, 0])
        send, recv = r["sa2a"].at[kind, d], r["ra2a"].at[kind, d]
        return remote(cut, dst, send, recv, sp=y * side + peer)

    for kind in range(3):
        piece(kind, 0).start()
    in_plane = lax.div(x, steps) == plane

    @pl.when(in_plane)
    def _():
        for kind in range(3, 6):
            piece(kind, 0).start()

    spread_bias(r["rel1"], r["band1"], x)
    spread_bias(r["rel2"], r["band2"], x)
    clear_halo(y, r["ks1"], r["vs1"])
    clear_halo(y, r["ks2"], r["vs2"])
    for load in loads:
        load.wait()
    meet()

    def take(kind):
        piece(kind, 0).wait()
        for d in range(1, side):
            piece(kind, d).wait_recv()

    def ring_rows(owner, parity):
        return pl.ds(pl.multiple_of(owner * group + parity * (group // 2), group // 2), group // 2)

    def ring(step, upward):
        owner = lax.rem(y + (-step if upward else step) + side, side)
        part = wall.at[ring_rows(owner, plane), :]
        send, recv = (r["squ"], r["rqu"]) if upward else (r["sqd"], r["rqd"])
        return remote(part, part, send.at[step], recv.at[step], sp=up if upward else down)

    def cross(t, parity):
        owner = lax.rem(y - t + side, side)
        part = wall.at[ring_rows(owner, parity), :]
        return remote(part, part, r["sqz"].at[t], r["rqz"].at[t], grp=other_plane(grp))

    def relay(step):
        if step == 0:
            @pl.when(in_plane)
            def _():
                for kind in range(3, 6):
                    piece(kind, 0).wait()

            for d in range(1, side):
                @pl.when(lax.div(lax.rem(x - d + side, side), steps) == plane)
                def _(d=d):
                    for kind in range(3, 6):
                        piece(kind, d).wait_recv()

        if step > 0:
            ring(step - 1, True).wait_recv()
        if step < steps:
            ring(step, True).start()
        if step > 1:
            cross(step, plane).start()
        if 0 < step < steps:
            ring(step - 1, False).wait_recv()
        if 1 < step < steps:
            cross(side - step, plane).start()
        if step < steps - 1:
            ring(step, False).start()

    g1.begin()

    opposite = side // 2
    odd = lax.rem(x, 2) == 1
    far_x = lax.rem(x + opposite, side)
    far_cut = pl.ds(pl.multiple_of(far_x * head, head), head)
    behind = pl.ds(pl.multiple_of(REACH + lax.rem(x + 1, side) * tok, tok), tok)
    behind_q = pl.ds(pl.multiple_of(lax.rem(x + 1, side) * tok, tok), tok)

    def detour(kind):
        src = v_ref if kind == 1 else q_ref
        return remote(
            src.at[:, far_cut], r["via"].at[kind - 1], r["sv"].at[kind, 0], r["rv"].at[kind - 1],
            sp=left,
        )

    def onward(kind):
        dst = r["vs1"].at[behind, :] if kind == 1 else r["qs1"].at[behind_q, :]
        return remote(
            r["via"].at[kind - 1], dst, r["sv"].at[kind, 1], r["ra2a"].at[kind, opposite],
            sp=y * side + lax.rem(x + opposite + 1, side),
        )

    def hand_out(kinds, distances):
        for d in distances:
            for kind in kinds:
                piece(kind, d).start()

    near, third = [1, side - 1, 2, side - 2], [3, side - 3]
    hand_out([0], near)
    g1.xevent(1)
    g1.xevent(2)
    hand_out([1], near)
    detour(1).start()
    g1.xevent(3)
    g1.xevent(4)
    hand_out([0], third + [opposite])
    g1.yevent(1, 0, 2)
    g1.xevent(5)
    g1.xevent(6)
    hand_out([1], third)
    detour(1).wait_recv()
    onward(1).start()

    @pl.when(odd)
    def _():
        detour(2).start()

    @pl.when(jnp.logical_not(odd))
    def _():
        hand_out([2], [opposite])

    hand_out([2], third + near)

    @pl.when(in_plane)
    def _():
        hand_out([3, 4, 5], range(1, side))

    g1.yevent(1, 2, 2)
    g1.yevent(2, 0, 2)
    g1.xevent(7)

    @pl.when(jnp.logical_not(odd))
    def _():
        detour(2).wait_recv()
        onward(2).start()

    g2.begin()

    g1.yevent(1, 4, 2)
    g1.yevent(2, 2, 2)
    g1.yevent(3, 0, 2)
    g1.yevent(1, 6, 2)
    g1.yevent(2, 4, 2)
    g1.yevent(3, 2, 2)
    take(0)
    take(1)
    halo1 = [
        remote(
            a.at[pl.ds(side * tok, REACH), :], a.at[pl.ds(0, REACH), :],
            r["sh1"].at[i], r["rh1"].at[i], sp=up,
        )
        for i, a in enumerate((r["ks1"], r["vs1"]))
    ]

    @pl.when(y < side - 1)
    def _():
        for copy in halo1:
            copy.start()

    take(2)

    def between():
        g1.yevent(2, 6, 2)
        g1.yevent(3, 4, 2)
        g2.xevent(1)
        g2.xevent(2)
        @pl.when(y > 0)
        def _():
            for copy in halo1:
                copy.wait_recv()


    take_back, back1 = attend_rows(
        side, x, y, r["qs1"], r["ks1"], r["vs1"], r["band1"], r["outs1"], r["mixed1"],
        r["sb1"], r["rb1"], between,
    )
    g1.yevent(3, 6, 2)
    relay(0)
    g2.xevent(3)
    g2.xevent(4)
    g1.yevent(4, 0, 4)
    g1.yevent(4, 4, 4)
    mixed1, mixedz = r["mixed1"], r["mixedz"]

    def lend(block):
        there = pl.ds(pl.multiple_of(block * head, head), head)
        return remote(
            mixed1.at[:, there], mixedz.at[:, there], r["smz"].at[block], r["rmz"].at[block],
            grp=other_plane(grp),
        )

    lend(x).start()
    take_back(lambda block: lend(block).start())

    n = group
    part1, partz, terms = r["part1"], r["partz"], r["terms1"]
    my_half = pl.ds(pl.multiple_of(c * half, half), half)
    their_half = pl.ds(pl.multiple_of(other * half, half), half)

    def columns(j):
        return pl.ds(pl.multiple_of((2 * j + plane) * n, n), n)

    swaps, pooled, given = [], [], []
    for j in range(steps):
        at, lent = columns(j), (r["srz"], r["rrz"])
        swaps.append(
            remote(
                part1.at[their_half, at], terms.at[1, :, at], r["sp1"].at[j], r["rp1"].at[j],
                tp=other,
            )
        )
        pooled.append(
            remote(
                partz.at[their_half, at], r["pool"].at[:, at], lent[0].at[0, j], lent[1].at[0, j],
                tp=other,
            )
        )
        given.append(
            remote(
                r["sums"].at[:, at], terms.at[0, :, at], lent[0].at[1, j], lent[1].at[1, j],
                grp=other_plane(grp),
            )
        )

    def out1(rows, j):
        return lax.dot_general(
            rows[...], r["w1"][columns(j), :], NT, preferred_element_type=F32
        ).astype(BF)

    for j in range(steps):
        part1[:, columns(j)] = out1(mixed1, j)
        swaps[j].start()
        terms[0, :, columns(j)] = part1[my_half, columns(j)]
        rest = pl.ds(pl.multiple_of((2 * j + 1 - plane) * n, n), n)
        terms[1, :, rest] = jnp.zeros((half, n), BF)
    g2.xevent(5)
    g2.xevent(6)
    relay(1)
    g2.ybegin(0, 1, 2, 3)
    for block in range(side):
        lend(block).wait_recv()
    for j in range(steps + 2):
        if j < steps:
            partz[:, columns(j)] = out1(mixedz, j)
            pooled[j].start()
        if j >= 2:
            at = columns(j - 2)
            pooled[j - 2].wait_recv()
            both = partz[my_half, at].astype(F32) + r["pool"][:, at].astype(F32)
            r["sums"][:, at] = both.astype(BF)
            given[j - 2].start()
    for t in (0, 1, side - 1):
        cross(t, plane).start()
    relay(2)
    g2.ybegin(4, 5, 6)
    for copy in swaps + given:
        copy.wait_recv()

    inp, hid = r["inp"], r["hid"]
    chunk = half // 2

    def rows_of(owner, core, i):
        return pl.ds(pl.multiple_of(owner * tok + core * half + i * chunk, chunk), chunk)

    def away(step):
        return lax.rem(x + step + side, side)

    def spread(owner, send, recv, **to):
        return lambda step, i: remote(
            inp.at[rows_of(owner(step), c, i), :], inp.at[rows_of(owner(step), c, i), :],
            send.at[step, i], recv.at[step, i], **to,
        )

    pass_right = spread(lambda s: away(-s), r["sr"], r["rr"], sp=right)
    pass_left = spread(lambda s: away(s), r["sl"], r["rl"], sp=left)
    from_left = spread(lambda s: away(-s - 1), r["sr"], r["rr"], sp=right)
    from_right = spread(lambda s: away(s + 1), r["sl"], r["rl"], sp=left)

    def share(offset, i, core):
        rows = rows_of(away(offset), core, i)
        slot = offset % side
        return remote(
            inp.at[rows, :], inp.at[rows, :], r["sd"].at[slot, i], r["rd"].at[slot, i], tp=other
        )

    def show(i, core):
        rows = rows_of(0, core, i)
        return remote(hid.at[rows, :], hid.at[rows, :], r["sw"].at[i], r["rw"].at[i], tp=other)

    for i in range(2):
        rows = rows_of(0, c, i)
        sub = pl.ds(i * chunk, chunk)
        branch = terms[0, sub, :].astype(F32) + terms[1, sub, :].astype(F32)
        branch = branch.astype(BF).astype(F32)
        scale = lax.rsqrt(jnp.mean(branch * branch, axis=-1, keepdims=True) + EPS)
        hidden = (r["resid"][sub, :].astype(F32) + branch * scale * r["post1"][...]).astype(BF)
        hid[rows, :] = hidden
        long = hidden.astype(F32)
        scale = lax.rsqrt(jnp.mean(long * long, axis=-1, keepdims=True) + EPS)
        inp[rows_of(x, c, i), :] = (long * scale * r["pre2"][...]).astype(BF)
        pass_right(0, i).start()
        pass_left(0, i).start()
        share(0, i, c).start()
        show(i, c).start()

    shift = REACH // tok
    qs2, ks2, vs2 = r["qs2"], r["ks2"], r["vs2"]

    def halo2(owner):
        slot = owner - (side - shift)
        rows = pl.ds(pl.multiple_of(REACH + owner * tok, tok), tok)
        dest = pl.ds(pl.multiple_of(slot * tok, tok), tok)
        return [
            remote(
                a.at[rows, :], a.at[dest, :], r["sh2"].at[i, slot], r["rh2"].at[i, slot], sp=up
            )
            for i, a in enumerate((ks2, vs2))
        ]

    def qkv(offset):
        for i in range(2):
            share(offset, i, other).wait_recv()
        owner = away(offset)
        rows = pl.ds(pl.multiple_of(owner * tok, tok), tok)
        late = pl.ds(pl.multiple_of(REACH + owner * tok, tok), tok)
        done = jnp.dot(inp[rows, :], wall[...], preferred_element_type=F32).astype(BF)
        qs2[rows, :] = done[:, :head]
        ks2[late, :] = done[:, head : 2 * head]
        vs2[late, :] = done[:, 2 * head :]

        @pl.when(jnp.logical_and(owner >= side - shift, y < side - 1))
        def _():
            for copy in halo2(owner):
                copy.start()

    relay(3)
    g2.xevent(7)
    g2.ybegin(7)
    last = steps - 1

    def fill(step, i):
        if (step, i) == (1, 0):
            relay(4)
        elif (step, i) == (1, 1):
            g2.yevent(1, 0, 4)
        elif (step, i) == (2, 0):
            g2.yevent(1, 4, 4)
        elif (step, i) == (2, 1):
            for t in range(side):
                cross(t, 1 - plane).wait_recv()
            qkv(0)
            qkv(-1)
            qkv(1)
            g2.yevent(2, 0, 4)
        elif (step, i) == (3, 0):
            qkv(-2)
            qkv(2)
            g2.yevent(2, 4, 4)

    for step in range(1, steps):
        for i in range(2):
            from_left(step - 1, i).wait_recv()
            if step < last or i == 0:
                pass_right(step, i).start()
            share(-step, i, c).start()
            from_right(step - 1, i).wait_recv()
            if step < last or i == 1:
                pass_left(step, i).start()
            share(step, i, c).start()
            fill(step, i)
    qkv(-last)
    qkv(last)
    from_left(last, 0).wait_recv()
    share(steps, 0, c).start()
    from_right(last, 1).wait_recv()
    share(steps, 1, c).start()
    qkv(steps)

    g2.yevent(3, 0, 4)

    def between2():
        @pl.when(y > 0)
        def _():
            for k in range(shift):
                for copy in halo2(side - shift + k):
                    copy.wait_recv()

        g2.yevent(3, 4, 4)

    take_back, back2 = attend_rows(
        side, x, y, qs2, ks2, vs2, r["band2"], r["outs2"], r["mixed2"], r["sb2"], r["rb2"],
        between2,
    )
    g2.yevent(4, 0, 4)
    g2.yevent(4, 4, 4)
    for kind in range(3):
        for d in range(1, side):
            if kind == 0 or d != opposite:
                piece(kind, d).wait_send()
    detour(1).wait_send()
    onward(1).wait_send()

    @pl.when(odd)
    def _():
        detour(2).wait_send()

    @pl.when(jnp.logical_not(odd))
    def _():
        onward(2).wait_send()
        piece(2, opposite).wait_send()

    @pl.when(in_plane)
    def _():
        for kind in range(3, 6):
            for d in range(1, side):
                piece(kind, d).wait_send()

    for step in range(steps):
        ring(step, True).wait_send()
        if step < last:
            ring(step, False).wait_send()
    for t in range(side):
        cross(t, plane).wait_send()
    g1.sent()
    back1()
    for copy in swaps + pooled + given:
        copy.wait_send()
    for block in range(side):
        lend(block).wait_send()
    for step in range(steps):
        for i in range(2):
            if step < last or i == 0:
                pass_right(step, i).wait_send()
            if step < last or i == 1:
                pass_left(step, i).wait_send()
    for i in range(2):
        show(i, c).wait_send()
        for offset in range(side):
            share(offset, i, c).wait_send()
    for i in range(2):
        show(i, other).wait_recv()
    take_back(lambda block: None)
    g2.zevent()

    part2, theirs2 = r["part2"], r["theirs2"]
    n = model // CUTS
    swaps2 = [
        remote(
            part2.at[:, pl.ds(i * n, n)], theirs2.at[:, pl.ds(i * n, n)],
            r["sp2"].at[i], r["rp2"].at[i], tp=other,
        )
        for i in range(CUTS)
    ]
    for i in range(CUTS):
        done = lax.dot_general(
            r["mixed2"][...], r["w2"][pl.ds(i * n, n), :], NT, preferred_element_type=F32
        )
        part2[:, pl.ds(i * n, n)] = done.astype(BF)
        swaps2[i].start()
    @pl.when(y < side - 1)
    def _():
        for copy in halo1:
            copy.wait_send()
        for k in range(shift):
            for copy in halo2(side - shift + k):
                copy.wait_send()

    g2.sent()
    back2()
    for copy in swaps2:
        copy.wait_recv()
    for i in range(tok // chunk):
        sub = pl.ds(i * chunk, chunk)
        branch = part2[sub, :].astype(F32) + theirs2[sub, :].astype(F32)
        branch = branch.astype(BF).astype(F32)
        scale = lax.rsqrt(jnp.mean(branch * branch, axis=-1, keepdims=True) + EPS)
        done = hid[sub, :].astype(F32) + branch * scale * r["post2"][...]
        r["out"][sub, :] = done.astype(BF)

    for copy in swaps2:
        copy.wait_send()


def shards(
    side, resid, queries_first, keys_first, values_first, rel_first, post_first, out_first,
    pre_second, query_weight, key_weight, value_weight, rel_second, post_second, out_second,
):
    tok, width = queries_first.shape
    model = resid.shape[1]
    head = width // rel_first.shape[0]
    rows = side * tok
    steps = side // 2
    inputs = {
        "q": (queries_first, ANY),
        "k": (keys_first, ANY),
        "v": (values_first, ANY),
        "rel1": (rel_first, VM),
        "rel2": (rel_second, VM),
        "o1": (out_first.T, ANY),
        "o2": (out_second.T, ANY),
        "resid_any": (resid, ANY),
        "post1": (post_first[None], VM),
        "pre2": (pre_second[None], VM),
        "post2": (post_second[None], VM),
        "wq": (query_weight, ANY),
        "wk": (key_weight, ANY),
        "wv": (value_weight, ANY),
    }

    def vmem(*dims):
        return pltpu.VMEM(dims, BF)

    def dma(*dims):
        return pltpu.SemaphoreType.DMA(dims)

    scratch = {
        "wall": vmem(model, 3 * head),
        "inp": vmem(rows, model),
        "hid": vmem(tok, model),
        "resid": vmem(tok // 2, model),
        "terms1": vmem(2, tok // 2, model),
        "mixedz": vmem(tok, width),
        "partz": vmem(tok, model),
        "pool": vmem(tok // 2, model),
        "sums": vmem(tok // 2, model),
        "theirs2": vmem(tok, model),
        "loads": dma(3),
        "via": vmem(2, tok, head),
        "sv": dma(3, 2),
        "rv": dma(2),
        "sa2a": dma(6, side),
        "ra2a": dma(6, side),
    }
    for i in (1, 2):
        scratch[f"w{i}"] = vmem(model, width)
        scratch[f"qs{i}"] = vmem(rows, head)
        scratch[f"ks{i}"] = vmem(rows + REACH, head)
        scratch[f"vs{i}"] = vmem(rows + REACH, head)
        scratch[f"outs{i}"] = vmem(rows, head)
        scratch[f"mixed{i}"] = vmem(tok, width)
        scratch[f"part{i}"] = vmem(tok, model)
        scratch[f"band{i}"] = pltpu.VMEM((tok, tok + REACH), F32)
    for d in "sr":
        for i in (1, 2):
            scratch[f"{d}xr{i}"] = dma(steps)
            scratch[f"{d}xl{i}"] = dma(steps)
            scratch[f"{d}yu{i}"] = dma(steps, side)
            scratch[f"{d}yd{i}"] = dma(steps, side)
            scratch[f"{d}z{i}"] = dma(side, side)
            scratch[f"{d}b{i}"] = dma(side)
            scratch[f"{d}p{i}"] = dma(CUTS)
        scratch[f"{d}mz"] = dma(side)
        scratch[f"{d}rz"] = dma(2, steps)
        scratch[f"{d}qu"] = dma(steps)
        scratch[f"{d}qd"] = dma(steps)
        scratch[f"{d}qz"] = dma(side)
        scratch[f"{d}h1"] = dma(2)
        scratch[f"{d}h2"] = dma(2, REACH // tok)
        scratch[f"{d}r"] = dma(steps, 2)
        scratch[f"{d}l"] = dma(steps, 2)
        scratch[f"{d}d"] = dma(side, 2)
        scratch[f"{d}w"] = dma(2)
    return pl.pallas_call(
        functools.partial(layers_kernel, side, [*inputs, "out", *scratch]),
        out_shape=jax.ShapeDtypeStruct((tok, model), BF),
        in_specs=[spec for _, spec in inputs.values()],
        out_specs=VM,
        scratch_shapes=list(scratch.values()),
        compiler_params=pltpu.CompilerParams(has_side_effects=True, collective_id=0),
    )(*(value for value, _ in inputs.values()))


def solution(mesh):
    side = math.isqrt(mesh.shape["sp"])
    in_specs = (
        P(("grp", "sp"), None),
        P(("grp", "sp"), "tp"),
        P(("grp", "sp"), "tp"),
        P(("grp", "sp"), "tp"),
        P("tp", None),
        P(),
        P("tp", "sp"),
        P(),
        P("sp", "tp"),
        P("sp", "tp"),
        P("sp", "tp"),
        P("tp", None),
        P(),
        P("tp", "sp"),
    )
    out_specs = P(("grp", "sp"), None)
    return jax.shard_map(
        functools.partial(shards, side),
        mesh=mesh,
        in_specs=in_specs,
        out_specs=out_specs,
        check_vma=False,
    )
```

```python
import functools
import math

import jax
import jax.numpy as jnp
from jax import lax
from jax.experimental import pallas as pl
from jax.experimental.pallas import tpu as pltpu
from jax.sharding import PartitionSpec as P

SEG = 64
LEFT = 8
REACH = 512
REL_CLIP = 128
EPS = 1e-06
NEG_FILL = -1e30
LOG2E = 1.4426950408889634
BF = jnp.bfloat16
F32 = jnp.float32
MESH = pl.DeviceIdType.MESH
VM = pl.BlockSpec(memory_space=pltpu.VMEM)
ANY = pl.BlockSpec(memory_space=pl.ANY)
NT = (((1,), (1,)), ((), ()))


def place(side):
    sp = lax.axis_index("sp")
    return lax.rem(sp, side), lax.div(sp, side), lax.axis_index("tp")


def remote(src, dst, send, recv, **where):
    return pltpu.make_async_remote_copy(
        src_ref=src,
        dst_ref=dst,
        send_sem=send,
        recv_sem=recv,
        device_id=dict(where),
        device_id_type=MESH,
    )


def greet(side, x, y, c, grp):
    barrier = pltpu.get_barrier_semaphore()
    peers = [{"sp": y * side + lax.rem(x + d, side)} for d in range(1, side)]
    peers += [{"sp": lax.rem(y + d, side) * side + x} for d in (1, side - 1)]
    peers += [{"tp": 1 - c}]
    peers += [{"grp": other_plane(grp)}]
    for peer in peers:
        pl.semaphore_signal(barrier, inc=1, device_id=peer, device_id_type=MESH)
    return lambda: pl.semaphore_wait(barrier, len(peers))


def other_plane(grp):
    return grp + 1 - 2 * lax.rem(grp, 2)


def spread_bias(table_ref, band_ref, x):
    tok, window = band_ref.shape
    length = window + tok
    near = table_ref[:, : 2 * REL_CLIP]
    far = table_ref[:, 2 * REL_CLIP :]
    end = REACH + REL_CLIP
    slot = end - lax.broadcasted_iota(jnp.int32, (2 * REL_CLIP, length), 1)
    pick = slot == lax.broadcasted_iota(jnp.int32, (2 * REL_CLIP, length), 0)
    lines = jnp.dot(
        near, pick.astype(F32), preferred_element_type=F32, precision=lax.Precision.HIGHEST
    )
    where = lax.broadcasted_iota(jnp.int32, lines.shape, 1)
    lines = jnp.where((where > end - 2 * REL_CLIP) & (where < end), lines, far)
    chosen = lax.broadcasted_iota(jnp.int32, lines.shape, 0) == x
    line = jnp.sum(jnp.where(chosen, lines, 0.0), axis=0, keepdims=True)
    wide = jnp.broadcast_to(line, (tok, length))
    wide = pltpu.roll(wide, 0, 1, stride=1, stride_axis=0)[:, :window] * LOG2E
    qseg = lax.broadcasted_iota(jnp.int32, (tok, window), 0) // SEG
    kseg = lax.broadcasted_iota(jnp.int32, (tok, window), 1) // SEG
    band_ref[...] = jnp.where((kseg >= qseg) & (kseg <= qseg + LEFT), wide, NEG_FILL)


def attend(block, first_row, qs, ks, vs, band_ref):
    tok, window = band_ref.shape
    head = qs.shape[1]
    at = pl.multiple_of(block * tok, tok)
    query = qs[pl.ds(at, tok), :]
    keys = ks[pl.ds(at, window), :]
    values = vs[pl.ds(at, window), :]
    scores = lax.dot_general(query, keys, NT, preferred_element_type=F32)
    scores = scores * (head**-0.5 * LOG2E) + band_ref[...]
    if first_row is not None:
        column = lax.broadcasted_iota(jnp.int32, (1, window), 1) + block * tok
        hidden = jnp.logical_and(column < REACH, first_row)
        scores = scores + jnp.where(hidden, NEG_FILL, 0.0)
    largest = jnp.max(scores, axis=-1, keepdims=True)
    weights = jnp.exp2(scores - largest)
    total = jnp.sum(weights, axis=-1, keepdims=True)
    mixed = jnp.dot(weights.astype(BF), values, preferred_element_type=F32)
    return (mixed / total).astype(BF)


def attend_rows(side, x, y, qs, ks, vs, band, outs, mixed, ssem, rsem, between):
    tok, head = band.shape[0], qs.shape[1]
    here = pl.ds(pl.multiple_of(x * head, head), head)

    def hand_back(block):
        rows = pl.ds(pl.multiple_of(block * tok, tok), tok)
        return remote(
            outs.at[rows, :], mixed.at[:, here], ssem.at[block], rsem.at[x], sp=y * side + block
        )

    def run(block, first_row):
        result = attend(block, first_row, qs, ks, vs, band)
        outs[pl.ds(pl.multiple_of(block * tok, tok), tok), :] = result

        @pl.when(block != x)
        def _():
            hand_back(block).start()

        @pl.when(block == x)
        def _():
            mixed[:, here] = result

    half = REACH // tok

    def late(i, carry):
        run(i + half, None)
        return carry

    lax.fori_loop(0, side - half, late, 0)
    between()

    def early(i, carry):
        run(i, y == 0)
        return carry

    lax.fori_loop(0, half, early, 0)

    def take_back(then):
        def finish(block, carry):
            @pl.when(block != x)
            def _():
                there = pl.ds(pl.multiple_of(block * head, head), head)
                remote(
                    outs.at[pl.ds(0, tok), :],
                    mixed.at[:, there],
                    ssem.at[block],
                    rsem.at[block],
                    sp=y * side + block,
                ).wait_recv()
                then(block)

            return carry

        lax.fori_loop(0, side, finish, 0)

    def sent():
        def finish(block, carry):
            @pl.when(block != x)
            def _():
                hand_back(block).wait_send()

            return carry

        lax.fori_loop(0, side, finish, 0)

    return take_back, sent


def clear_halo(y, ks, vs):
    @pl.when(y == 0)
    def _():
        ks[pl.ds(0, REACH), :] = jnp.zeros((REACH, ks.shape[1]), BF)
        vs[pl.ds(0, REACH), :] = jnp.zeros((REACH, vs.shape[1]), BF)


class Gather:
    def __init__(self, side, x, y, grp, buf, shared, xr, xl, yu, yd, z):
        self.side, self.x, self.y, self.grp, self.buf = side, x, y, grp, buf
        self.xr, self.xl, self.yu, self.yd, self.z = xr, xl, yu, yd, z
        self.shared = shared
        self.rows = buf.shape[0] // (side * side)
        quarter = buf.shape[1] // 4
        self.plane = lax.rem(grp, 2)
        self.inside = pl.ds(0, buf.shape[1])
        if not shared:
            self.inside = pl.ds(pl.multiple_of(self.plane * quarter, quarter), 3 * quarter)
        self.across = pl.ds(pl.multiple_of(self.plane * 3 * quarter, quarter), quarter)
        self.theirs = pl.ds(pl.multiple_of((1 - self.plane) * 3 * quarter, quarter), quarter)

    def guard(self, step):
        if self.shared:
            return pl.when(lax.rem(self.y + step, 2) == self.plane)
        return lambda run: run()

    def slab(self, xp, yp, columns):
        at = pl.multiple_of((yp * self.side + xp) * self.rows, self.rows)
        return self.buf.at[pl.ds(at, self.rows), columns]

    def column(self, k):
        if isinstance(k, int):
            off = -(k + 1) // 2 if k % 2 else k // 2
        else:
            off = jnp.where(lax.rem(k, 2) == 1, -lax.div(k + 1, 2), lax.div(k, 2))
        return lax.rem(self.x + off + self.side, self.side)

    def xcopy(self, step, right):
        owner = lax.rem(self.x + (-step if right else step) + self.side, self.side)
        to = lax.rem(self.x + (1 if right else self.side - 1), self.side)
        part = self.slab(owner, self.y, self.inside)
        send, recv = self.xr if right else self.xl
        return remote(part, part, send.at[step], recv.at[step], sp=self.y * self.side + to)

    def xarrival(self, step, right):
        owner = lax.rem(self.x + (-step - 1 if right else step + 1) + self.side, self.side)
        part = self.slab(owner, self.y, self.inside)
        send, recv = self.xr if right else self.xl
        return remote(part, part, send.at[step], recv.at[step], sp=self.y * self.side + self.x)

    def ycopy(self, step, k, upward):
        owner = lax.rem(self.y + (-step if upward else step) + self.side, self.side)
        to = lax.rem(self.y + (1 if upward else self.side - 1), self.side)
        part = self.slab(self.column(k), owner, self.inside)
        send, recv = self.yu if upward else self.yd
        return remote(part, part, send.at[step, k], recv.at[step, k], sp=to * self.side + self.x)

    def yarrival(self, step, k, upward):
        owner = lax.rem(self.y + (-step - 1 if upward else step + 1) + self.side, self.side)
        part = self.slab(self.column(k), owner, self.inside)
        send, recv = self.yu if upward else self.yd
        return remote(part, part, send.at[step, k], recv.at[step, k], sp=self.x)

    def zcopy(self, t, k, columns):
        owner = lax.rem(self.y - t + self.side, self.side)
        part = self.slab(self.column(k), owner, columns)
        send, recv = self.z
        return remote(part, part, send.at[t, k], recv.at[t, k], grp=other_plane(self.grp))

    def begin(self):
        @self.guard(0)
        def _():
            self.xcopy(0, True).start()
            self.xcopy(0, False).start()
            if self.shared:
                self.ycopy(0, 0, True).start()
                self.ycopy(0, 0, False).start()

    def xevent(self, k):
        right = k % 2 == 1
        step = (k + 1) // 2 if right else k // 2

        @self.guard(0)
        def _():
            self.xarrival(step - 1, right).wait_recv()
            if step < self.side // 2 - (0 if right else 1):
                self.xcopy(step, right).start()
            if self.shared:
                self.ycopy(0, k, True).start()
                self.ycopy(0, k, False).start()
            else:
                self.zcopy(0, k, self.across).start()

    def ybegin(self, *pieces):
        for k in pieces:
            self.ycopy(0, k, True).start()
            self.ycopy(0, k, False).start()

    def yevent(self, step, base, count):
        side = self.side
        half = side // 2
        far = step == half
        lower = base < half

        def one(k, carry):
            if not far or lower:
                self.yarrival(step - 1, k, True).wait_recv()
                if step < half - 1 or (step == half - 1 and lower):
                    self.ycopy(step, k, True).start()
                if not self.shared:
                    self.zcopy(step, k, self.across).start()
            if not far or not lower:
                self.yarrival(step - 1, k, False).wait_recv()
                if step < half - 1 or (step == half - 1 and not lower):
                    self.ycopy(step, k, False).start()
                if not self.shared:
                    self.zcopy(side - step, k, self.across).start()
            return carry

        @self.guard(step)
        def _():
            lax.fori_loop(base, base + count, one, 0)

    def zevent(self):
        side = self.side

        def one(i, carry):
            t, k = lax.div(i, side), lax.rem(i, side)
            self.zcopy(t, k, self.theirs).wait_recv()
            return carry

        lax.fori_loop(1, side * side, one, 0)

    def sent(self):
        side = self.side
        half = side // 2

        @self.guard(0)
        def _():
            for step in range(half):
                self.xcopy(step, True).wait_send()
                if step < half - 1:
                    self.xcopy(step, False).wait_send()

        for step in range(half):

            def one(k, carry, step=step):
                if step < half - 1:
                    self.ycopy(step, k, True).wait_send()
                    self.ycopy(step, k + half, True).wait_send()
                    self.ycopy(step, k, False).wait_send()
                else:
                    self.ycopy(step, k, True).wait_send()
                self.ycopy(step, k + half, False).wait_send()
                return carry

            @self.guard(step)
            def _(one=one):
                lax.fori_loop(0, half, one, 0)

        def one(i, carry):
            self.zcopy(lax.div(i, side), lax.rem(i, side), self.across).wait_send()
            return carry

        if not self.shared:
            lax.fori_loop(1, side * side, one, 0)


CUTS = 4


def layers_kernel(side, names, *refs):
    r = dict(zip(names, refs))
    x, y, c = place(side)
    grp = lax.axis_index("grp")
    plane = lax.rem(grp, 2)
    q_ref, k_ref, v_ref = r["q"], r["k"], r["v"]
    tok, width = q_ref.shape
    head = width // side
    wall = r["wall"]
    wrow = r["wq"].shape[0]
    group = side * wrow
    model = r["w1"].shape[0]
    other = 1 - c
    half = tok // 2
    steps = side // 2
    up = lax.rem(y + 1, side) * side + x
    down = lax.rem(y + side - 1, side) * side + x
    right = y * side + lax.rem(x + 1, side)
    left = y * side + lax.rem(x + side - 1, side)

    meet = greet(side, x, y, c, grp)
    own = pl.ds(pl.multiple_of((y * side + x) * wrow, wrow), wrow)
    loads = [
        pltpu.make_async_copy(r["o1"], r["w1"].at[own, :], r["loads"].at[0]),
        pltpu.make_async_copy(r["o2"], r["w2"].at[own, :], r["loads"].at[1]),
        pltpu.make_async_copy(
            r["resid_any"].at[pl.ds(pl.multiple_of(c * half, half), half), :],
            r["resid"],
            r["loads"].at[2],
        ),
    ]
    for load in loads:
        load.start()
    g1, g2 = [
        Gather(
            side, x, y, grp, r[f"w{i}"], i == 1,
            *((r[f"s{kind}{i}"], r[f"r{kind}{i}"]) for kind in ("xr", "xl", "yu", "yd", "z")),
        )
        for i in (1, 2)
    ]

    mine = pl.ds(pl.multiple_of(x * tok, tok), tok)
    mine_late = pl.ds(pl.multiple_of(REACH + x * tok, tok), tok)
    kinds = [
        (k_ref, r["ks1"].at[mine_late, :]),
        (v_ref, r["vs1"].at[mine_late, :]),
        (q_ref, r["qs1"].at[mine, :]),
    ] + [(r[f"w{n}"], wall.at[own, pl.ds(i * head, head)]) for i, n in enumerate("qkv")]

    def piece(kind, d):
        peer = lax.rem(x + d, side)
        src, dst = kinds[kind]
        cut = src.at[:, pl.ds(pl.multiple_of(peer * head, head), head)]
        if d == 0:
            return pltpu.make_async_copy(cut, dst, r["ra2a"].at[kind, 0])
        send, recv = r["sa2a"].at[kind, d], r["ra2a"].at[kind, d]
        return remote(cut, dst, send, recv, sp=y * side + peer)

    for kind in range(3):
        piece(kind, 0).start()
    in_plane = lax.div(x, steps) == plane

    @pl.when(in_plane)
    def _():
        for kind in range(3, 6):
            piece(kind, 0).start()

    spread_bias(r["rel1"], r["band1"], x)
    spread_bias(r["rel2"], r["band2"], x)
    clear_halo(y, r["ks1"], r["vs1"])
    clear_halo(y, r["ks2"], r["vs2"])
    for load in loads:
        load.wait()
    meet()

    def take(kind):
        piece(kind, 0).wait()
        for d in range(1, side):
            piece(kind, d).wait_recv()

    def ring_rows(owner, parity):
        return pl.ds(pl.multiple_of(owner * group + parity * (group // 2), group // 2), group // 2)

    def ring(step, upward):
        owner = lax.rem(y + (-step if upward else step) + side, side)
        part = wall.at[ring_rows(owner, plane), :]
        send, recv = (r["squ"], r["rqu"]) if upward else (r["sqd"], r["rqd"])
        return remote(part, part, send.at[step], recv.at[step], sp=up if upward else down)

    def cross(t, parity):
        owner = lax.rem(y - t + side, side)
        part = wall.at[ring_rows(owner, parity), :]
        return remote(part, part, r["sqz"].at[t], r["rqz"].at[t], grp=other_plane(grp))

    def relay(step):
        if step == 0:
            @pl.when(in_plane)
            def _():
                for kind in range(3, 6):
                    piece(kind, 0).wait()

            for d in range(1, side):
                @pl.when(lax.div(lax.rem(x - d + side, side), steps) == plane)
                def _(d=d):
                    for kind in range(3, 6):
                        piece(kind, d).wait_recv()

        if step > 0:
            ring(step - 1, True).wait_recv()
        if step < steps:
            ring(step, True).start()
        if step > 1:
            cross(step, plane).start()
        if 0 < step < steps:
            ring(step - 1, False).wait_recv()
        if 1 < step < steps:
            cross(side - step, plane).start()
        if step < steps - 1:
            ring(step, False).start()

    g1.begin()

    opposite = side // 2
    odd = lax.rem(x, 2) == 1
    far_x = lax.rem(x + opposite, side)
    far_cut = pl.ds(pl.multiple_of(far_x * head, head), head)
    behind = pl.ds(pl.multiple_of(REACH + lax.rem(x + 1, side) * tok, tok), tok)
    behind_q = pl.ds(pl.multiple_of(lax.rem(x + 1, side) * tok, tok), tok)

    def detour(kind):
        src = v_ref if kind == 1 else q_ref
        return remote(
            src.at[:, far_cut], r["via"].at[kind - 1], r["sv"].at[kind, 0], r["rv"].at[kind - 1],
            sp=left,
        )

    def onward(kind):
        dst = r["vs1"].at[behind, :] if kind == 1 else r["qs1"].at[behind_q, :]
        return remote(
            r["via"].at[kind - 1], dst, r["sv"].at[kind, 1], r["ra2a"].at[kind, opposite],
            sp=y * side + lax.rem(x + opposite + 1, side),
        )

    def hand_out(kinds, distances):
        for d in distances:
            for kind in kinds:
                piece(kind, d).start()

    near, third = [1, side - 1, 2, side - 2], [3, side - 3]
    hand_out([0], near)
    g1.xevent(1)
    g1.xevent(2)
    hand_out([1], near)
    detour(1).start()
    g1.xevent(3)
    g1.xevent(4)
    hand_out([0], third + [opposite])
    g1.yevent(1, 0, 2)
    g1.xevent(5)
    g1.xevent(6)
    hand_out([1], third)
    detour(1).wait_recv()
    onward(1).start()

    @pl.when(odd)
    def _():
        detour(2).start()

    @pl.when(jnp.logical_not(odd))
    def _():
        hand_out([2], [opposite])

    hand_out([2], third + near)

    @pl.when(in_plane)
    def _():
        hand_out([3, 4, 5], range(1, side))

    g1.yevent(1, 2, 2)
    g1.yevent(2, 0, 2)
    g1.xevent(7)

    @pl.when(jnp.logical_not(odd))
    def _():
        detour(2).wait_recv()
        onward(2).start()

    g2.begin()

    g1.yevent(1, 4, 2)
    g1.yevent(2, 2, 2)
    g1.yevent(3, 0, 2)
    g1.yevent(1, 6, 2)
    g1.yevent(2, 4, 2)
    g1.yevent(3, 2, 2)
    take(0)
    take(1)
    halo1 = [
        remote(
            a.at[pl.ds(side * tok, REACH), :], a.at[pl.ds(0, REACH), :],
            r["sh1"].at[i], r["rh1"].at[i], sp=up,
        )
        for i, a in enumerate((r["ks1"], r["vs1"]))
    ]

    @pl.when(y < side - 1)
    def _():
        for copy in halo1:
            copy.start()

    take(2)

    def between():
        g1.yevent(2, 6, 2)
        g1.yevent(3, 4, 2)
        g2.xevent(1)
        g2.xevent(2)
        @pl.when(y > 0)
        def _():
            for copy in halo1:
                copy.wait_recv()


    take_back, back1 = attend_rows(
        side, x, y, r["qs1"], r["ks1"], r["vs1"], r["band1"], r["outs1"], r["mixed1"],
        r["sb1"], r["rb1"], between,
    )
    g1.yevent(3, 6, 2)
    relay(0)
    g2.xevent(3)
    g2.xevent(4)
    g1.yevent(4, 0, 4)
    g1.yevent(4, 4, 4)
    mixed1, mixedz = r["mixed1"], r["mixedz"]

    def lend(block):
        there = pl.ds(pl.multiple_of(block * head, head), head)
        return remote(
            mixed1.at[:, there], mixedz.at[:, there], r["smz"].at[block], r["rmz"].at[block],
            grp=other_plane(grp),
        )

    lend(x).start()
    take_back(lambda block: lend(block).start())

    n = group
    part1, partz, terms = r["part1"], r["partz"], r["terms1"]
    my_half = pl.ds(pl.multiple_of(c * half, half), half)
    their_half = pl.ds(pl.multiple_of(other * half, half), half)

    def columns(j):
        return pl.ds(pl.multiple_of((2 * j + plane) * n, n), n)

    swaps, pooled, given = [], [], []
    for j in range(steps):
        at, lent = columns(j), (r["srz"], r["rrz"])
        swaps.append(
            remote(
                part1.at[their_half, at], terms.at[1, :, at], r["sp1"].at[j], r["rp1"].at[j],
                tp=other,
            )
        )
        pooled.append(
            remote(
                partz.at[their_half, at], r["pool"].at[:, at], lent[0].at[0, j], lent[1].at[0, j],
                tp=other,
            )
        )
        given.append(
            remote(
                r["sums"].at[:, at], terms.at[0, :, at], lent[0].at[1, j], lent[1].at[1, j],
                grp=other_plane(grp),
            )
        )

    def out1(rows, j):
        return lax.dot_general(
            rows[...], r["w1"][columns(j), :], NT, preferred_element_type=F32
        ).astype(BF)

    for j in range(steps):
        part1[:, columns(j)] = out1(mixed1, j)
        swaps[j].start()
        terms[0, :, columns(j)] = part1[my_half, columns(j)]
        rest = pl.ds(pl.multiple_of((2 * j + 1 - plane) * n, n), n)
        terms[1, :, rest] = jnp.zeros((half, n), BF)
    g2.xevent(5)
    g2.xevent(6)
    relay(1)
    g2.ybegin(0, 1, 2, 3)
    for block in range(side):
        lend(block).wait_recv()
    for j in range(steps + 2):
        if j < steps:
            partz[:, columns(j)] = out1(mixedz, j)
            pooled[j].start()
        if j >= 2:
            at = columns(j - 2)
            pooled[j - 2].wait_recv()
            both = partz[my_half, at].astype(F32) + r["pool"][:, at].astype(F32)
            r["sums"][:, at] = both.astype(BF)
            given[j - 2].start()
    for t in (0, 1, side - 1):
        cross(t, plane).start()
    relay(2)
    g2.ybegin(4, 5, 6)
    for copy in swaps + given:
        copy.wait_recv()

    inp, hid = r["inp"], r["hid"]
    chunk = half // 2

    def rows_of(owner, core, i):
        return pl.ds(pl.multiple_of(owner * tok + core * half + i * chunk, chunk), chunk)

    def away(step):
        return lax.rem(x + step + side, side)

    def spread(owner, send, recv, **to):
        return lambda step, i: remote(
            inp.at[rows_of(owner(step), c, i), :], inp.at[rows_of(owner(step), c, i), :],
            send.at[step, i], recv.at[step, i], **to,
        )

    pass_right = spread(lambda s: away(-s), r["sr"], r["rr"], sp=right)
    pass_left = spread(lambda s: away(s), r["sl"], r["rl"], sp=left)
    from_left = spread(lambda s: away(-s - 1), r["sr"], r["rr"], sp=right)
    from_right = spread(lambda s: away(s + 1), r["sl"], r["rl"], sp=left)

    def share(offset, i, core):
        rows = rows_of(away(offset), core, i)
        slot = offset % side
        return remote(
            inp.at[rows, :], inp.at[rows, :], r["sd"].at[slot, i], r["rd"].at[slot, i], tp=other
        )

    def show(i, core):
        rows = rows_of(0, core, i)
        return remote(hid.at[rows, :], hid.at[rows, :], r["sw"].at[i], r["rw"].at[i], tp=other)

    for i in range(2):
        rows = rows_of(0, c, i)
        sub = pl.ds(i * chunk, chunk)
        branch = terms[0, sub, :].astype(F32) + terms[1, sub, :].astype(F32)
        branch = branch.astype(BF).astype(F32)
        scale = lax.rsqrt(jnp.mean(branch * branch, axis=-1, keepdims=True) + EPS)
        hidden = (r["resid"][sub, :].astype(F32) + branch * scale * r["post1"][...]).astype(BF)
        hid[rows, :] = hidden
        long = hidden.astype(F32)
        scale = lax.rsqrt(jnp.mean(long * long, axis=-1, keepdims=True) + EPS)
        inp[rows_of(x, c, i), :] = (long * scale * r["pre2"][...]).astype(BF)
        pass_right(0, i).start()
        pass_left(0, i).start()
        share(0, i, c).start()
        show(i, c).start()

    shift = REACH // tok
    qs2, ks2, vs2 = r["qs2"], r["ks2"], r["vs2"]

    def halo2(owner):
        slot = owner - (side - shift)
        rows = pl.ds(pl.multiple_of(REACH + owner * tok, tok), tok)
        dest = pl.ds(pl.multiple_of(slot * tok, tok), tok)
        return [
            remote(
                a.at[rows, :], a.at[dest, :], r["sh2"].at[i, slot], r["rh2"].at[i, slot], sp=up
            )
            for i, a in enumerate((ks2, vs2))
        ]

    def qkv(offset):
        for i in range(2):
            share(offset, i, other).wait_recv()
        owner = away(offset)
        rows = pl.ds(pl.multiple_of(owner * tok, tok), tok)
        late = pl.ds(pl.multiple_of(REACH + owner * tok, tok), tok)
        done = jnp.dot(inp[rows, :], wall[...], preferred_element_type=F32).astype(BF)
        qs2[rows, :] = done[:, :head]
        ks2[late, :] = done[:, head : 2 * head]
        vs2[late, :] = done[:, 2 * head :]

        @pl.when(jnp.logical_and(owner >= side - shift, y < side - 1))
        def _():
            for copy in halo2(owner):
                copy.start()

    relay(3)
    g2.xevent(7)
    g2.ybegin(7)
    last = steps - 1

    def fill(step, i):
        if (step, i) == (1, 0):
            relay(4)
        elif (step, i) == (1, 1):
            g2.yevent(1, 0, 4)
        elif (step, i) == (2, 0):
            g2.yevent(1, 4, 4)
        elif (step, i) == (2, 1):
            for t in range(side):
                cross(t, 1 - plane).wait_recv()
            qkv(0)
            qkv(-1)
            qkv(1)
            g2.yevent(2, 0, 4)
        elif (step, i) == (3, 0):
            qkv(-2)
            qkv(2)
            g2.yevent(2, 4, 4)

    for step in range(1, steps):
        for i in range(2):
            from_left(step - 1, i).wait_recv()
            if step < last or i == 0:
                pass_right(step, i).start()
            share(-step, i, c).start()
            from_right(step - 1, i).wait_recv()
            if step < last or i == 1:
                pass_left(step, i).start()
            share(step, i, c).start()
            fill(step, i)
    qkv(-last)
    qkv(last)
    from_left(last, 0).wait_recv()
    share(steps, 0, c).start()
    from_right(last, 1).wait_recv()
    share(steps, 1, c).start()
    qkv(steps)

    g2.yevent(3, 0, 4)

    def between2():
        g2.yevent(3, 4, 4)
        @pl.when(y > 0)
        def _():
            for k in range(shift):
                for copy in halo2(side - shift + k):
                    copy.wait_recv()


    take_back, back2 = attend_rows(
        side, x, y, qs2, ks2, vs2, r["band2"], r["outs2"], r["mixed2"], r["sb2"], r["rb2"],
        between2,
    )
    g2.yevent(4, 0, 4)
    g2.yevent(4, 4, 4)
    for kind in range(3):
        for d in range(1, side):
            if kind == 0 or d != opposite:
                piece(kind, d).wait_send()
    detour(1).wait_send()
    onward(1).wait_send()

    @pl.when(odd)
    def _():
        detour(2).wait_send()

    @pl.when(jnp.logical_not(odd))
    def _():
        onward(2).wait_send()
        piece(2, opposite).wait_send()

    @pl.when(in_plane)
    def _():
        for kind in range(3, 6):
            for d in range(1, side):
                piece(kind, d).wait_send()

    for step in range(steps):
        ring(step, True).wait_send()
        if step < last:
            ring(step, False).wait_send()
    for t in range(side):
        cross(t, plane).wait_send()
    g1.sent()
    back1()
    for copy in swaps + pooled + given:
        copy.wait_send()
    for block in range(side):
        lend(block).wait_send()
    for step in range(steps):
        for i in range(2):
            if step < last or i == 0:
                pass_right(step, i).wait_send()
            if step < last or i == 1:
                pass_left(step, i).wait_send()
    for i in range(2):
        show(i, c).wait_send()
        for offset in range(side):
            share(offset, i, c).wait_send()
    for i in range(2):
        show(i, other).wait_recv()
    take_back(lambda block: None)
    g2.zevent()

    part2, theirs2 = r["part2"], r["theirs2"]
    n = model // CUTS
    swaps2 = [
        remote(
            part2.at[:, pl.ds(i * n, n)], theirs2.at[:, pl.ds(i * n, n)],
            r["sp2"].at[i], r["rp2"].at[i], tp=other,
        )
        for i in range(CUTS)
    ]
    for i in range(CUTS):
        done = lax.dot_general(
            r["mixed2"][...], r["w2"][pl.ds(i * n, n), :], NT, preferred_element_type=F32
        )
        part2[:, pl.ds(i * n, n)] = done.astype(BF)
        swaps2[i].start()
    @pl.when(y < side - 1)
    def _():
        for copy in halo1:
            copy.wait_send()
        for k in range(shift):
            for copy in halo2(side - shift + k):
                copy.wait_send()

    g2.sent()
    back2()
    for copy in swaps2:
        copy.wait_recv()
    for i in range(tok // chunk):
        sub = pl.ds(i * chunk, chunk)
        branch = part2[sub, :].astype(F32) + theirs2[sub, :].astype(F32)
        branch = branch.astype(BF).astype(F32)
        scale = lax.rsqrt(jnp.mean(branch * branch, axis=-1, keepdims=True) + EPS)
        done = hid[sub, :].astype(F32) + branch * scale * r["post2"][...]
        r["out"][sub, :] = done.astype(BF)

    for copy in swaps2:
        copy.wait_send()


def shards(
    side, resid, queries_first, keys_first, values_first, rel_first, post_first, out_first,
    pre_second, query_weight, key_weight, value_weight, rel_second, post_second, out_second,
):
    tok, width = queries_first.shape
    model = resid.shape[1]
    head = width // rel_first.shape[0]
    rows = side * tok
    steps = side // 2
    inputs = {
        "q": (queries_first, ANY),
        "k": (keys_first, ANY),
        "v": (values_first, ANY),
        "rel1": (rel_first, VM),
        "rel2": (rel_second, VM),
        "o1": (out_first.T, ANY),
        "o2": (out_second.T, ANY),
        "resid_any": (resid, ANY),
        "post1": (post_first[None], VM),
        "pre2": (pre_second[None], VM),
        "post2": (post_second[None], VM),
        "wq": (query_weight, ANY),
        "wk": (key_weight, ANY),
        "wv": (value_weight, ANY),
    }

    def vmem(*dims):
        return pltpu.VMEM(dims, BF)

    def dma(*dims):
        return pltpu.SemaphoreType.DMA(dims)

    scratch = {
        "wall": vmem(model, 3 * head),
        "inp": vmem(rows, model),
        "hid": vmem(tok, model),
        "resid": vmem(tok // 2, model),
        "terms1": vmem(2, tok // 2, model),
        "mixedz": vmem(tok, width),
        "partz": vmem(tok, model),
        "pool": vmem(tok // 2, model),
        "sums": vmem(tok // 2, model),
        "theirs2": vmem(tok, model),
        "loads": dma(3),
        "via": vmem(2, tok, head),
        "sv": dma(3, 2),
        "rv": dma(2),
        "sa2a": dma(6, side),
        "ra2a": dma(6, side),
    }
    for i in (1, 2):
        scratch[f"w{i}"] = vmem(model, width)
        scratch[f"qs{i}"] = vmem(rows, head)
        scratch[f"ks{i}"] = vmem(rows + REACH, head)
        scratch[f"vs{i}"] = vmem(rows + REACH, head)
        scratch[f"outs{i}"] = vmem(rows, head)
        scratch[f"mixed{i}"] = vmem(tok, width)
        scratch[f"part{i}"] = vmem(tok, model)
        scratch[f"band{i}"] = pltpu.VMEM((tok, tok + REACH), F32)
    for d in "sr":
        for i in (1, 2):
            scratch[f"{d}xr{i}"] = dma(steps)
            scratch[f"{d}xl{i}"] = dma(steps)
            scratch[f"{d}yu{i}"] = dma(steps, side)
            scratch[f"{d}yd{i}"] = dma(steps, side)
            scratch[f"{d}z{i}"] = dma(side, side)
            scratch[f"{d}b{i}"] = dma(side)
            scratch[f"{d}p{i}"] = dma(CUTS)
        scratch[f"{d}mz"] = dma(side)
        scratch[f"{d}rz"] = dma(2, steps)
        scratch[f"{d}qu"] = dma(steps)
        scratch[f"{d}qd"] = dma(steps)
        scratch[f"{d}qz"] = dma(side)
        scratch[f"{d}h1"] = dma(2)
        scratch[f"{d}h2"] = dma(2, REACH // tok)
        scratch[f"{d}r"] = dma(steps, 2)
        scratch[f"{d}l"] = dma(steps, 2)
        scratch[f"{d}d"] = dma(side, 2)
        scratch[f"{d}w"] = dma(2)
    return pl.pallas_call(
        functools.partial(layers_kernel, side, [*inputs, "out", *scratch]),
        out_shape=jax.ShapeDtypeStruct((tok, model), BF),
        in_specs=[spec for _, spec in inputs.values()],
        out_specs=VM,
        scratch_shapes=list(scratch.values()),
        compiler_params=pltpu.CompilerParams(has_side_effects=True, collective_id=0),
    )(*(value for value, _ in inputs.values()))


def solution(mesh):
    side = math.isqrt(mesh.shape["sp"])
    in_specs = (
        P(("grp", "sp"), None),
        P(("grp", "sp"), "tp"),
        P(("grp", "sp"), "tp"),
        P(("grp", "sp"), "tp"),
        P("tp", None),
        P(),
        P("tp", "sp"),
        P(),
        P("sp", "tp"),
        P("sp", "tp"),
        P("sp", "tp"),
        P("tp", None),
        P(),
        P("tp", "sp"),
    )
    out_specs = P(("grp", "sp"), None)
    return jax.shard_map(
        functools.partial(shards, side),
        mesh=mesh,
        in_specs=in_specs,
        out_specs=out_specs,
        check_vma=False,
    )
```
